32 devices in a mesh: grp: 2 (over y), sp: 4 (over z), tp: 4 (over x, core).
Axes of the slice: x: 2, y: 2, z: 4, core: 2. Of those that a mesh axis runs over, the one named last changes fastest.
Arguments:
- query_first: bfloat16 [1536, 512], P(('grp', 'sp'), 'tp'), parts along dimension 0, may hold values from -172 to 172
- key_first: bfloat16 [1536, 512], P(('grp', 'sp'), 'tp'), parts along dimension 0, may hold values from -7.8 to 7.8
- query_second: bfloat16 [1536, 1024], P(('grp', 'sp'), 'tp'), parts along dimension 0, may hold values from -172 to 172
- key_second: bfloat16 [1536, 1024], P(('grp', 'sp'), 'tp'), parts along dimension 0, may hold values from -7.8 to 7.8
- values: bfloat16 [1536, 2, 512], P(('grp', 'sp'), None, 'tp'), parts along dimension 0, may hold values from -6 to 6
- lambdas: float32 [2, 4], P(None, 'tp'), may hold values from 0.3 to 0.8
- residual: bfloat16 [1536, 2048], P(('grp', 'sp'), 'tp'), parts along dimension 0, may hold values from -130 to 130
- norm_gain: bfloat16 [2048], P('tp'), may hold values from 0.099609375 to 1.8984375
- out_weight: bfloat16 [2, 512, 2048], P(None, 'tp'), may hold values from -0.1875 to 0.1875
- gate_weight: bfloat16 [2048, 5632], P('sp', 'tp'), may hold values from -0.125 to 0.125
- up_weight: bfloat16 [2048, 5632], P('sp', 'tp'), may hold values from -0.125 to 0.125
- down_weight: bfloat16 [5632, 2048], P('tp', 'sp'), may hold values from -0.078125 to 0.078125
Outputs:
- layer_out: bfloat16 [1536, 2048], P(('grp', 'sp'), 'tp'), parts along dimension 0
The draws below stay inside these ranges and needn't reach their ends.
There are 2 independent parts, one for each index of `grp`. The reference program is written for one: setup_inputs(seed, part) draws one part's arguments, and reference() takes and returns one part's arrays. A program takes and returns all parts, laid end to end along the dimension named above; an argument that names none is the same for every part. Nothing has to cross between parts.
All inputs are finite; a program needn't handle non-finite values.
Results may differ from the reference program's by a relative error of at most 0.0065.
Values may be sent and summed in bfloat16 or wider, within the bound.
A program may use at most 128 MiB of HBM per device.

```python
import jax
import jax.numpy as jnp
from jax import lax

D = 2048
FF = 5632
HEADS = 4
DKA = 64
DKB = 128
DV = 128
SEQ = 768


def paired_draw(key, salt, key_width):
    base = jax.random.fold_in(key, salt)
    key_draw = jax.random.normal(jax.random.fold_in(base, 1), (SEQ, HEADS * 2 * key_width), jnp.float32)
    query_draw = jax.random.normal(jax.random.fold_in(base, 2), (SEQ, HEADS * 2 * key_width), jnp.float32)
    keys_out = 1.3 * jnp.clip(key_draw, -6.0, 6.0)
    queries_out = 1.3 * jnp.clip(query_draw, -6.0, 6.0)
    return (queries_out, keys_out)


def draw_query_first(key, part):
    return paired_draw(key, 11, DKA)[0].astype(jnp.bfloat16)


def draw_key_first(key, part):
    return paired_draw(key, 11, DKA)[1].astype(jnp.bfloat16)


def draw_query_second(key, part):
    return paired_draw(key, 23, DKB)[0].astype(jnp.bfloat16)


def draw_key_second(key, part):
    return paired_draw(key, 23, DKB)[1].astype(jnp.bfloat16)


def draw_residual(key, part):
    base = jax.random.fold_in(key, 37)
    entries = jnp.clip(jax.random.normal(jax.random.fold_in(base, 1), (SEQ, D), jnp.float32), -6.0, 6.0)
    jitter = jnp.clip(jax.random.normal(jax.random.fold_in(base, 2), (1, D), jnp.float32), -2.0, 2.0)
    column = 0.3 * 10.0 ** (jnp.arange(D, dtype=jnp.float32)[None, :] / D + 0.1 * jitter)
    row_scale = 0.3 * 10.0 ** jax.random.uniform(jax.random.fold_in(base, 3), (SEQ, 1), jnp.float32)
    result = entries * column * row_scale
    return result.astype(jnp.bfloat16)


def block_scale(rng, dims, pieces, low, top_value):
    def one(axis_at, parts):
        heights = jax.random.uniform(jax.random.fold_in(jax.random.fold_in(rng, 6), axis_at), (parts,), jnp.float32, low / len(pieces), top_value / len(pieces))
        return jnp.repeat(jnp.exp(heights), dims[axis_at] // parts).reshape((-1,) + (1,) * (len(dims) - axis_at - 1))

    factor_of = one(*pieces[0])
    for cut in pieces[1:]:
        factor_of = factor_of * one(*cut)
    return factor_of


def bell_draw(rng, shape, spread, reach, pieces=(), held_as=jnp.bfloat16):
    values = jax.random.normal(rng, shape, jnp.float32) * spread
    if len(pieces) > 0:
        values = block_scale(rng, shape, pieces, -0.22, 0.18) * values
    return jnp.clip(values, min=-reach, max=reach).astype(held_as)


def setup_inputs(seed: int = 0, part: int = 0) -> dict:
    seeds = jax.random.split(jax.random.key(seed), 13)
    own_keys = jax.random.split(jax.random.fold_in(seeds[12], part), 13)
    query_first = draw_query_first(jax.random.fold_in(jax.random.fold_in(seeds[12], part), 71), part)
    key_first = draw_key_first(jax.random.fold_in(jax.random.fold_in(seeds[12], part), 71), part)
    query_second = draw_query_second(jax.random.fold_in(jax.random.fold_in(seeds[12], part), 71), part)
    key_second = draw_key_second(jax.random.fold_in(jax.random.fold_in(seeds[12], part), 71), part)
    values = bell_draw(own_keys[4], (SEQ, 2, HEADS * DV), 1.0, 6.0, ((0, 4), (2, 4)))
    lambdas = jnp.clip(0.3 + 0.5 * jax.random.uniform(seeds[5], (2, HEADS), jnp.float32) ** block_scale(seeds[5], (2, HEADS), ((1, 4),), -0.2, 0.2), 0.3, 0.8)
    residual = draw_residual(jax.random.fold_in(jax.random.fold_in(seeds[12], part), 71), part)
    norm_gain = jnp.clip(1.0 + 0.18 * jax.random.normal(seeds[7], (D,), jnp.float32), 0.099609375, 1.8984375).astype(jnp.bfloat16)
    out_weight = bell_draw(seeds[8], (2, HEADS * DV, D), (2 * HEADS * DV) ** -0.5, 0.1875, ((1, 4),))
    gate_weight = bell_draw(seeds[9], (D, FF), D ** -0.5, 0.125, ((0, 4), (1, 4)))
    up_weight = bell_draw(seeds[10], (D, FF), D ** -0.5, 0.125, ((0, 4), (1, 4)))
    down_weight = bell_draw(seeds[11], (FF, D), FF ** -0.5, 0.078125, ((0, 4), (1, 4)))
    return dict(query_first=query_first, key_first=key_first, query_second=query_second, key_second=key_second, values=values, lambdas=lambdas, residual=residual, norm_gain=norm_gain, out_weight=out_weight, gate_weight=gate_weight, up_weight=up_weight, down_weight=down_weight)


def one_head(query_rows, key_rows, value_rows, lam_value, key_width):
    block_rows = 512 if SEQ % 512 == 0 else SEQ
    blocks = SEQ // block_rows
    query_blocks = query_rows.reshape(blocks, block_rows, 2, key_width)
    starts = jnp.arange(blocks, dtype=jnp.int32) * block_rows
    key_pos = jnp.arange(SEQ, dtype=jnp.int32)[None, :]
    key_f32 = key_rows.astype(jnp.float32)
    value_f32 = value_rows.astype(jnp.float32)

    def per_block(inputs):
        query_block, offset = inputs
        query_pos = offset + jnp.arange(block_rows, dtype=jnp.int32)[:, None]
        allowed = key_pos <= query_pos
        scores = jnp.einsum('qmd,kmd->mqk', query_block.astype(jnp.float32), key_f32) * key_width ** (-0.5)
        scores = jnp.where(allowed, scores, -1e+30)
        peak = lax.optimization_barrier(jnp.max(scores, axis=-1, keepdims=True))
        weights = jnp.where(allowed, jnp.exp(scores - peak), 0.0)
        totals = lax.optimization_barrier(jnp.sum(weights, axis=-1, keepdims=True))
        rounded = weights.astype(jnp.bfloat16).astype(jnp.float32)
        map_out = jnp.einsum('mqk,ke->mqe', rounded, value_f32) / totals
        differ = map_out[0] - lam_value * map_out[1]
        scale = lax.rsqrt(lax.optimization_barrier(jnp.mean(differ * differ, axis=-1, keepdims=True)) + 1e-06)
        return (0.8 * differ * scale).astype(jnp.bfloat16)
    result = lax.map(per_block, (query_blocks, starts))
    return result.reshape(SEQ, DV)

def reference(query_first, key_first, query_second, key_second, values, lambdas, residual, norm_gain, out_weight, gate_weight, up_weight, down_weight):
    mixed = jnp.zeros((SEQ, D), jnp.float32)
    groups = ((query_first, key_first, DKA), (query_second, key_second, DKB))
    for group_idx in range(2):
        query_all, key_all, key_width = groups[group_idx]
        query_heads = query_all.reshape(SEQ, HEADS, 2, key_width)
        key_heads = key_all.reshape(SEQ, HEADS, 2, key_width)
        value_heads = values[:, group_idx].reshape(SEQ, HEADS, DV)
        outputs = []
        for head in range(HEADS):
            outputs.append(one_head(query_heads[:, head], key_heads[:, head], value_heads[:, head], lambdas[group_idx, head], key_width))
        attended = jnp.concatenate(outputs, axis=1)
        mixed = mixed + jnp.dot(attended, out_weight[group_idx], preferred_element_type=jnp.float32)
    stream = residual.astype(jnp.float32) + mixed
    scale = lax.rsqrt(lax.optimization_barrier(jnp.mean(stream * stream, axis=1, keepdims=True)) + 1e-06)
    normed = (stream * scale * norm_gain.astype(jnp.float32)).astype(jnp.bfloat16)
    gate = jnp.dot(normed, gate_weight, preferred_element_type=jnp.float32)
    up_part = jnp.dot(normed, up_weight, preferred_element_type=jnp.float32)
    hidden = (jax.nn.silu(gate) * up_part).astype(jnp.bfloat16)
    ffn = jnp.dot(hidden, down_weight, preferred_element_type=jnp.float32)
    return (stream + 0.5 * ffn).astype(jnp.bfloat16)
```

```python
import functools

import jax
import jax.numpy as jnp
from jax import lax
from jax.experimental import pallas as pl
from jax.experimental.pallas import tpu as pltpu
from jax.sharding import PartitionSpec as P

D = 2048


def per_device(
    query_first,
    key_first,
    query_second,
    key_second,
    values,
    lambdas,
    residual,
    norm_gain,
    out_weight,
    gate_weight,
    up_weight,
    down_weight,
):
    tok_rows = query_first.shape[0]
    heads_here = lambdas.shape[1]
    width_first = query_first.shape[1] // (2 * heads_here)
    width_second = query_second.shape[1] // (2 * heads_here)
    value_size = values.shape[2] // heads_here
    offset = lax.axis_index("sp") * tok_rows
    query_pos = offset + lax.broadcasted_iota(jnp.int32, (tok_rows, 1), 0)
    query_groups = (
        query_first.reshape(tok_rows, heads_here, 2, width_first),
        query_second.reshape(tok_rows, heads_here, 2, width_second),
    )
    key_widths = (width_first, width_second)
    start_state = (
        jnp.full((heads_here, 2, tok_rows, 1), -1e30, jnp.float32),
        jnp.zeros((heads_here, 2, tok_rows, 1), jnp.float32),
        jnp.zeros((heads_here, 2, tok_rows, value_size), jnp.float32),
    )
    states = (start_state, start_state)
    pieces = (
        lax.all_gather(key_first, "sp", axis=0, tiled=True),
        lax.all_gather(key_second, "sp", axis=0, tiled=True),
        lax.all_gather(values, "sp", axis=0, tiled=True),
    )
    piece_rows = pieces[0].shape[0]
    key_pos = lax.broadcasted_iota(jnp.int32, (1, piece_rows), 1)
    allowed = key_pos <= query_pos
    value_rows = pieces[2].reshape(piece_rows, 2, heads_here, value_size)
    results = []
    for group_idx in range(2):
        key_width = key_widths[group_idx]
        key_part = pieces[group_idx].reshape(piece_rows, heads_here, 2, key_width)
        scores = jnp.einsum(
            "qhmd,khmd->hmqk", query_groups[group_idx], key_part, preferred_element_type=jnp.float32
        ) * key_width ** (-0.5)
        scores = jnp.where(allowed, scores, -1e30)
        running, totals, weighted = states[group_idx]
        new_peak = jnp.maximum(running, jnp.max(scores, axis=-1, keepdims=True))
        weights = jnp.where(allowed, jnp.exp(scores - new_peak), 0.0)
        totals = jnp.sum(weights, axis=-1, keepdims=True)
        weighted = jnp.einsum(
            "hmqk,khe->hmqe",
            weights.astype(jnp.bfloat16),
            value_rows[:, group_idx],
            preferred_element_type=jnp.float32,
        )
        results.append((new_peak, totals, weighted))
    states = (results[0], results[1])
    map_out = jnp.stack([states[0][2] / states[0][1], states[1][2] / states[1][1]])
    differ = map_out[:, :, 0] - lambdas[:, :, None, None] * map_out[:, :, 1]
    head_scale = lax.rsqrt(jnp.mean(differ * differ, axis=-1, keepdims=True) + 1e-06)
    attended = (0.8 * differ * head_scale).astype(jnp.bfloat16)
    projection = out_weight.reshape(2, heads_here, value_size, out_weight.shape[2])
    mixed_part = jnp.einsum(
        "ghqe,gher->qr", attended, projection, preferred_element_type=jnp.float32
    )
    mixed = lax.psum_scatter(
        mixed_part.astype(jnp.bfloat16), "tp", scatter_dimension=1, tiled=True
    ).astype(jnp.float32)
    stream = residual.astype(jnp.float32) + mixed
    squares = lax.psum(jnp.sum(stream * stream, axis=1), "tp")
    row_scale = lax.rsqrt(squares[:, None] / D + 1e-06)
    normed = (stream * row_scale * norm_gain.astype(jnp.float32)).astype(jnp.bfloat16)
    full_rows = lax.all_gather(normed, "tp", axis=1, tiled=True)
    pieces = (
        lax.all_gather(gate_weight, "sp", axis=0, tiled=True),
        lax.all_gather(up_weight, "sp", axis=0, tiled=True),
    )
    gate = jnp.dot(full_rows, pieces[0], preferred_element_type=jnp.float32)
    up_part = jnp.dot(full_rows, pieces[1], preferred_element_type=jnp.float32)
    hidden = (jax.nn.silu(gate) * up_part).astype(jnp.bfloat16)
    partial_out = jnp.dot(
        hidden,
        lax.all_gather(down_weight, "sp", axis=1, tiled=True),
        preferred_element_type=jnp.float32,
    )
    ffn = lax.psum_scatter(
        partial_out.astype(jnp.bfloat16), "tp", scatter_dimension=1, tiled=True
    ).astype(jnp.float32)
    return (stream + 0.5 * ffn).astype(jnp.bfloat16)


def flip(index, bits):
    bit = 1
    while bit <= bits:
        if (bits // bit) % 2:
            index = index + bit - 2 * bit * ((index // bit) % 2)
        bit *= 2
    return index


def nt_dot(a, b):
    return lax.dot_general(a, b, (((1,), (1,)), ((), ())), preferred_element_type=jnp.float32)


def dot(a, b):
    return jnp.dot(a, b, preferred_element_type=jnp.float32)


def scoped(name):
    return jax.named_scope(name)


PLAN = (
    {
        (0, 1): ((1, 0, 3),),
        (1, 0): ((0, 1, 0),),
        (1, 1): ((1, 1, 2), (0, 1, 0), (1, 1, 0)),
        (2, 0): ((1, 2, 0), (0, 2, 0), (0, 2, 1)),
        (2, 1): ((0, 2, 1), (1, 2, 0), (1, 2, 3), (0, 2, 0)),
        (3, 0): ((0, 3, 0), (1, 3, 0), (0, 3, 2), (1, 3, 2)),
        (3, 1): ((0, 3, 0), (0, 3, 2), (0, 3, 1)),
    },
    {
        (0, 0): ((1, 0, 3),),
        (1, 1): ((0, 1, 2), (2, 2)),
        (2, 1): ((3, 1),),
        (3, 1): ((1, 3, 2),),
    },
    {
        (0, 0): ((0, 0, 1),),
        (1, 0): ((0, 1, 3),),
        (2, 0): ((0, 3, 0), (0, 1, 3), (0, 2, 3), (1, 3, 0)),
        (3, 0): ((2, 1),),
    },
    {
        (0, 0): ((0, 0, 3), (1, 0, 1), (2, 1)),
        (0, 1): ((0, 0, 1),),
        (1, 0): ((1, 1, 0), (0, 2, 0), (0, 1, 2)),
        (2, 0): ((1, 2, 1), (2, 1), (3, 3)),
        (2, 1): ((0, 2, 3), (0, 3, 0), (2, 1)),
        (3, 0): ((0, 3, 1),),
    },
    {
        (0, 0): ((5, 0), (0, 0, 2), (2, 2), (1, 0, 2), (4, 1), (2, 3), (4, 2)),
        (0, 1): ((0, 0, 3), (1, 0, 1), (2, 1), (4, 1), (0, 0, 2), (1, 0, 2), (5, 1), (2, 3), (2, 2), (4, 2), (3, 1), (4, 3)),
        (1, 0): ((2, 2), (1, 1, 3), (0, 0, 3), (2, 0), (0, 3, 0), (4, 0), (1, 0, 3), (1, 3, 0), (1, 1, 2), (5, 2), (5, 0), (3, 2), (0, 0, 2), (4, 2), (4, 3), (1, 2, 0), (1, 0, 2), (2, 3), (3, 3)),
        (1, 1): ((4, 0), (2, 0), (1, 0, 3), (0, 2, 0), (0, 3, 0), (0, 1, 3), (0, 0, 3), (1, 1, 3), (5, 1), (4, 2), (3, 0), (2, 3), (0, 0, 2), (4, 3), (5, 3), (1, 0, 2)),
        (2, 0): ((4, 1), (2, 3), (4, 3), (0, 0, 3), (0, 3, 1), (4, 0), (1, 3, 1), (1, 2, 3), (5, 1), (5, 2), (5, 3), (1, 1, 3), (1, 0, 3), (3, 1), (2, 0)),
        (2, 1): ((0, 3, 1), (4, 1), (2, 3), (4, 0), (0, 1, 3), (4, 3), (1, 3, 1), (0, 0, 3), (1, 1, 3), (1, 3, 0), (1, 2, 1), (1, 0, 3), (5, 0), (2, 0), (3, 0), (5, 3), (5, 1)),
        (3, 0): ((5, 3), (4, 2), (2, 2), (1, 3, 1), (4, 1), (2, 0), (5, 0), (4, 0), (3, 2)),
        (3, 1): ((2, 2), (1, 3, 1), (4, 1), (3, 2), (5, 3), (4, 2), (1, 3, 0), (2, 1), (4, 0), (2, 0), (3, 1), (5, 1), (3, 0), (5, 0)),
    },
    {
        (0, 0): ((3, 3), (4, 3), (5, 1), (3, 2), (5, 3), (3, 1), (5, 2)),
        (0, 1): ((3, 2), (5, 0), (5, 3), (5, 2)),
        (1, 0): ((3, 0), (5, 3), (5, 1)),
        (1, 1): ((1, 2, 0), (3, 3), (1, 3, 0), (5, 2), (3, 2)),
        (2, 0): ((5, 0),),
        (2, 1): ((5, 2),),
        (3, 0): ((3, 0), (5, 1), (3, 1)),
    },
    {
        (1, 1): ((5, 0),),
        (2, 0): ((3, 0),),
    },
    {
        (2, 1): ((3, 3),),
        (3, 1): ((5, 2),),
    },
    {
        (0, 1): ((3, 3),),
        (3, 0): ((5, 2),),
    },
    {},
    {},
    {},
    {},
    {},
    {},
    {},
    {},
    {},
    {},
    {},
    {},
    {},
    {},
    {},
    {},
    {},
    {},
    {},
)

WEIGHTS_IN, DOWN_IN, HAND_IN, HAND_DOWN, ROW, ACROSS = range(6)


def transit_slot(here, source, target):
    outer = 0 if source < here else 2
    if outer:
        return outer + (target if here == 2 else source - 2)
    return outer + (target - 2 if here == 1 else source)


def layer_kernel(
    sp_count,
    widths,
    q1_ref,
    q2_ref,
    k1_ref,
    k2_ref,
    v_ref,
    lam_ref,
    residual_ref,
    gain_ref,
    proj_hbm,
    gate_ref,
    up_ref,
    down_ref,
    out_ref,
    k1b,
    k2b,
    vb,
    proj_ref,
    peak,
    total,
    acc,
    wg,
    wu,
    wd,
    tg,
    tu,
    td,
    mp,
    rsb,
    mine_ref,
    stream,
    act,
    gains,
    hid,
    c1,
    c1r,
    po,
    c2,
    c2r,
    c3,
    c3r,
    kv_ss,
    kv_rs,
    w_ss,
    w_rs,
    t_ss,
    t_rs,
    f_ss,
    f_rs,
    own_sem,
    g_ss,
    g_rs,
    rs_ss,
    rs_rs,
    az_ss,
    az_rs,
    ax_ss,
    ax_rs,
    ac_ss,
    ac_rs,
    c_ss,
    c_rs,
):
    s = lax.axis_index("sp")
    t = lax.axis_index("tp")
    y = lax.axis_index("grp")
    rows, blk = residual_ref.shape
    cols = wg.shape[2]
    hidden_all = gate_ref.shape[1]
    xpeer, cpeer, dpeer = flip(t, 2), flip(t, 1), flip(t, 3)
    others = range(1, sp_count)
    everyone = range(sp_count)
    last = sp_count - 1

    def remote(src, dst, ssem, rsem, **where):
        return pltpu.make_async_remote_copy(
            src_ref=src,
            dst_ref=dst,
            send_sem=ssem,
            recv_sem=rsem,
            device_id=where,
            device_id_type=pl.DeviceIdType.MESH,
        )

    def either(test, action):
        pl.when(test)(lambda: action(True))
        pl.when(jnp.logical_not(test))(lambda: action(False))

    barrier = pltpu.get_barrier_semaphore()
    for k in others:
        pl.semaphore_signal(barrier, inc=1, device_id={"sp": flip(s, k)}, device_id_type=pl.DeviceIdType.MESH)
        pl.semaphore_signal(barrier, inc=1, device_id={"tp": flip(t, k)}, device_id_type=pl.DeviceIdType.MESH)
    pl.semaphore_signal(barrier, inc=1, device_id={"grp": 1 - y}, device_id_type=pl.DeviceIdType.MESH)
    with scoped("barrier"):
        pl.semaphore_wait(barrier, 2 * (sp_count - 1) + 1)

    sends = []
    half_d = wg.shape[1] // 2
    extra = sp_count * cols - hidden_all
    d_half = pl.ds(pl.multiple_of(y * half_d, half_d), half_d)

    def kv_copies(back):
        pairs = ((k1_ref, k1b), (k2_ref, k2b), (v_ref, vb))
        right = lax.rem(s + 1, sp_count)
        return [
            remote(dst.at[back] if back else src, dst.at[back + 1], kv_ss.at[i, back], kv_rs.at[i, back + 1], sp=right)
            for i, (src, dst) in enumerate(pairs)
        ]

    def arrived(back):
        pairs = ((k1_ref, k1b), (k2_ref, k2b), (v_ref, vb))
        left = lax.rem(s + sp_count - 1, sp_count)
        return [
            remote(src, dst.at[back], kv_ss.at[i, back - 1], kv_rs.at[i, back], sp=left)
            for i, (src, dst) in enumerate(pairs)
        ]

    def piece_bounds(target):
        short = target == last
        begin = hidden_all - cols + extra if short else target * cols
        return (begin, extra, cols - extra) if short else (begin, 0, cols)

    def own_piece(kind, target):
        src = (gate_ref, up_ref, down_ref)[kind]
        begin, _, size = piece_bounds(target)
        if kind < 2:
            return src.at[d_half, pl.ds(begin, size)]
        return src.at[pl.ds(pl.multiple_of(begin + y * (size // 2), 64), size // 2), :]

    def final_place(kind, source, target):
        dst = (wg, wu, wd)[kind]
        _, skip, size = piece_bounds(target)
        if kind < 2:
            return dst.at[source, d_half, pl.ds(skip, size)]
        return dst.at[source, pl.ds(pl.multiple_of(skip + y * (size // 2), 64), size // 2)]

    def transit_place(kind, here, source, target):
        buffer = (tg, tu, td)[kind].at[transit_slot(here, source, target)]
        _, _, size = piece_bounds(target)
        return buffer.at[:, pl.ds(0, size)] if kind < 2 else buffer.at[pl.ds(0, size // 2)]

    def weight_hop(kind, here, source, target):
        there = here + 1 if target > here else here - 1
        if source == here:
            piece, ssem = own_piece(kind, target), w_ss.at[kind, target]
        else:
            piece, ssem = transit_place(kind, here, source, target), t_ss.at[kind, transit_slot(here, source, target)]
        if there == target:
            place, rsem = final_place(kind, source, target), w_rs.at[kind, source]
        else:
            place, rsem = transit_place(kind, there, source, target), t_rs.at[kind, transit_slot(there, source, target)]
        return remote(piece, place, ssem, rsem, sp=there)

    def move_weights(kinds, here, source, target):
        for kind in kinds:
            if source != here:
                before = here - 1 if source < here else here + 1
                with scoped(f"pass{kind}_{source}{target}"):
                    weight_hop(kind, before, source, target).wait_recv()
            weight_hop(kind, here, source, target).start()

    def weight_hand(kind, source, target):
        place = final_place(kind, source, target)
        return remote(place, place, f_ss.at[kind, source], f_rs.at[kind, source], grp=1 - y)

    def hand_over(kinds, here, source):
        for kind in kinds:
            before = here - 1 if source < here else here + 1
            with scoped(f"hand{kind}_{source}"):
                weight_hop(kind, before, source, here).wait_recv()
            weight_hand(kind, source, here).start()

    def own_copy(kind, short):
        src, dst = ((gate_ref, wg), (up_ref, wu), (down_ref, wd))[kind]
        begin = hidden_all - cols + extra if short else pl.multiple_of(s * cols, 128)
        skip, size = (extra, cols - extra) if short else (0, cols)
        if kind < 2:
            return pltpu.make_async_copy(src.at[:, pl.ds(begin, size)], dst.at[s, :, pl.ds(skip, size)], own_sem.at[kind])
        return pltpu.make_async_copy(src.at[pl.ds(begin, size), :], dst.at[s, pl.ds(skip, size)], own_sem.at[kind])

    def act_z(row, begin, target, way):
        piece = act.at[t, row]
        return remote(piece, piece, az_ss.at[way, row], az_rs.at[row], sp=target)

    def along(here, row, action):
        if row <= here < last:
            action(act_z(row, here, here + 1, 0))
        if row >= here > 0:
            action(act_z(row, here, here - 1, 1))

    def act_x(row):
        piece = act.at[t, row]
        return remote(piece, piece, ax_ss.at[row], ax_rs.at[row], tp=xpeer)

    def act_c(row, second):
        piece = act.at[xpeer if second else t, row]
        return remote(piece, piece, ac_ss.at[second, row], ac_rs.at[second, row], tp=cpeer)

    def start(copy):
        copy.start()

    def perform(here, event):
        kind, index = event[:2]
        if kind == WEIGHTS_IN:
            move_weights((0, 1), here, index, event[2])
        elif kind == DOWN_IN:
            move_weights((2,), here, index, event[2])
        elif kind == HAND_IN:
            hand_over((0, 1), here, index)
        elif kind == HAND_DOWN:
            hand_over((2,), here, index)
        elif kind == ROW:
            with scoped(f"row{index}"):
                act_z(index, here, here, 0).wait_recv()
            send_row(here, index)
        elif kind == ACROSS:
            with scoped(f"across{index}"):
                act_x(index).wait_recv()
            act_c(index, 1).start()

    def send_row(here, row):
        along(here, row, start)
        act_x(row).start()
        act_c(row, 0).start()

    x = t // 2
    steps = iter(PLAN)

    def next_step():
        plan = next(steps)
        for here in everyone:
            lists = [plan.get((here, side), ()) for side in range(2)]
            tests = [(s == here, lists[0])]
            if lists[0] != lists[1]:
                tests = [(jnp.logical_and(s == here, x == side), lists[side]) for side in range(2)]
            for test, events in tests:
                if events:

                    @pl.when(test)
                    def _(here=here, events=events):
                        for event in events:
                            perform(here, event)

    next_step()

    @pl.when(s < last)
    def _():
        for copy in kv_copies(0):
            copy.start()

    @pl.when(s == last)
    def _():
        wg[:, :, :extra] = jnp.zeros((sp_count, wg.shape[1], extra), jnp.bfloat16)
        wu[:, :, :extra] = jnp.zeros((sp_count, wg.shape[1], extra), jnp.bfloat16)
        wd[:, :extra, :] = jnp.zeros((sp_count, extra, blk), jnp.bfloat16)

    proj_copy = pltpu.make_async_copy(proj_hbm, proj_ref, own_sem.at[3])
    proj_copy.start()

    def start_own(short):
        for kind in range(3):
            own_copy(kind, short).start()

    either(s == last, start_own)

    gains[t] = jnp.broadcast_to(gain_ref[...].reshape(1, blk), gains.shape[1:])
    gain_copies = []
    for k in others:
        copy = remote(gains.at[t], gains.at[t], g_ss.at[k], g_rs.at[k], tp=flip(t, k))
        copy.start()
        gain_copies.append(copy)
        sends.append(copy)

    q_refs = (q1_ref, q2_ref)
    lane = lax.broadcasted_iota(jnp.int32, (1, 2 * widths[0]), 1)

    def block(keys, v, diagonal):
        for group in range(2):
            width = widths[group]
            values = v[:, group, :]
            for m in range(2):
                if width % 128:
                    span = slice(0, 2 * width)
                    queries = q_refs[group][:, span]
                    queries = jnp.where(lane // width == m, queries.astype(jnp.float32), 0.0).astype(jnp.bfloat16)
                else:
                    span = slice(m * width, (m + 1) * width)
                    queries = q_refs[group][:, span]
                scores = nt_dot(queries, keys[group][:, span]) * width ** (-0.5)
                state = 2 * group + m
                if diagonal:
                    allowed = lax.broadcasted_iota(jnp.int32, (rows, rows), 1) <= lax.broadcasted_iota(
                        jnp.int32, (rows, rows), 0
                    )
                    scores = jnp.where(allowed, scores, -1e30)
                    top = jnp.max(scores, axis=1, keepdims=True)
                    weights = jnp.exp(scores - top)
                    peak[state] = top
                    total[state] = jnp.sum(weights, axis=1, keepdims=True)
                    acc[state] = dot(weights.astype(jnp.bfloat16), values)
                else:
                    before = peak[state]
                    top = jnp.maximum(before, jnp.max(scores, axis=1, keepdims=True))
                    fade = jnp.exp(before - top)
                    weights = jnp.exp(scores - top)
                    peak[state] = top
                    total[state] = total[state] * fade + jnp.sum(weights, axis=1, keepdims=True)
                    acc[state] = acc[state] * fade + dot(weights.astype(jnp.bfloat16), values)

    with scoped("diag"):
        block((k1_ref, k2_ref), v_ref, True)
    for back in others:

        @pl.when(s >= back)
        def _(back=back):
            with scoped(f"kvwait{back}"):
                for i, copy in enumerate(arrived(back)):
                    copy.wait_recv()
                    if back < last:
                        pl.when(s < last)(kv_copies(back)[i].start)
            with scoped(f"block{back}"):
                block((k1b.at[back], k2b.at[back]), vb.at[back], False)

    next_step()
    proj_copy.wait()
    with scoped("finish"):
        attended = []
        for group in range(2):
            first = acc[2 * group] / total[2 * group]
            second = acc[2 * group + 1] / total[2 * group + 1]
            differ = first - lam_ref[0, group] * second
            scale = lax.rsqrt(jnp.mean(differ * differ, axis=1, keepdims=True) + 1e-06)
            attended.append((0.8 * differ * scale).astype(jnp.bfloat16))

    def project(owner):
        columns = pl.ds(pl.multiple_of(owner * blk, blk), blk)
        return dot(attended[0], proj_ref[0, :, columns]) + dot(attended[1], proj_ref[1, :, columns])

    with scoped("project"):
        mp[0] = project(cpeer).astype(jnp.bfloat16)
        mp[1] = project(dpeer).astype(jnp.bfloat16)
        to_core = remote(mp.at[pl.ds(0, 2)], rsb.at[pl.ds(0, 2)], rs_ss.at[0], rs_rs.at[0], tp=cpeer)
        to_core.start()
        to_x = remote(mp.at[2], rsb.at[2], rs_ss.at[1], rs_rs.at[1], tp=xpeer)
        sends.extend((to_core, to_x))
        mine_ref[1] = project(xpeer)
        mine_ref[0] = residual_ref[...].astype(jnp.float32) + project(t)
    next_step()
    with scoped("rscore"):
        to_core.wait_recv()
    mp[2] = (mine_ref[1] + rsb[1].astype(jnp.float32)).astype(jnp.bfloat16)
    to_x.start()
    mine_ref[0] = mine_ref[0] + rsb[0].astype(jnp.float32)
    next_step()
    with scoped("rsx"):
        to_x.wait_recv()
    stream[...] = mine_ref[0] + rsb[2].astype(jnp.float32)
    act[t, s] = stream[...].astype(jnp.bfloat16)

    for here in everyone:

        @pl.when(s == here)
        def _(here=here):
            send_row(here, here)

    next_step()

    for copy in gain_copies:
        copy.wait_recv()

    def place_of(kind, source, short):
        size = cols - extra if short else cols
        skip = extra if short else 0
        if kind < 2:
            half = pl.ds(pl.multiple_of((1 - y) * half_d, half_d), half_d)
            return (wg, wu)[kind].at[source, half, pl.ds(skip, size)]
        part = (1 - y) * (size // 2)
        return wd.at[source, pl.ds(pl.multiple_of(skip + part, 64), size // 2)]

    def await_weights(kinds, source):
        def go(short):
            for kind in kinds:
                place = place_of(kind, source, short)

                @pl.when(source != s)
                def _(kind=kind, place=place):
                    remote(place, place, f_ss.at[kind, source], f_rs.at[kind, source], grp=1 - y).wait_recv()

                @pl.when(source == s)
                def _(kind=kind):
                    own_copy(kind, short).wait()

        either(s == last, go)

    with scoped("await_gu"):
        for source in everyone:
            await_weights((0, 1), source)
    column = jnp.minimum(s * cols, hidden_all - cols) + lax.broadcasted_iota(jnp.int32, (1, cols), 1)
    mine = column >= s * cols

    def hidden_of(k):
        row = flip(s, k)
        next_step()
        with scoped(f"acwait{k}"):
            act_c(row, 0).wait_recv()
            act_c(row, 1).wait_recv()
        with scoped(f"hidden{k}"):
            squares = jnp.zeros((rows, 1), jnp.float32)
            for part in range(sp_count):
                piece = act[part, row].astype(jnp.float32)
                squares = squares + jnp.sum(piece * piece, axis=1, keepdims=True)
            scale = lax.rsqrt(squares / (sp_count * blk) + 1e-06)
            gate = jnp.zeros((rows, cols), jnp.float32)
            up = jnp.zeros((rows, cols), jnp.float32)
            for part in range(sp_count):
                gain = gains[part, 0:1, :].astype(jnp.float32)
                normed = (act[part, row].astype(jnp.float32) * scale * gain).astype(jnp.bfloat16)
                gate = gate + dot(normed, wg[part])
                up = up + dot(normed, wu[part])
            hidden = gate / (1.0 + jnp.exp(-gate)) * up
            hid[k] = jnp.where(mine, hidden, 0.0).astype(jnp.bfloat16)

    r1a, r1b, r2 = {}, {}, {}
    for k in everyone:
        r1a[k] = remote(c1.at[k, 1], c1r.at[k, 1], c_ss.at[0, k], c_rs.at[0, k], tp=cpeer)
        r1b[k] = remote(c1.at[k, 0], c1r.at[k, 0], c_ss.at[3, k], c_rs.at[3, k], tp=cpeer)
        r2[k] = remote(c2.at[k], c2r.at[k], c_ss.at[1, k], c_rs.at[1, k], tp=xpeer)
    r3 = {k: remote(c3.at[k], c3r.at[k], c_ss.at[2, k], c_rs.at[2, k], sp=flip(s, k - 2 if k == 3 else k)) for k in others}

    def cross(k):
        next_step()
        with scoped(f"cross{k}"):
            c1[k, 1] = dot(hid[k], wd[dpeer]).astype(jnp.bfloat16)
            r1a[k].start()
            po[k, 1] = dot(hid[k], wd[xpeer])

    def to_other_chip(k):
        next_step()
        with scoped(f"r1a{k}"):
            r1a[k].wait_recv()
        c2[k] = (po[k, 1] + c1r[k, 1].astype(jnp.float32)).astype(jnp.bfloat16)
        r2[k].start()

    def near(k):
        next_step()
        with scoped(f"near{k}"):
            c1[k, 0] = dot(hid[k], wd[cpeer]).astype(jnp.bfloat16)
            r1b[k].start()
            po[k, 0] = dot(hid[k], wd[t])

    def finish_row(k):
        next_step()
        with scoped(f"r1b{k}"):
            r1b[k].wait_recv()
        with scoped(f"r2_{k}"):
            r2[k].wait_recv()
        result = po[k, 0] + c1r[k, 0].astype(jnp.float32) + c2r[k].astype(jnp.float32)
        if k == 2:
            with scoped("r3_3"):
                r3[3].wait_recv()
            result = result + c3r[3].astype(jnp.float32)
        if k:
            c3[k] = result.astype(jnp.bfloat16)
            r3[k].start()
        else:
            po[0, 0] = result

    hidden_of(3)
    next_step()
    with scoped("await_cross"):
        await_weights((2,), dpeer)
        await_weights((2,), xpeer)
    cross(3)
    hidden_of(2)
    to_other_chip(3)
    cross(2)
    hidden_of(1)
    to_other_chip(2)
    cross(1)
    hidden_of(0)
    to_other_chip(1)
    cross(0)
    to_other_chip(0)
    next_step()
    with scoped("await_near"):
        await_weights((2,), cpeer)
        await_weights((2,), t)
    near(3)
    near(2)
    finish_row(3)
    near(1)
    near(0)
    finish_row(2)
    finish_row(1)
    finish_row(0)

    next_step()
    ffn = po[0, 0]
    for k in (1, 2):
        with scoped(f"r3_{k}"):
            r3[k].wait_recv()
        ffn = ffn + c3r[k].astype(jnp.float32)
    out_ref[...] = (stream[...] + 0.5 * ffn).astype(jnp.bfloat16)

    with scoped("drain"):
        for here in everyone:

            @pl.when(s == here)
            def _(here=here):
                if here < last:
                    for back in range(here + 1):
                        for copy in kv_copies(back):
                            copy.wait_send()
                for kind in range(3):
                    for there in everyone:
                        if there != here:
                            weight_hop(kind, here, here, there).wait_send()
                            weight_hand(kind, there, here).wait_send()
                    for source in everyone:
                        for target in everyone:
                            if min(source, target) < here < max(source, target):
                                weight_hop(kind, here, source, target).wait_send()
                for row in everyone:
                    along(here, row, lambda copy: copy.wait_send())

        for row in everyone:
            sends.extend((act_x(row), act_c(row, 0), act_c(row, 1)))
        for copies in (r1a, r1b, r2, r3):
            sends.extend(copies.values())
        for copy in sends:
            copy.wait_send()


def fits(axes, query_first, values, lambdas, residual, gate_weight):
    sp, tp = axes["sp"], axes["tp"]
    rows, blk = residual.shape
    depth, hidden_all = gate_weight.shape
    if axes["grp"] != 2 or sp != tp or tp != 4 or lambdas.shape[1] != 1:
        return False
    if depth != blk or blk % 128 or hidden_all % 128 or rows % 16:
        return False
    if (2 * query_first.shape[1]) % 256 or values.shape[2] % 128:
        return False
    cols = -(-hidden_all // (128 * sp)) * 128
    if cols * sp - hidden_all >= cols or cols > hidden_all:
        return False
    if (cols * sp - hidden_all) % 128 or blk % 32:
        return False
    need = 6 * sp * blk * cols + rows * blk * 2 * 20 * sp
    return need < 40 * 1024 * 1024


def one_device(
    axes,
    query_first,
    key_first,
    query_second,
    key_second,
    values,
    lambdas,
    residual,
    norm_gain,
    out_weight,
    gate_weight,
    up_weight,
    down_weight,
):
    if not fits(axes, query_first, values, lambdas, residual, gate_weight):
        return per_device(
            query_first,
            key_first,
            query_second,
            key_second,
            values,
            lambdas,
            residual,
            norm_gain,
            out_weight,
            gate_weight,
            up_weight,
            down_weight,
        )
    n = axes["sp"]
    rows, blk = residual.shape
    hidden_all = gate_weight.shape[1]
    cols = -(-hidden_all // (128 * n)) * 128
    value_size = values.shape[2]
    widths = (query_first.shape[1] // 2, query_second.shape[1] // 2)
    bf16, f32 = jnp.bfloat16, jnp.float32
    vmem = pl.BlockSpec(memory_space=pltpu.VMEM)
    smem = pl.BlockSpec(memory_space=pltpu.SMEM)
    hbm = pl.BlockSpec(memory_space=pl.ANY)
    dma = pltpu.SemaphoreType.DMA
    return pl.pallas_call(
        functools.partial(layer_kernel, n, widths),
        out_shape=jax.ShapeDtypeStruct((rows, blk), bf16),
        in_specs=[vmem] * 5 + [smem, vmem, vmem] + [hbm] * 4,
        out_specs=vmem,
        scratch_shapes=[
            pltpu.VMEM((n,) + key_first.shape, bf16),
            pltpu.VMEM((n,) + key_second.shape, bf16),
            pltpu.VMEM((n,) + values.shape, bf16),
            pltpu.VMEM(out_weight.shape, bf16),
            pltpu.VMEM((4, rows, 1), f32),
            pltpu.VMEM((4, rows, 1), f32),
            pltpu.VMEM((4, rows, value_size), f32),
            pltpu.VMEM((n, blk, cols), bf16),
            pltpu.VMEM((n, blk, cols), bf16),
            pltpu.VMEM((n, cols, blk), bf16),
            pltpu.VMEM((4, blk // 2, cols), bf16),
            pltpu.VMEM((4, blk // 2, cols), bf16),
            pltpu.VMEM((4, cols // 2, blk), bf16),
            pltpu.VMEM((3, rows, blk), bf16),
            pltpu.VMEM((3, rows, blk), bf16),
            pltpu.VMEM((2, rows, blk), f32),
            pltpu.VMEM((rows, blk), f32),
            pltpu.VMEM((n, n, rows, blk), bf16),
            pltpu.VMEM((n, 16, blk), bf16),
            pltpu.VMEM((n, rows, cols), bf16),
            pltpu.VMEM((n, 2, rows, blk), bf16),
            pltpu.VMEM((n, 2, rows, blk), bf16),
            pltpu.VMEM((n, 2, rows, blk), f32),
            pltpu.VMEM((n, rows, blk), bf16),
            pltpu.VMEM((n, rows, blk), bf16),
            pltpu.VMEM((n, rows, blk), bf16),
            pltpu.VMEM((n, rows, blk), bf16),
            dma((3, n)),
            dma((3, n)),
            dma((3, n)),
            dma((3, n)),
            dma((3, n)),
            dma((3, n)),
            dma((3, n)),
            dma((3, n)),
            dma((4,)),
            dma((n,)),
            dma((n,)),
            dma((2,)),
            dma((2,)),
            dma((2, n)),
            dma((n,)),
            dma((n,)),
            dma((n,)),
            dma((2, n)),
            dma((2, n)),
            dma((4, n)),
            dma((4, n)),
        ],
        compiler_params=pltpu.CompilerParams(
            collective_id=0, has_side_effects=True, vmem_limit_bytes=60 * 1024 * 1024
        ),
    )(
        query_first,
        query_second,
        key_first,
        key_second,
        values,
        lambdas.T,
        residual,
        norm_gain,
        out_weight,
        gate_weight,
        up_weight,
        down_weight,
    )

def solution(mesh):
    return jax.shard_map(
        functools.partial(one_device, dict(mesh.shape)),
        mesh=mesh,
        in_specs=(
            P(("grp", "sp"), "tp"),
            P(("grp", "sp"), "tp"),
            P(("grp", "sp"), "tp"),
            P(("grp", "sp"), "tp"),
            P(("grp", "sp"), None, "tp"),
            P(None, "tp"),
            P(("grp", "sp"), "tp"),
            P("tp"),
            P(None, "tp", None),
            P("sp", "tp"),
            P("sp", "tp"),
            P("tp", "sp"),
        ),
        out_specs=P(("grp", "sp"), "tp"),
        check_vma=False,
    )
```

```python
import functools

import jax
import jax.numpy as jnp
from jax import lax
from jax.experimental import pallas as pl
from jax.experimental.pallas import tpu as pltpu
from jax.sharding import PartitionSpec as P

D = 2048


def per_device(
    query_first,
    key_first,
    query_second,
    key_second,
    values,
    lambdas,
    residual,
    norm_gain,
    out_weight,
    gate_weight,
    up_weight,
    down_weight,
):
    tok_rows = query_first.shape[0]
    heads_here = lambdas.shape[1]
    width_first = query_first.shape[1] // (2 * heads_here)
    width_second = query_second.shape[1] // (2 * heads_here)
    value_size = values.shape[2] // heads_here
    offset = lax.axis_index("sp") * tok_rows
    query_pos = offset + lax.broadcasted_iota(jnp.int32, (tok_rows, 1), 0)
    query_groups = (
        query_first.reshape(tok_rows, heads_here, 2, width_first),
        query_second.reshape(tok_rows, heads_here, 2, width_second),
    )
    key_widths = (width_first, width_second)
    start_state = (
        jnp.full((heads_here, 2, tok_rows, 1), -1e30, jnp.float32),
        jnp.zeros((heads_here, 2, tok_rows, 1), jnp.float32),
        jnp.zeros((heads_here, 2, tok_rows, value_size), jnp.float32),
    )
    states = (start_state, start_state)
    pieces = (
        lax.all_gather(key_first, "sp", axis=0, tiled=True),
        lax.all_gather(key_second, "sp", axis=0, tiled=True),
        lax.all_gather(values, "sp", axis=0, tiled=True),
    )
    piece_rows = pieces[0].shape[0]
    key_pos = lax.broadcasted_iota(jnp.int32, (1, piece_rows), 1)
    allowed = key_pos <= query_pos
    value_rows = pieces[2].reshape(piece_rows, 2, heads_here, value_size)
    results = []
    for group_idx in range(2):
        key_width = key_widths[group_idx]
        key_part = pieces[group_idx].reshape(piece_rows, heads_here, 2, key_width)
        scores = jnp.einsum(
            "qhmd,khmd->hmqk", query_groups[group_idx], key_part, preferred_element_type=jnp.float32
        ) * key_width ** (-0.5)
        scores = jnp.where(allowed, scores, -1e30)
        running, totals, weighted = states[group_idx]
        new_peak = jnp.maximum(running, jnp.max(scores, axis=-1, keepdims=True))
        weights = jnp.where(allowed, jnp.exp(scores - new_peak), 0.0)
        totals = jnp.sum(weights, axis=-1, keepdims=True)
        weighted = jnp.einsum(
            "hmqk,khe->hmqe",
            weights.astype(jnp.bfloat16),
            value_rows[:, group_idx],
            preferred_element_type=jnp.float32,
        )
        results.append((new_peak, totals, weighted))
    states = (results[0], results[1])
    map_out = jnp.stack([states[0][2] / states[0][1], states[1][2] / states[1][1]])
    differ = map_out[:, :, 0] - lambdas[:, :, None, None] * map_out[:, :, 1]
    head_scale = lax.rsqrt(jnp.mean(differ * differ, axis=-1, keepdims=True) + 1e-06)
    attended = (0.8 * differ * head_scale).astype(jnp.bfloat16)
    projection = out_weight.reshape(2, heads_here, value_size, out_weight.shape[2])
    mixed_part = jnp.einsum(
        "ghqe,gher->qr", attended, projection, preferred_element_type=jnp.float32
    )
    mixed = lax.psum_scatter(
        mixed_part.astype(jnp.bfloat16), "tp", scatter_dimension=1, tiled=True
    ).astype(jnp.float32)
    stream = residual.astype(jnp.float32) + mixed
    squares = lax.psum(jnp.sum(stream * stream, axis=1), "tp")
    row_scale = lax.rsqrt(squares[:, None] / D + 1e-06)
    normed = (stream * row_scale * norm_gain.astype(jnp.float32)).astype(jnp.bfloat16)
    full_rows = lax.all_gather(normed, "tp", axis=1, tiled=True)
    pieces = (
        lax.all_gather(gate_weight, "sp", axis=0, tiled=True),
        lax.all_gather(up_weight, "sp", axis=0, tiled=True),
    )
    gate = jnp.dot(full_rows, pieces[0], preferred_element_type=jnp.float32)
    up_part = jnp.dot(full_rows, pieces[1], preferred_element_type=jnp.float32)
    hidden = (jax.nn.silu(gate) * up_part).astype(jnp.bfloat16)
    partial_out = jnp.dot(
        hidden,
        lax.all_gather(down_weight, "sp", axis=1, tiled=True),
        preferred_element_type=jnp.float32,
    )
    ffn = lax.psum_scatter(
        partial_out.astype(jnp.bfloat16), "tp", scatter_dimension=1, tiled=True
    ).astype(jnp.float32)
    return (stream + 0.5 * ffn).astype(jnp.bfloat16)


def flip(index, bits):
    bit = 1
    while bit <= bits:
        if (bits // bit) % 2:
            index = index + bit - 2 * bit * ((index // bit) % 2)
        bit *= 2
    return index


def nt_dot(a, b):
    return lax.dot_general(a, b, (((1,), (1,)), ((), ())), preferred_element_type=jnp.float32)


def dot(a, b):
    return jnp.dot(a, b, preferred_element_type=jnp.float32)


def scoped(name):
    return jax.named_scope(name)


PLAN = (
    {
        (1, 0): ((0, 1, 0),),
        (1, 1): ((1, 1, 3), (0, 1, 0)),
        (2, 0): ((0, 2, 0), (1, 2, 1), (1, 2, 3), (1, 2, 0)),
        (2, 1): ((0, 2, 3), (1, 2, 1), (0, 2, 0), (1, 2, 0)),
        (3, 0): ((1, 3, 0), (0, 3, 0), (0, 3, 1), (0, 3, 2), (1, 3, 2)),
        (3, 1): ((0, 3, 0), (1, 3, 0), (0, 3, 2), (1, 3, 1)),
    },
    {
        (0, 0): ((0, 0, 2),),
        (0, 1): ((0, 0, 1),),
        (1, 0): ((0, 1, 3),),
        (2, 0): ((0, 2, 1),),
        (2, 1): ((0, 3, 0), (1, 1, 3)),
    },
    {
        (1, 1): ((0, 1, 2), (0, 2, 0)),
        (2, 0): ((1, 3, 0),),
        (2, 1): ((0, 2, 1), (2, 3)),
        (3, 1): ((0, 3, 1),),
    },
    {
        (0, 0): ((1, 0, 3),),
        (0, 1): ((2, 1),),
        (1, 0): ((0, 1, 2), (0, 2, 0)),
        (1, 1): ((1, 2, 0), (3, 2), (0, 1, 3)),
        (2, 0): ((0, 1, 3), (0, 2, 3), (0, 3, 0), (2, 3)),
    },
    {
        (0, 0): ((2, 1), (0, 0, 3), (2, 2), (4, 1), (0, 0, 1), (3, 3), (1, 0, 2), (5, 1), (1, 0, 1), (2, 3), (4, 2), (4, 3), (3, 2), (5, 0), (3, 1), (5, 2), (5, 3)),
        (0, 1): ((0, 0, 2), (5, 0), (1, 0, 3), (1, 0, 1), (4, 1), (5, 1), (0, 0, 3), (2, 2), (1, 0, 2), (3, 2), (3, 1), (2, 3), (3, 3), (4, 2), (4, 3), (5, 2), (5, 3)),
        (1, 0): ((4, 0), (1, 1, 0), (0, 0, 3), (3, 2), (1, 3, 0), (0, 0, 2), (2, 2), (1, 0, 3), (0, 3, 0), (2, 0), (4, 2), (4, 3), (1, 0, 2), (1, 2, 0), (1, 1, 3), (1, 1, 2), (2, 3), (5, 1), (3, 3), (3, 0), (5, 2), (5, 3), (5, 0)),
        (1, 1): ((4, 0), (1, 1, 0), (0, 0, 2), (2, 0), (0, 3, 0), (5, 1), (1, 1, 2), (4, 2), (2, 2), (0, 0, 3), (3, 0), (1, 3, 0), (4, 3), (5, 0), (1, 0, 3), (1, 0, 2), (2, 3), (5, 2), (3, 3), (5, 3)),
        (2, 0): ((2, 1), (4, 0), (4, 3), (5, 0), (0, 0, 3), (3, 3), (0, 3, 1), (5, 2), (4, 1), (2, 0), (1, 3, 1), (5, 3), (3, 0), (1, 0, 3), (5, 1)),
        (2, 1): ((1, 3, 0), (4, 1), (2, 1), (4, 0), (4, 3), (1, 2, 3), (2, 0), (0, 3, 1), (0, 1, 3), (1, 3, 1), (5, 0), (3, 3), (3, 1), (5, 2), (5, 3), (0, 0, 3)),
        (3, 0): ((1, 3, 1), (2, 2), (3, 2), (4, 2), (4, 0), (2, 1), (2, 0), (4, 1), (5, 0), (3, 0)),
        (3, 1): ((1, 3, 2), (4, 2), (3, 1), (2, 2), (4, 0), (4, 1), (3, 2), (2, 1), (5, 0), (5, 2), (2, 0), (3, 0), (5, 3), (5, 1)),
    },
    {
        (2, 1): ((1, 0, 3), (5, 1), (3, 0)),
    },
    {
        (3, 0): ((5, 1), (3, 1)),
    },
    {
        (3, 0): ((5, 3), (5, 2)),
    },
    {
        (2, 0): ((1, 1, 3),),
    },
    {},
    {},
    {},
    {
        (2, 0): ((3, 1),),
    },
    {},
    {},
    {},
    {},
    {},
    {},
    {},
    {},
    {},
    {},
    {},
    {},
    {},
    {},
    {},
    {},
    {},
    {},
    {},
)

WEIGHTS_IN, DOWN_IN, HAND_IN, HAND_DOWN, ROW, ACROSS = range(6)


PARTS = 2


def transit_slot(here, source, target):
    outer = 0 if source < here else 2
    if outer:
        return outer + (target if here == 2 else source - 2)
    return outer + (target - 2 if here == 1 else source)


def layer_kernel(
    sp_count,
    widths,
    q1_ref,
    q2_ref,
    k1_ref,
    k2_ref,
    v_ref,
    lam_ref,
    residual_ref,
    gain_ref,
    proj_hbm,
    gate_ref,
    up_ref,
    down_ref,
    out_ref,
    k1b,
    k2b,
    vb,
    proj_ref,
    peak,
    total,
    acc,
    wg,
    wu,
    wd,
    tg,
    tu,
    td,
    mp,
    rsb,
    mine_ref,
    stream,
    act,
    gains,
    hid,
    c1,
    c1r,
    po,
    c2,
    c2r,
    c3,
    c3r,
    kv_ss,
    kv_rs,
    w_ss,
    w_rs,
    t_ss,
    t_rs,
    f_ss,
    f_rs,
    own_sem,
    g_ss,
    g_rs,
    rs_ss,
    rs_rs,
    az_ss,
    az_rs,
    ax_ss,
    ax_rs,
    ac_ss,
    ac_rs,
    c_ss,
    c_rs,
):
    s = lax.axis_index("sp")
    t = lax.axis_index("tp")
    y = lax.axis_index("grp")
    rows, blk = residual_ref.shape
    cols = wg.shape[2]
    hidden_all = gate_ref.shape[1]
    xpeer, cpeer, dpeer = flip(t, 2), flip(t, 1), flip(t, 3)
    others = range(1, sp_count)
    everyone = range(sp_count)
    last = sp_count - 1

    def remote(src, dst, ssem, rsem, **where):
        return pltpu.make_async_remote_copy(
            src_ref=src,
            dst_ref=dst,
            send_sem=ssem,
            recv_sem=rsem,
            device_id=where,
            device_id_type=pl.DeviceIdType.MESH,
        )

    def either(test, action):
        pl.when(test)(lambda: action(True))
        pl.when(jnp.logical_not(test))(lambda: action(False))

    barrier = pltpu.get_barrier_semaphore()
    for k in others:
        pl.semaphore_signal(barrier, inc=1, device_id={"sp": flip(s, k)}, device_id_type=pl.DeviceIdType.MESH)
        pl.semaphore_signal(barrier, inc=1, device_id={"tp": flip(t, k)}, device_id_type=pl.DeviceIdType.MESH)
    pl.semaphore_signal(barrier, inc=1, device_id={"grp": 1 - y}, device_id_type=pl.DeviceIdType.MESH)
    with scoped("barrier"):
        pl.semaphore_wait(barrier, 2 * (sp_count - 1) + 1)

    half_d = wg.shape[1] // 2
    extra = sp_count * cols - hidden_all
    d_half = pl.ds(pl.multiple_of(y * half_d, half_d), half_d)

    def kv_copies(back):
        pairs = ((k1_ref, k1b), (k2_ref, k2b), (v_ref, vb))
        right = lax.rem(s + 1, sp_count)
        return [
            remote(dst.at[back] if back else src, dst.at[back + 1], kv_ss.at[i], kv_rs.at[i, back], sp=right)
            for i, (src, dst) in enumerate(pairs)
        ]

    def arrived(back):
        pairs = ((k1_ref, k1b), (k2_ref, k2b), (v_ref, vb))
        left = lax.rem(s + sp_count - 1, sp_count)
        return [
            remote(src, dst.at[back], kv_ss.at[i], kv_rs.at[i, back - 1], sp=left)
            for i, (src, dst) in enumerate(pairs)
        ]

    def piece_bounds(target):
        short = target == last
        begin = hidden_all - cols + extra if short else target * cols
        return (begin, extra, cols - extra) if short else (begin, 0, cols)

    def part_rows(kind, target, part, side):
        _, _, size = piece_bounds(target)
        whole = half_d if kind < 2 else size // 2
        rows_here = whole // PARTS
        return pl.multiple_of(side * whole + part * rows_here, 16), rows_here

    def own_piece(kind, target, part):
        src = (gate_ref, up_ref, down_ref)[kind]
        begin, _, size = piece_bounds(target)
        first, count = part_rows(kind, target, part, y)
        if kind < 2:
            return src.at[pl.ds(first, count), pl.ds(begin, size)]
        return src.at[pl.ds(pl.multiple_of(begin + first, 16), count), :]

    def final_place(kind, source, target, part, side):
        dst = (wg, wu, wd)[kind]
        _, skip, size = piece_bounds(target)
        first, count = part_rows(kind, target, part, side)
        if kind < 2:
            return dst.at[source, pl.ds(first, count), pl.ds(skip, size)]
        return dst.at[source, pl.ds(pl.multiple_of(skip + first, 16), count)]

    def transit_place(kind, here, source, target, part):
        buffer = (tg, tu, td)[kind].at[transit_slot(here, source, target)]
        _, _, size = piece_bounds(target)
        first, count = part_rows(kind, target, part, 0)
        return buffer.at[pl.ds(first, count), pl.ds(0, size)] if kind < 2 else buffer.at[pl.ds(first, count)]

    def weight_hop(kind, here, source, target, part):
        there = here + 1 if target > here else here - 1
        if source == here:
            piece, ssem = own_piece(kind, target, part), w_ss.at[kind // 2]
        else:
            piece = transit_place(kind, here, source, target, part)
            ssem = t_ss.at[kind // 2]
        if there == target:
            place, rsem = final_place(kind, source, target, part, y), w_rs.at[kind, PARTS * source + part]
        else:
            place = transit_place(kind, there, source, target, part)
            rsem = t_rs.at[kind, PARTS * transit_slot(there, source, target) + part]
        return remote(piece, place, ssem, rsem, sp=there)

    def move_weights(kinds, here, source, target):
        for kind in kinds:
            for part in range(PARTS):
                if source != here:
                    before = here - 1 if source < here else here + 1
                    with scoped(f"pass{kind}{part}_{source}{target}"):
                        weight_hop(kind, before, source, target, part).wait_recv()
                weight_hop(kind, here, source, target, part).start()

    def weight_hand(kind, source, target, part):
        place = final_place(kind, source, target, part, y)
        return remote(place, place, f_ss.at[kind // 2], f_rs.at[kind, PARTS * source + part], grp=1 - y)

    def hand_over(kinds, here, source):
        for kind in kinds:
            for part in range(PARTS):
                before = here - 1 if source < here else here + 1
                with scoped(f"hand{kind}{part}_{source}"):
                    weight_hop(kind, before, source, here, part).wait_recv()
                weight_hand(kind, source, here, part).start()

    def own_copy(kind, short):
        src, dst = ((gate_ref, wg), (up_ref, wu), (down_ref, wd))[kind]
        begin = hidden_all - cols + extra if short else pl.multiple_of(s * cols, 128)
        skip, size = (extra, cols - extra) if short else (0, cols)
        if kind < 2:
            return pltpu.make_async_copy(src.at[:, pl.ds(begin, size)], dst.at[s, :, pl.ds(skip, size)], own_sem.at[kind])
        return pltpu.make_async_copy(src.at[pl.ds(begin, size), :], dst.at[s, pl.ds(skip, size)], own_sem.at[kind])

    def act_z(row, begin, target, way):
        piece = act.at[t, row]
        return remote(piece, piece, az_ss.at[way], az_rs.at[row], sp=target)

    def along(here, row, action):
        if row <= here < last:
            action(act_z(row, here, here + 1, 0))
        if row >= here > 0:
            action(act_z(row, here, here - 1, 1))

    def act_x(row):
        piece = act.at[t, row]
        return remote(piece, piece, ax_ss.at[0], ax_rs.at[row], tp=xpeer)

    def act_c(row, second):
        piece = act.at[xpeer if second else t, row]
        return remote(piece, piece, ac_ss.at[0], ac_rs.at[second, row], tp=cpeer)

    def start(copy):
        copy.start()

    def perform(here, event):
        kind, index = event[:2]
        if kind == WEIGHTS_IN:
            move_weights((0, 1), here, index, event[2])
        elif kind == DOWN_IN:
            move_weights((2,), here, index, event[2])
        elif kind == HAND_IN:
            hand_over((0, 1), here, index)
        elif kind == HAND_DOWN:
            hand_over((2,), here, index)
        elif kind == ROW:
            with scoped(f"row{index}"):
                act_z(index, here, here, 0).wait_recv()
            send_row(here, index)
        elif kind == ACROSS:
            with scoped(f"across{index}"):
                act_x(index).wait_recv()
            act_c(index, 1).start()

    def send_row(here, row):
        along(here, row, start)
        act_x(row).start()
        act_c(row, 0).start()

    x = t // 2
    steps = iter(PLAN)

    def next_step():
        plan = next(steps)
        for here in everyone:
            lists = [plan.get((here, side), ()) for side in range(2)]
            tests = [(s == here, lists[0])]
            if lists[0] != lists[1]:
                tests = [(jnp.logical_and(s == here, x == side), lists[side]) for side in range(2)]
            for test, events in tests:
                if events:

                    @pl.when(test)
                    def _(here=here, events=events):
                        for event in events:
                            perform(here, event)

    next_step()

    @pl.when(s < last)
    def _():
        for copy in kv_copies(0):
            copy.start()

    @pl.when(s == last)
    def _():
        wg[:, :, :extra] = jnp.zeros((sp_count, wg.shape[1], extra), jnp.bfloat16)
        wu[:, :, :extra] = jnp.zeros((sp_count, wg.shape[1], extra), jnp.bfloat16)
        wd[:, :extra, :] = jnp.zeros((sp_count, extra, blk), jnp.bfloat16)

    proj_copy = pltpu.make_async_copy(proj_hbm, proj_ref, own_sem.at[3])
    proj_copy.start()

    def start_own(short):
        for kind in range(3):
            own_copy(kind, short).start()

    either(s == last, start_own)

    gains[t] = jnp.broadcast_to(gain_ref[...].reshape(1, blk), gains.shape[1:])
    gain_copies = []
    for k in others:
        copy = remote(gains.at[t], gains.at[t], g_ss.at[0], g_rs.at[k - 1], tp=flip(t, k))
        copy.start()
        gain_copies.append(copy)

    q_refs = (q1_ref, q2_ref)
    lane = lax.broadcasted_iota(jnp.int32, (1, 2 * widths[0]), 1)

    def block(keys, v, diagonal):
        for group in range(2):
            width = widths[group]
            values = v[:, group, :]
            for m in range(2):
                if width % 128:
                    span = slice(0, 2 * width)
                    queries = q_refs[group][:, span]
                    queries = jnp.where(lane // width == m, queries.astype(jnp.float32), 0.0).astype(jnp.bfloat16)
                else:
                    span = slice(m * width, (m + 1) * width)
                    queries = q_refs[group][:, span]
                scores = nt_dot(queries, keys[group][:, span]) * width ** (-0.5)
                state = 2 * group + m
                if diagonal:
                    allowed = lax.broadcasted_iota(jnp.int32, (rows, rows), 1) <= lax.broadcasted_iota(
                        jnp.int32, (rows, rows), 0
                    )
                    scores = jnp.where(allowed, scores, -1e30)
                    top = jnp.max(scores, axis=1, keepdims=True)
                    weights = jnp.exp(scores - top)
                    peak[state] = top
                    total[state] = jnp.sum(weights, axis=1, keepdims=True)
                    acc[state] = dot(weights.astype(jnp.bfloat16), values)
                else:
                    before = peak[state]
                    top = jnp.maximum(before, jnp.max(scores, axis=1, keepdims=True))
                    fade = jnp.exp(before - top)
                    weights = jnp.exp(scores - top)
                    peak[state] = top
                    total[state] = total[state] * fade + jnp.sum(weights, axis=1, keepdims=True)
                    acc[state] = acc[state] * fade + dot(weights.astype(jnp.bfloat16), values)

    with scoped("diag"):
        block((k1_ref, k2_ref), v_ref, True)
    for back in others:

        @pl.when(s >= back)
        def _(back=back):
            with scoped(f"kvwait{back}"):
                for i, copy in enumerate(arrived(back)):
                    copy.wait_recv()
                    if back < last:
                        pl.when(s < last)(kv_copies(back)[i].start)
            with scoped(f"block{back}"):
                block((k1b.at[back], k2b.at[back]), vb.at[back], False)

    next_step()
    proj_copy.wait()
    with scoped("finish"):
        attended = []
        for group in range(2):
            first = acc[2 * group] / total[2 * group]
            second = acc[2 * group + 1] / total[2 * group + 1]
            differ = first - lam_ref[0, group] * second
            scale = lax.rsqrt(jnp.mean(differ * differ, axis=1, keepdims=True) + 1e-06)
            attended.append((0.8 * differ * scale).astype(jnp.bfloat16))

    def project(owner):
        columns = pl.ds(pl.multiple_of(owner * blk, blk), blk)
        return dot(attended[0], proj_ref[0, :, columns]) + dot(attended[1], proj_ref[1, :, columns])

    with scoped("project"):
        mp[0] = project(cpeer).astype(jnp.bfloat16)
        mp[1] = project(dpeer).astype(jnp.bfloat16)
        to_core = remote(mp.at[pl.ds(0, 2)], rsb.at[pl.ds(0, 2)], rs_ss.at[0], rs_rs.at[0], tp=cpeer)
        to_core.start()
        to_x = remote(mp.at[2], rsb.at[2], rs_ss.at[0], rs_rs.at[1], tp=xpeer)
        mine_ref[1] = project(xpeer)
        mine_ref[0] = residual_ref[...].astype(jnp.float32) + project(t)
    next_step()
    with scoped("rscore"):
        to_core.wait_recv()
    mp[2] = (mine_ref[1] + rsb[1].astype(jnp.float32)).astype(jnp.bfloat16)
    to_x.start()
    mine_ref[0] = mine_ref[0] + rsb[0].astype(jnp.float32)
    next_step()
    with scoped("rsx"):
        to_x.wait_recv()
    stream[...] = mine_ref[0] + rsb[2].astype(jnp.float32)
    act[t, s] = stream[...].astype(jnp.bfloat16)

    for here in everyone:

        @pl.when(s == here)
        def _(here=here):
            send_row(here, here)

    next_step()

    for copy in gain_copies:
        copy.wait_recv()

    def await_weights(kinds, source):
        def go(short):
            for kind in kinds:

                @pl.when(source != s)
                def _(kind=kind):
                    for part in range(PARTS):
                        place = final_place(kind, source, last if short else 0, part, 1 - y)
                        sem = PARTS * source + part
                        remote(place, place, f_ss.at[kind // 2], f_rs.at[kind, sem], grp=1 - y).wait_recv()

                @pl.when(source == s)
                def _(kind=kind):
                    own_copy(kind, short).wait()

        either(s == last, go)

    with scoped("await_gu"):
        for source in everyone:
            await_weights((0, 1), source)
    column = jnp.minimum(s * cols, hidden_all - cols) + lax.broadcasted_iota(jnp.int32, (1, cols), 1)
    mine = column >= s * cols

    def hidden_of(k):
        row = flip(s, k)
        next_step()
        with scoped(f"acwait{k}"):
            act_c(row, 0).wait_recv()
            act_c(row, 1).wait_recv()
        with scoped(f"hidden{k}"):
            squares = jnp.zeros((rows, 1), jnp.float32)
            for part in range(sp_count):
                piece = act[part, row].astype(jnp.float32)
                squares = squares + jnp.sum(piece * piece, axis=1, keepdims=True)
            scale = lax.rsqrt(squares / (sp_count * blk) + 1e-06)
            gate = jnp.zeros((rows, cols), jnp.float32)
            up = jnp.zeros((rows, cols), jnp.float32)
            for part in range(sp_count):
                gain = gains[part, 0:1, :].astype(jnp.float32)
                normed = (act[part, row].astype(jnp.float32) * scale * gain).astype(jnp.bfloat16)
                gate = gate + dot(normed, wg[part])
                up = up + dot(normed, wu[part])
            hidden = gate / (1.0 + jnp.exp(-gate)) * up
            hid[k] = jnp.where(mine, hidden, 0.0).astype(jnp.bfloat16)

    r1a, r1b, r2, r3 = {}, {}, {}, {}
    half_rows = rows // 2
    for k in everyone:
        r1a[k] = remote(c1.at[k, 1], c1r.at[k, 1], c_ss.at[0], c_rs.at[0, k], tp=cpeer)
        r1b[k] = remote(c1.at[k, 0], c1r.at[k, 0], c_ss.at[0], c_rs.at[1, k], tp=cpeer)
        for h in range(2):
            some = pl.ds(h * half_rows, half_rows)
            r2[k, h] = remote(c2.at[k, some], c2r.at[k, some], c_ss.at[1], c_rs.at[2 + h, k], tp=xpeer)
            if k:
                target = flip(s, 1 if k == 3 else k)
                r3[k, h] = remote(c3.at[k, some], c3r.at[k, some], c_ss.at[2], c_rs.at[4 + h, k], sp=target)

    def cross(k):
        next_step()
        with scoped(f"cross{k}"):
            c1[k, 1] = dot(hid[k], wd[dpeer]).astype(jnp.bfloat16)
            r1a[k].start()
            po[k, 1] = dot(hid[k], wd[xpeer])

    def to_other_chip(k):
        next_step()
        with scoped(f"r1a{k}"):
            r1a[k].wait_recv()
        for h in range(2):
            some = pl.ds(h * half_rows, half_rows)
            c2[k, some] = (po[k, 1, some] + c1r[k, 1, some].astype(jnp.float32)).astype(jnp.bfloat16)
            r2[k, h].start()

    def near(k):
        next_step()
        with scoped(f"near{k}"):
            c1[k, 0] = dot(hid[k], wd[cpeer]).astype(jnp.bfloat16)
            r1b[k].start()
            po[k, 0] = dot(hid[k], wd[t])

    def finish_row(k, h):
        next_step()
        some = pl.ds(h * half_rows, half_rows)
        if h == 0:
            with scoped(f"r1b{k}"):
                r1b[k].wait_recv()
        with scoped(f"r2_{k}{h}"):
            r2[k, h].wait_recv()
        result = po[k, 0, some] + c1r[k, 0, some].astype(jnp.float32) + c2r[k, some].astype(jnp.float32)
        if k == 2:
            with scoped(f"r3_3{h}"):
                r3[3, h].wait_recv()
            result = result + c3r[3, some].astype(jnp.float32)
        if k:
            c3[k, some] = result.astype(jnp.bfloat16)
            r3[k, h].start()
        else:
            po[0, 0, some] = result

    hidden_of(3)
    next_step()
    with scoped("await_cross"):
        await_weights((2,), dpeer)
        await_weights((2,), xpeer)
    cross(3)
    hidden_of(2)
    to_other_chip(3)
    cross(2)
    hidden_of(1)
    to_other_chip(2)
    cross(1)
    next_step()
    with scoped("await_near"):
        await_weights((2,), cpeer)
        await_weights((2,), t)
    near(3)
    hidden_of(0)
    to_other_chip(1)
    finish_row(3, 0)
    cross(0)
    finish_row(3, 1)
    to_other_chip(0)
    near(2)
    finish_row(2, 0)
    finish_row(2, 1)
    near(1)
    near(0)
    finish_row(1, 0)
    finish_row(1, 1)
    finish_row(0, 0)
    finish_row(0, 1)

    next_step()
    for h in range(2):
        some = pl.ds(h * half_rows, half_rows)
        for k in (1, 2):
            with scoped(f"r3_{k}{h}"):
                r3[k, h].wait_recv()
        ffn = po[0, 0, some] + c3r[1, some].astype(jnp.float32) + c3r[2, some].astype(jnp.float32)
        out_ref[some, :] = (stream[some, :] + 0.5 * ffn).astype(jnp.bfloat16)

    def sent(ref, sem):
        remote(ref, ref, sem, rs_rs.at[0], tp=cpeer).wait_send()

    def weights_sent(sems, width):
        sent(gate_ref.at[:, pl.ds(0, width)], sems.at[0])
        sent(down_ref.at[pl.ds(0, width // 2), :], sems.at[1])

    def width_of(target):
        return piece_bounds(target)[2]

    with scoped("drain"):
        for here in everyone:

            @pl.when(s == here)
            def _(here=here):
                if here < last:
                    for i, buffer in enumerate((k1b, k2b, vb)):
                        sent(buffer.at[pl.ds(0, here + 1)], kv_ss.at[i])
                    sent(act.at[0, pl.ds(0, here + 1)], az_ss.at[0])
                if here:
                    sent(act.at[0, pl.ds(0, sp_count - here)], az_ss.at[1])
                weights_sent(w_ss, sum(width_of(there) for there in everyone if there != here))
                weights_sent(f_ss, (sp_count - 1) * width_of(here))
                through = [
                    width_of(target)
                    for source in everyone
                    for target in everyone
                    if min(source, target) < here < max(source, target)
                ]
                if through:
                    weights_sent(t_ss, sum(through))

        sent(act.at[0], ax_ss.at[0])
        sent(act.at[pl.ds(0, 2)], ac_ss.at[0])
        sent(gains.at[pl.ds(0, sp_count - 1)], g_ss.at[0])
        sent(mp, rs_ss.at[0])
        sent(c1, c_ss.at[0])
        sent(c2, c_ss.at[1])
        sent(c3.at[pl.ds(0, sp_count - 1)], c_ss.at[2])


def fits(axes, query_first, values, lambdas, residual, gate_weight):
    sp, tp = axes["sp"], axes["tp"]
    rows, blk = residual.shape
    depth, hidden_all = gate_weight.shape
    if axes["grp"] != 2 or sp != tp or tp != 4 or lambdas.shape[1] != 1:
        return False
    if depth != blk or blk % 128 or hidden_all % 128 or rows % 16:
        return False
    if (2 * query_first.shape[1]) % 256 or values.shape[2] % 128:
        return False
    cols = -(-hidden_all // (128 * sp)) * 128
    if cols * sp - hidden_all >= cols or cols > hidden_all:
        return False
    if (cols * sp - hidden_all) % 128 or blk % 64 or rows % 32:
        return False
    need = 6 * sp * blk * cols + rows * blk * 2 * 20 * sp
    return need < 40 * 1024 * 1024


def one_device(
    axes,
    query_first,
    key_first,
    query_second,
    key_second,
    values,
    lambdas,
    residual,
    norm_gain,
    out_weight,
    gate_weight,
    up_weight,
    down_weight,
):
    if not fits(axes, query_first, values, lambdas, residual, gate_weight):
        return per_device(
            query_first,
            key_first,
            query_second,
            key_second,
            values,
            lambdas,
            residual,
            norm_gain,
            out_weight,
            gate_weight,
            up_weight,
            down_weight,
        )
    n = axes["sp"]
    rows, blk = residual.shape
    hidden_all = gate_weight.shape[1]
    cols = -(-hidden_all // (128 * n)) * 128
    value_size = values.shape[2]
    widths = (query_first.shape[1] // 2, query_second.shape[1] // 2)
    bf16, f32 = jnp.bfloat16, jnp.float32
    vmem = pl.BlockSpec(memory_space=pltpu.VMEM)
    smem = pl.BlockSpec(memory_space=pltpu.SMEM)
    hbm = pl.BlockSpec(memory_space=pl.ANY)
    dma = pltpu.SemaphoreType.DMA
    return pl.pallas_call(
        functools.partial(layer_kernel, n, widths),
        out_shape=jax.ShapeDtypeStruct((rows, blk), bf16),
        in_specs=[vmem] * 5 + [smem, vmem, vmem] + [hbm] * 4,
        out_specs=vmem,
        scratch_shapes=[
            pltpu.VMEM((n,) + key_first.shape, bf16),
            pltpu.VMEM((n,) + key_second.shape, bf16),
            pltpu.VMEM((n,) + values.shape, bf16),
            pltpu.VMEM(out_weight.shape, bf16),
            pltpu.VMEM((4, rows, 1), f32),
            pltpu.VMEM((4, rows, 1), f32),
            pltpu.VMEM((4, rows, value_size), f32),
            pltpu.VMEM((n, blk, cols), bf16),
            pltpu.VMEM((n, blk, cols), bf16),
            pltpu.VMEM((n, cols, blk), bf16),
            pltpu.VMEM((4, blk // 2, cols), bf16),
            pltpu.VMEM((4, blk // 2, cols), bf16),
            pltpu.VMEM((4, cols // 2, blk), bf16),
            pltpu.VMEM((3, rows, blk), bf16),
            pltpu.VMEM((3, rows, blk), bf16),
            pltpu.VMEM((2, rows, blk), f32),
            pltpu.VMEM((rows, blk), f32),
            pltpu.VMEM((n, n, rows, blk), bf16),
            pltpu.VMEM((n, 16, blk), bf16),
            pltpu.VMEM((n, rows, cols), bf16),
            pltpu.VMEM((n, 2, rows, blk), bf16),
            pltpu.VMEM((n, 2, rows, blk), bf16),
            pltpu.VMEM((n, 2, rows, blk), f32),
            pltpu.VMEM((n, rows, blk), bf16),
            pltpu.VMEM((n, rows, blk), bf16),
            pltpu.VMEM((n, rows, blk), bf16),
            pltpu.VMEM((n, rows, blk), bf16),
            dma((3,)),
            dma((3, n - 1)),
            dma((2,)),
            dma((3, PARTS * n)),
            dma((2,)),
            dma((3, PARTS * n)),
            dma((2,)),
            dma((3, PARTS * n)),
            dma((4,)),
            dma((1,)),
            dma((n - 1,)),
            dma((1,)),
            dma((2,)),
            dma((2,)),
            dma((n,)),
            dma((1,)),
            dma((n,)),
            dma((1,)),
            dma((2, n)),
            dma((3,)),
            dma((6, n)),
        ],
        compiler_params=pltpu.CompilerParams(
            collective_id=0, has_side_effects=True, vmem_limit_bytes=60 * 1024 * 1024
        ),
    )(
        query_first,
        query_second,
        key_first,
        key_second,
        values,
        lambdas.T,
        residual,
        norm_gain,
        out_weight,
        gate_weight,
        up_weight,
        down_weight,
    )

def solution(mesh):
    return jax.shard_map(
        functools.partial(one_device, dict(mesh.shape)),
        mesh=mesh,
        in_specs=(
            P(("grp", "sp"), "tp"),
            P(("grp", "sp"), "tp"),
            P(("grp", "sp"), "tp"),
            P(("grp", "sp"), "tp"),
            P(("grp", "sp"), None, "tp"),
            P(None, "tp"),
            P(("grp", "sp"), "tp"),
            P("tp"),
            P(None, "tp", None),
            P("sp", "tp"),
            P("sp", "tp"),
            P("tp", "sp"),
        ),
        out_specs=P(("grp", "sp"), "tp"),
        check_vma=False,
    )
```

```python
import functools

import jax
import jax.numpy as jnp
from jax import lax
from jax.experimental import pallas as pl
from jax.experimental.pallas import tpu as pltpu
from jax.sharding import PartitionSpec as P

D = 2048


def per_device(
    query_first,
    key_first,
    query_second,
    key_second,
    values,
    lambdas,
    residual,
    norm_gain,
    out_weight,
    gate_weight,
    up_weight,
    down_weight,
):
    tok_rows = query_first.shape[0]
    heads_here = lambdas.shape[1]
    width_first = query_first.shape[1] // (2 * heads_here)
    width_second = query_second.shape[1] // (2 * heads_here)
    value_size = values.shape[2] // heads_here
    offset = lax.axis_index("sp") * tok_rows
    query_pos = offset + lax.broadcasted_iota(jnp.int32, (tok_rows, 1), 0)
    query_groups = (
        query_first.reshape(tok_rows, heads_here, 2, width_first),
        query_second.reshape(tok_rows, heads_here, 2, width_second),
    )
    key_widths = (width_first, width_second)
    start_state = (
        jnp.full((heads_here, 2, tok_rows, 1), -1e30, jnp.float32),
        jnp.zeros((heads_here, 2, tok_rows, 1), jnp.float32),
        jnp.zeros((heads_here, 2, tok_rows, value_size), jnp.float32),
    )
    states = (start_state, start_state)
    pieces = (
        lax.all_gather(key_first, "sp", axis=0, tiled=True),
        lax.all_gather(key_second, "sp", axis=0, tiled=True),
        lax.all_gather(values, "sp", axis=0, tiled=True),
    )
    piece_rows = pieces[0].shape[0]
    key_pos = lax.broadcasted_iota(jnp.int32, (1, piece_rows), 1)
    allowed = key_pos <= query_pos
    value_rows = pieces[2].reshape(piece_rows, 2, heads_here, value_size)
    results = []
    for group_idx in range(2):
        key_width = key_widths[group_idx]
        key_part = pieces[group_idx].reshape(piece_rows, heads_here, 2, key_width)
        scores = jnp.einsum(
            "qhmd,khmd->hmqk", query_groups[group_idx], key_part, preferred_element_type=jnp.float32
        ) * key_width ** (-0.5)
        scores = jnp.where(allowed, scores, -1e30)
        running, totals, weighted = states[group_idx]
        new_peak = jnp.maximum(running, jnp.max(scores, axis=-1, keepdims=True))
        weights = jnp.where(allowed, jnp.exp(scores - new_peak), 0.0)
        totals = jnp.sum(weights, axis=-1, keepdims=True)
        weighted = jnp.einsum(
            "hmqk,khe->hmqe",
            weights.astype(jnp.bfloat16),
            value_rows[:, group_idx],
            preferred_element_type=jnp.float32,
        )
        results.append((new_peak, totals, weighted))
    states = (results[0], results[1])
    map_out = jnp.stack([states[0][2] / states[0][1], states[1][2] / states[1][1]])
    differ = map_out[:, :, 0] - lambdas[:, :, None, None] * map_out[:, :, 1]
    head_scale = lax.rsqrt(jnp.mean(differ * differ, axis=-1, keepdims=True) + 1e-06)
    attended = (0.8 * differ * head_scale).astype(jnp.bfloat16)
    projection = out_weight.reshape(2, heads_here, value_size, out_weight.shape[2])
    mixed_part = jnp.einsum(
        "ghqe,gher->qr", attended, projection, preferred_element_type=jnp.float32
    )
    mixed = lax.psum_scatter(
        mixed_part.astype(jnp.bfloat16), "tp", scatter_dimension=1, tiled=True
    ).astype(jnp.float32)
    stream = residual.astype(jnp.float32) + mixed
    squares = lax.psum(jnp.sum(stream * stream, axis=1), "tp")
    row_scale = lax.rsqrt(squares[:, None] / D + 1e-06)
    normed = (stream * row_scale * norm_gain.astype(jnp.float32)).astype(jnp.bfloat16)
    full_rows = lax.all_gather(normed, "tp", axis=1, tiled=True)
    pieces = (
        lax.all_gather(gate_weight, "sp", axis=0, tiled=True),
        lax.all_gather(up_weight, "sp", axis=0, tiled=True),
    )
    gate = jnp.dot(full_rows, pieces[0], preferred_element_type=jnp.float32)
    up_part = jnp.dot(full_rows, pieces[1], preferred_element_type=jnp.float32)
    hidden = (jax.nn.silu(gate) * up_part).astype(jnp.bfloat16)
    partial_out = jnp.dot(
        hidden,
        lax.all_gather(down_weight, "sp", axis=1, tiled=True),
        preferred_element_type=jnp.float32,
    )
    ffn = lax.psum_scatter(
        partial_out.astype(jnp.bfloat16), "tp", scatter_dimension=1, tiled=True
    ).astype(jnp.float32)
    return (stream + 0.5 * ffn).astype(jnp.bfloat16)


def flip(index, bits):
    bit = 1
    while bit <= bits:
        if (bits // bit) % 2:
            index = index + bit - 2 * bit * ((index // bit) % 2)
        bit *= 2
    return index


def nt_dot(a, b):
    return lax.dot_general(a, b, (((1,), (1,)), ((), ())), preferred_element_type=jnp.float32)


def dot(a, b):
    return jnp.dot(a, b, preferred_element_type=jnp.float32)


def scoped(name):
    return jax.named_scope(name)


PLAN = (
    {
        (1, 0): ((0, 1, 0),),
        (1, 1): ((1, 1, 3), (0, 1, 0)),
        (2, 0): ((0, 2, 0), (1, 2, 1), (1, 2, 3), (1, 2, 0)),
        (2, 1): ((0, 2, 3), (1, 2, 1), (0, 2, 0), (1, 2, 0)),
        (3, 0): ((1, 3, 0), (0, 3, 0), (0, 3, 1), (0, 3, 2), (1, 3, 2)),
        (3, 1): ((0, 3, 0), (1, 3, 0), (0, 3, 2), (1, 3, 1)),
    },
    {
        (0, 0): ((0, 0, 2),),
        (0, 1): ((0, 0, 1),),
        (1, 0): ((0, 1, 3),),
        (2, 0): ((0, 2, 1),),
        (2, 1): ((0, 3, 0), (1, 1, 3)),
    },
    {
        (1, 1): ((0, 1, 2), (0, 2, 0)),
        (2, 0): ((1, 3, 0),),
        (2, 1): ((0, 2, 1), (2, 3)),
        (3, 1): ((0, 3, 1),),
    },
    {
        (0, 0): ((1, 0, 3),),
        (0, 1): ((2, 1),),
        (1, 0): ((0, 1, 2), (0, 2, 0)),
        (1, 1): ((1, 2, 0), (3, 2), (0, 1, 3)),
        (2, 0): ((0, 1, 3), (0, 2, 3), (0, 3, 0), (2, 3)),
    },
    {
        (0, 0): ((2, 1), (0, 0, 3), (2, 2), (4, 1), (0, 0, 1), (3, 3), (1, 0, 2), (5, 1), (1, 0, 1), (2, 3), (4, 2), (4, 3), (3, 2), (5, 0), (3, 1), (5, 2), (5, 3)),
        (0, 1): ((0, 0, 2), (5, 0), (1, 0, 3), (1, 0, 1), (4, 1), (5, 1), (0, 0, 3), (2, 2), (1, 0, 2), (3, 2), (3, 1), (2, 3), (3, 3), (4, 2), (4, 3), (5, 2), (5, 3)),
        (1, 0): ((4, 0), (1, 1, 0), (0, 0, 3), (3, 2), (1, 3, 0), (0, 0, 2), (2, 2), (1, 0, 3), (0, 3, 0), (2, 0), (4, 2), (4, 3), (1, 0, 2), (1, 2, 0), (1, 1, 3), (1, 1, 2), (2, 3), (5, 1), (3, 3), (3, 0), (5, 2), (5, 3), (5, 0)),
        (1, 1): ((4, 0), (1, 1, 0), (0, 0, 2), (2, 0), (0, 3, 0), (5, 1), (1, 1, 2), (4, 2), (2, 2), (0, 0, 3), (3, 0), (1, 3, 0), (4, 3), (5, 0), (1, 0, 3), (1, 0, 2), (2, 3), (5, 2), (3, 3), (5, 3)),
        (2, 0): ((2, 1), (4, 0), (4, 3), (5, 0), (0, 0, 3), (3, 3), (0, 3, 1), (5, 2), (4, 1), (2, 0), (1, 3, 1), (5, 3), (3, 0), (1, 0, 3), (5, 1)),
        (2, 1): ((1, 3, 0), (4, 1), (2, 1), (4, 0), (4, 3), (1, 2, 3), (2, 0), (0, 3, 1), (0, 1, 3), (1, 3, 1), (5, 0), (3, 3), (3, 1), (5, 2), (5, 3), (0, 0, 3)),
        (3, 0): ((1, 3, 1), (2, 2), (3, 2), (4, 2), (4, 0), (2, 1), (2, 0), (4, 1), (5, 0), (3, 0)),
        (3, 1): ((1, 3, 2), (4, 2), (3, 1), (2, 2), (4, 0), (4, 1), (3, 2), (2, 1), (5, 0), (5, 2), (2, 0), (3, 0), (5, 3), (5, 1)),
    },
    {
        (2, 1): ((1, 0, 3), (5, 1), (3, 0)),
    },
    {
        (3, 0): ((5, 1), (3, 1)),
    },
    {
        (3, 0): ((5, 3), (5, 2)),
    },
    {
        (2, 0): ((1, 1, 3),),
    },
    {},
    {},
    {},
    {
        (2, 0): ((3, 1),),
    },
    {},
    {},
    {},
    {},
    {},
    {},
    {},
    {},
    {},
    {},
    {},
    {},
    {},
    {},
    {},
    {},
    {},
    {},
    {},
)

WEIGHTS_IN, DOWN_IN, HAND_IN, HAND_DOWN, ROW, ACROSS = range(6)


PARTS = 2


def transit_slot(here, source, target):
    outer = 0 if source < here else 2
    if outer:
        return outer + (target if here == 2 else source - 2)
    return outer + (target - 2 if here == 1 else source)


def layer_kernel(
    sp_count,
    widths,
    q1_hbm,
    q2_hbm,
    k1_hbm,
    k2_hbm,
    v_hbm,
    lam_hbm,
    residual_hbm,
    gain_hbm,
    proj_hbm,
    gate_ref,
    up_ref,
    down_ref,
    out_ref,
    q1_ref,
    q2_ref,
    k1_ref,
    k2_ref,
    v_ref,
    lam_ref,
    residual_ref,
    gain_ref,
    k1b,
    k2b,
    vb,
    proj_ref,
    peak,
    total,
    acc,
    wg,
    wu,
    wd,
    tg,
    tu,
    td,
    mp,
    rsb,
    mine_ref,
    stream,
    act,
    gains,
    hid,
    c1,
    c1r,
    po,
    c2,
    c2r,
    c3,
    c3r,
    kv_ss,
    kv_rs,
    w_ss,
    w_rs,
    t_ss,
    t_rs,
    f_ss,
    f_rs,
    own_sem,
    in_sem,
    g_ss,
    g_rs,
    rs_ss,
    rs_rs,
    az_ss,
    az_rs,
    ax_ss,
    ax_rs,
    ac_ss,
    ac_rs,
    c_ss,
    c_rs,
):
    s = lax.axis_index("sp")
    t = lax.axis_index("tp")
    y = lax.axis_index("grp")
    rows, blk = residual_ref.shape
    cols = wg.shape[2]
    hidden_all = gate_ref.shape[1]
    xpeer, cpeer, dpeer = flip(t, 2), flip(t, 1), flip(t, 3)
    others = range(1, sp_count)
    everyone = range(sp_count)
    last = sp_count - 1

    def remote(src, dst, ssem, rsem, **where):
        return pltpu.make_async_remote_copy(
            src_ref=src,
            dst_ref=dst,
            send_sem=ssem,
            recv_sem=rsem,
            device_id=where,
            device_id_type=pl.DeviceIdType.MESH,
        )

    def either(test, action):
        pl.when(test)(lambda: action(True))
        pl.when(jnp.logical_not(test))(lambda: action(False))

    barrier = pltpu.get_barrier_semaphore()
    for k in others:
        pl.semaphore_signal(barrier, inc=1, device_id={"sp": flip(s, k)}, device_id_type=pl.DeviceIdType.MESH)
        pl.semaphore_signal(barrier, inc=1, device_id={"tp": flip(t, k)}, device_id_type=pl.DeviceIdType.MESH)
    pl.semaphore_signal(barrier, inc=1, device_id={"grp": 1 - y}, device_id_type=pl.DeviceIdType.MESH)
    inputs = (
        (k1_hbm, k1_ref),
        (k2_hbm, k2_ref),
        (v_hbm, v_ref),
        (q1_hbm, q1_ref),
        (q2_hbm, q2_ref),
        (gain_hbm, gain_ref),
        (lam_hbm, lam_ref),
        (residual_hbm, residual_ref),
    )
    loads = [pltpu.make_async_copy(far, here, in_sem.at[i]) for i, (far, here) in enumerate(inputs)]
    for load in loads:
        load.start()

    half_d = wg.shape[1] // 2
    extra = sp_count * cols - hidden_all
    d_half = pl.ds(pl.multiple_of(y * half_d, half_d), half_d)

    def kv_copies(back):
        pairs = ((k1_ref, k1b), (k2_ref, k2b), (v_ref, vb))
        right = lax.rem(s + 1, sp_count)
        return [
            remote(dst.at[back] if back else src, dst.at[back + 1], kv_ss.at[i], kv_rs.at[i, back], sp=right)
            for i, (src, dst) in enumerate(pairs)
        ]

    def arrived(back):
        pairs = ((k1_ref, k1b), (k2_ref, k2b), (v_ref, vb))
        left = lax.rem(s + sp_count - 1, sp_count)
        return [
            remote(src, dst.at[back], kv_ss.at[i], kv_rs.at[i, back - 1], sp=left)
            for i, (src, dst) in enumerate(pairs)
        ]

    def piece_bounds(target):
        short = target == last
        begin = hidden_all - cols + extra if short else target * cols
        return (begin, extra, cols - extra) if short else (begin, 0, cols)

    def part_rows(kind, target, part, side):
        _, _, size = piece_bounds(target)
        whole = half_d if kind < 2 else size // 2
        rows_here = whole // PARTS
        return pl.multiple_of(side * whole + part * rows_here, 16), rows_here

    def own_piece(kind, target, part):
        src = (gate_ref, up_ref, down_ref)[kind]
        begin, _, size = piece_bounds(target)
        first, count = part_rows(kind, target, part, y)
        if kind < 2:
            return src.at[pl.ds(first, count), pl.ds(begin, size)]
        return src.at[pl.ds(pl.multiple_of(begin + first, 16), count), :]

    def final_place(kind, source, target, part, side):
        dst = (wg, wu, wd)[kind]
        _, skip, size = piece_bounds(target)
        first, count = part_rows(kind, target, part, side)
        if kind < 2:
            return dst.at[source, pl.ds(first, count), pl.ds(skip, size)]
        return dst.at[source, pl.ds(pl.multiple_of(skip + first, 16), count)]

    def transit_place(kind, here, source, target, part):
        buffer = (tg, tu, td)[kind].at[transit_slot(here, source, target)]
        _, _, size = piece_bounds(target)
        first, count = part_rows(kind, target, part, 0)
        return buffer.at[pl.ds(first, count), pl.ds(0, size)] if kind < 2 else buffer.at[pl.ds(first, count)]

    def weight_hop(kind, here, source, target, part):
        there = here + 1 if target > here else here - 1
        if source == here:
            piece, ssem = own_piece(kind, target, part), w_ss.at[kind // 2]
        else:
            piece = transit_place(kind, here, source, target, part)
            ssem = t_ss.at[kind // 2]
        if there == target:
            place, rsem = final_place(kind, source, target, part, y), w_rs.at[kind, PARTS * source + part]
        else:
            place = transit_place(kind, there, source, target, part)
            rsem = t_rs.at[kind, PARTS * transit_slot(there, source, target) + part]
        return remote(piece, place, ssem, rsem, sp=there)

    def move_weights(kinds, here, source, target):
        for kind in kinds:
            for part in range(PARTS):
                if source != here:
                    before = here - 1 if source < here else here + 1
                    with scoped(f"pass{kind}{part}_{source}{target}"):
                        weight_hop(kind, before, source, target, part).wait_recv()
                weight_hop(kind, here, source, target, part).start()

    def weight_hand(kind, source, target, part):
        place = final_place(kind, source, target, part, y)
        return remote(place, place, f_ss.at[kind // 2], f_rs.at[kind, PARTS * source + part], grp=1 - y)

    def hand_over(kinds, here, source):
        for kind in kinds:
            for part in range(PARTS):
                before = here - 1 if source < here else here + 1
                with scoped(f"hand{kind}{part}_{source}"):
                    weight_hop(kind, before, source, here, part).wait_recv()
                weight_hand(kind, source, here, part).start()

    def own_copy(kind, short):
        src, dst = ((gate_ref, wg), (up_ref, wu), (down_ref, wd))[kind]
        begin = hidden_all - cols + extra if short else pl.multiple_of(s * cols, 128)
        skip, size = (extra, cols - extra) if short else (0, cols)
        if kind < 2:
            return pltpu.make_async_copy(src.at[:, pl.ds(begin, size)], dst.at[s, :, pl.ds(skip, size)], own_sem.at[kind])
        return pltpu.make_async_copy(src.at[pl.ds(begin, size), :], dst.at[s, pl.ds(skip, size)], own_sem.at[kind])

    def act_z(row, begin, target, way):
        piece = act.at[t, row]
        return remote(piece, piece, az_ss.at[way], az_rs.at[row], sp=target)

    def along(here, row, action):
        if row <= here < last:
            action(act_z(row, here, here + 1, 0))
        if row >= here > 0:
            action(act_z(row, here, here - 1, 1))

    def act_x(row):
        piece = act.at[t, row]
        return remote(piece, piece, ax_ss.at[0], ax_rs.at[row], tp=xpeer)

    def act_c(row, second):
        piece = act.at[xpeer if second else t, row]
        return remote(piece, piece, ac_ss.at[0], ac_rs.at[second, row], tp=cpeer)

    def start(copy):
        copy.start()

    def perform(here, event):
        kind, index = event[:2]
        if kind == WEIGHTS_IN:
            move_weights((0, 1), here, index, event[2])
        elif kind == DOWN_IN:
            move_weights((2,), here, index, event[2])
        elif kind == HAND_IN:
            hand_over((0, 1), here, index)
        elif kind == HAND_DOWN:
            hand_over((2,), here, index)
        elif kind == ROW:
            with scoped(f"row{index}"):
                act_z(index, here, here, 0).wait_recv()
            send_row(here, index)
        elif kind == ACROSS:
            with scoped(f"across{index}"):
                act_x(index).wait_recv()
            act_c(index, 1).start()

    def send_row(here, row):
        along(here, row, start)
        act_x(row).start()
        act_c(row, 0).start()

    x = t // 2
    steps = iter(PLAN)

    def next_step():
        plan = next(steps)
        for here in everyone:
            lists = [plan.get((here, side), ()) for side in range(2)]
            tests = [(s == here, lists[0])]
            if lists[0] != lists[1]:
                tests = [(jnp.logical_and(s == here, x == side), lists[side]) for side in range(2)]
            for test, events in tests:
                if events:

                    @pl.when(test)
                    def _(here=here, events=events):
                        for event in events:
                            perform(here, event)

    @pl.when(s == last)
    def _():
        wg[:, :, :extra] = jnp.zeros((sp_count, wg.shape[1], extra), jnp.bfloat16)
        wu[:, :, :extra] = jnp.zeros((sp_count, wg.shape[1], extra), jnp.bfloat16)
        wd[:, :extra, :] = jnp.zeros((sp_count, extra, blk), jnp.bfloat16)

    proj_copy = pltpu.make_async_copy(proj_hbm, proj_ref, own_sem.at[3])
    proj_copy.start()

    def start_own(short):
        for kind in range(3):
            own_copy(kind, short).start()

    either(s == last, start_own)

    for load in loads[:-1]:
        load.wait()
    gains[t] = jnp.broadcast_to(gain_ref[...].reshape(1, blk), gains.shape[1:])
    with scoped("barrier"):
        pl.semaphore_wait(barrier, 2 * (sp_count - 1) + 1)
    next_step()

    @pl.when(s < last)
    def _():
        for copy in kv_copies(0):
            copy.start()

    gain_copies = []
    for k in others:
        copy = remote(gains.at[t], gains.at[t], g_ss.at[0], g_rs.at[k - 1], tp=flip(t, k))
        copy.start()
        gain_copies.append(copy)

    q_refs = (q1_ref, q2_ref)
    lane = lax.broadcasted_iota(jnp.int32, (1, 2 * widths[0]), 1)

    def block(keys, v, diagonal):
        for group in range(2):
            width = widths[group]
            values = v[:, group, :]
            for m in range(2):
                if width % 128:
                    span = slice(0, 2 * width)
                    queries = q_refs[group][:, span]
                    queries = jnp.where(lane // width == m, queries.astype(jnp.float32), 0.0).astype(jnp.bfloat16)
                else:
                    span = slice(m * width, (m + 1) * width)
                    queries = q_refs[group][:, span]
                scores = nt_dot(queries, keys[group][:, span]) * width ** (-0.5)
                state = 2 * group + m
                if diagonal:
                    allowed = lax.broadcasted_iota(jnp.int32, (rows, rows), 1) <= lax.broadcasted_iota(
                        jnp.int32, (rows, rows), 0
                    )
                    scores = jnp.where(allowed, scores, -1e30)
                    top = jnp.max(scores, axis=1, keepdims=True)
                    weights = jnp.exp(scores - top)
                    peak[state] = top
                    total[state] = jnp.sum(weights, axis=1, keepdims=True)
                    acc[state] = dot(weights.astype(jnp.bfloat16), values)
                else:
                    before = peak[state]
                    top = jnp.maximum(before, jnp.max(scores, axis=1, keepdims=True))
                    fade = jnp.exp(before - top)
                    weights = jnp.exp(scores - top)
                    peak[state] = top
                    total[state] = total[state] * fade + jnp.sum(weights, axis=1, keepdims=True)
                    acc[state] = acc[state] * fade + dot(weights.astype(jnp.bfloat16), values)

    with scoped("diag"):
        block((k1_ref, k2_ref), v_ref, True)
    for back in others:

        @pl.when(s >= back)
        def _(back=back):
            with scoped(f"kvwait{back}"):
                for i, copy in enumerate(arrived(back)):
                    copy.wait_recv()
                    if back < last:
                        pl.when(s < last)(kv_copies(back)[i].start)
            with scoped(f"block{back}"):
                block((k1b.at[back], k2b.at[back]), vb.at[back], False)

    next_step()
    proj_copy.wait()
    loads[-1].wait()
    with scoped("finish"):
        attended = []
        for group in range(2):
            first = acc[2 * group] / total[2 * group]
            second = acc[2 * group + 1] / total[2 * group + 1]
            differ = first - lam_ref[0, group] * second
            scale = lax.rsqrt(jnp.mean(differ * differ, axis=1, keepdims=True) + 1e-06)
            attended.append((0.8 * differ * scale).astype(jnp.bfloat16))

    def project(owner):
        columns = pl.ds(pl.multiple_of(owner * blk, blk), blk)
        return dot(attended[0], proj_ref[0, :, columns]) + dot(attended[1], proj_ref[1, :, columns])

    with scoped("project"):
        mp[0] = project(cpeer).astype(jnp.bfloat16)
        mp[1] = project(dpeer).astype(jnp.bfloat16)
        to_core = remote(mp.at[pl.ds(0, 2)], rsb.at[pl.ds(0, 2)], rs_ss.at[0], rs_rs.at[0], tp=cpeer)
        to_core.start()
        to_x = remote(mp.at[2], rsb.at[2], rs_ss.at[0], rs_rs.at[1], tp=xpeer)
        mine_ref[1] = project(xpeer)
        mine_ref[0] = residual_ref[...].astype(jnp.float32) + project(t)
    next_step()
    with scoped("rscore"):
        to_core.wait_recv()
    mp[2] = (mine_ref[1] + rsb[1].astype(jnp.float32)).astype(jnp.bfloat16)
    to_x.start()
    mine_ref[0] = mine_ref[0] + rsb[0].astype(jnp.float32)
    next_step()
    with scoped("rsx"):
        to_x.wait_recv()
    stream[...] = mine_ref[0] + rsb[2].astype(jnp.float32)
    act[t, s] = stream[...].astype(jnp.bfloat16)

    for here in everyone:

        @pl.when(s == here)
        def _(here=here):
            send_row(here, here)

    next_step()

    for copy in gain_copies:
        copy.wait_recv()

    def await_weights(kinds, source):
        def go(short):
            for kind in kinds:

                @pl.when(source != s)
                def _(kind=kind):
                    for part in range(PARTS):
                        place = final_place(kind, source, last if short else 0, part, 1 - y)
                        sem = PARTS * source + part
                        remote(place, place, f_ss.at[kind // 2], f_rs.at[kind, sem], grp=1 - y).wait_recv()

                @pl.when(source == s)
                def _(kind=kind):
                    own_copy(kind, short).wait()

        either(s == last, go)

    with scoped("await_gu"):
        for source in everyone:
            await_weights((0, 1), source)
    column = jnp.minimum(s * cols, hidden_all - cols) + lax.broadcasted_iota(jnp.int32, (1, cols), 1)
    mine = column >= s * cols

    def hidden_of(k):
        row = flip(s, k)
        next_step()
        with scoped(f"acwait{k}"):
            act_c(row, 0).wait_recv()
            act_c(row, 1).wait_recv()
        with scoped(f"hidden{k}"):
            squares = jnp.zeros((rows, 1), jnp.float32)
            for part in range(sp_count):
                piece = act[part, row].astype(jnp.float32)
                squares = squares + jnp.sum(piece * piece, axis=1, keepdims=True)
            scale = lax.rsqrt(squares / (sp_count * blk) + 1e-06)
            gate = jnp.zeros((rows, cols), jnp.float32)
            up = jnp.zeros((rows, cols), jnp.float32)
            for part in range(sp_count):
                gain = gains[part, 0:1, :].astype(jnp.float32)
                normed = (act[part, row].astype(jnp.float32) * scale * gain).astype(jnp.bfloat16)
                gate = gate + dot(normed, wg[part])
                up = up + dot(normed, wu[part])
            hidden = gate / (1.0 + jnp.exp(-gate)) * up
            hid[k] = jnp.where(mine, hidden, 0.0).astype(jnp.bfloat16)

    r1a, r1b, r2, r3 = {}, {}, {}, {}
    half_rows = rows // 2
    for k in everyone:
        r1a[k] = remote(c1.at[k, 1], c1r.at[k, 1], c_ss.at[0], c_rs.at[0, k], tp=cpeer)
        r1b[k] = remote(c1.at[k, 0], c1r.at[k, 0], c_ss.at[0], c_rs.at[1, k], tp=cpeer)
        for h in range(2):
            some = pl.ds(h * half_rows, half_rows)
            r2[k, h] = remote(c2.at[k, some], c2r.at[k, some], c_ss.at[1], c_rs.at[2 + h, k], tp=xpeer)
            if k:
                target = flip(s, 1 if k == 3 else k)
                r3[k, h] = remote(c3.at[k, some], c3r.at[k, some], c_ss.at[2], c_rs.at[4 + h, k], sp=target)

    def cross(k):
        next_step()
        with scoped(f"cross{k}"):
            c1[k, 1] = dot(hid[k], wd[dpeer]).astype(jnp.bfloat16)
            r1a[k].start()
            po[k, 1] = dot(hid[k], wd[xpeer])

    def to_other_chip(k):
        next_step()
        with scoped(f"r1a{k}"):
            r1a[k].wait_recv()
        for h in range(2):
            some = pl.ds(h * half_rows, half_rows)
            c2[k, some] = (po[k, 1, some] + c1r[k, 1, some].astype(jnp.float32)).astype(jnp.bfloat16)
            r2[k, h].start()

    def near(k):
        next_step()
        with scoped(f"near{k}"):
            c1[k, 0] = dot(hid[k], wd[cpeer]).astype(jnp.bfloat16)
            r1b[k].start()
            po[k, 0] = dot(hid[k], wd[t])

    def finish_row(k, h):
        next_step()
        some = pl.ds(h * half_rows, half_rows)
        if h == 0:
            with scoped(f"r1b{k}"):
                r1b[k].wait_recv()
        with scoped(f"r2_{k}{h}"):
            r2[k, h].wait_recv()
        result = po[k, 0, some] + c1r[k, 0, some].astype(jnp.float32) + c2r[k, some].astype(jnp.float32)
        if k == 2:
            with scoped(f"r3_3{h}"):
                r3[3, h].wait_recv()
            result = result + c3r[3, some].astype(jnp.float32)
        if k:
            c3[k, some] = result.astype(jnp.bfloat16)
            r3[k, h].start()
        else:
            po[0, 0, some] = result

    hidden_of(3)
    next_step()
    with scoped("await_cross"):
        await_weights((2,), dpeer)
        await_weights((2,), xpeer)
    cross(3)
    hidden_of(2)
    to_other_chip(3)
    cross(2)
    hidden_of(1)
    to_other_chip(2)
    cross(1)
    next_step()
    with scoped("await_near"):
        await_weights((2,), cpeer)
        await_weights((2,), t)
    near(3)
    hidden_of(0)
    to_other_chip(1)
    finish_row(3, 0)
    cross(0)
    finish_row(3, 1)
    to_other_chip(0)
    near(2)
    finish_row(2, 0)
    finish_row(2, 1)
    near(1)
    near(0)
    finish_row(1, 0)
    finish_row(1, 1)
    finish_row(0, 0)
    finish_row(0, 1)

    next_step()
    for h in range(2):
        some = pl.ds(h * half_rows, half_rows)
        for k in (1, 2):
            with scoped(f"r3_{k}{h}"):
                r3[k, h].wait_recv()
        ffn = po[0, 0, some] + c3r[1, some].astype(jnp.float32) + c3r[2, some].astype(jnp.float32)
        out_ref[some, :] = (stream[some, :] + 0.5 * ffn).astype(jnp.bfloat16)

    def sent(ref, sem):
        remote(ref, ref, sem, rs_rs.at[0], tp=cpeer).wait_send()

    def weights_sent(sems, width):
        sent(gate_ref.at[:, pl.ds(0, width)], sems.at[0])
        sent(down_ref.at[pl.ds(0, width // 2), :], sems.at[1])

    def width_of(target):
        return piece_bounds(target)[2]

    with scoped("drain"):
        for here in everyone:

            @pl.when(s == here)
            def _(here=here):
                if here < last:
                    for i, buffer in enumerate((k1b, k2b, vb)):
                        sent(buffer.at[pl.ds(0, here + 1)], kv_ss.at[i])
                    sent(act.at[0, pl.ds(0, here + 1)], az_ss.at[0])
                if here:
                    sent(act.at[0, pl.ds(0, sp_count - here)], az_ss.at[1])
                weights_sent(w_ss, sum(width_of(there) for there in everyone if there != here))
                weights_sent(f_ss, (sp_count - 1) * width_of(here))
                through = [
                    width_of(target)
                    for source in everyone
                    for target in everyone
                    if min(source, target) < here < max(source, target)
                ]
                if through:
                    weights_sent(t_ss, sum(through))

        sent(act.at[0], ax_ss.at[0])
        sent(act.at[pl.ds(0, 2)], ac_ss.at[0])
        sent(gains.at[pl.ds(0, sp_count - 1)], g_ss.at[0])
        sent(mp, rs_ss.at[0])
        sent(c1, c_ss.at[0])
        sent(c2, c_ss.at[1])
        sent(c3.at[pl.ds(0, sp_count - 1)], c_ss.at[2])


def fits(axes, query_first, values, lambdas, residual, gate_weight):
    sp, tp = axes["sp"], axes["tp"]
    rows, blk = residual.shape
    depth, hidden_all = gate_weight.shape
    if axes["grp"] != 2 or sp != tp or tp != 4 or lambdas.shape[1] != 1:
        return False
    if depth != blk or blk % 128 or hidden_all % 128 or rows % 16:
        return False
    if (2 * query_first.shape[1]) % 256 or values.shape[2] % 128:
        return False
    cols = -(-hidden_all // (128 * sp)) * 128
    if cols * sp - hidden_all >= cols or cols > hidden_all:
        return False
    if (cols * sp - hidden_all) % 128 or blk % 64 or rows % 32:
        return False
    need = 6 * sp * blk * cols + rows * blk * 2 * 20 * sp
    return need < 40 * 1024 * 1024


def one_device(
    axes,
    query_first,
    key_first,
    query_second,
    key_second,
    values,
    lambdas,
    residual,
    norm_gain,
    out_weight,
    gate_weight,
    up_weight,
    down_weight,
):
    if not fits(axes, query_first, values, lambdas, residual, gate_weight):
        return per_device(
            query_first,
            key_first,
            query_second,
            key_second,
            values,
            lambdas,
            residual,
            norm_gain,
            out_weight,
            gate_weight,
            up_weight,
            down_weight,
        )
    n = axes["sp"]
    rows, blk = residual.shape
    hidden_all = gate_weight.shape[1]
    cols = -(-hidden_all // (128 * n)) * 128
    value_size = values.shape[2]
    widths = (query_first.shape[1] // 2, query_second.shape[1] // 2)
    bf16, f32 = jnp.bfloat16, jnp.float32
    vmem = pl.BlockSpec(memory_space=pltpu.VMEM)
    hbm = pl.BlockSpec(memory_space=pl.ANY)
    dma = pltpu.SemaphoreType.DMA
    return pl.pallas_call(
        functools.partial(layer_kernel, n, widths),
        out_shape=jax.ShapeDtypeStruct((rows, blk), bf16),
        in_specs=[hbm] * 12,
        out_specs=vmem,
        scratch_shapes=[
            pltpu.VMEM(query_first.shape, bf16),
            pltpu.VMEM(query_second.shape, bf16),
            pltpu.VMEM(key_first.shape, bf16),
            pltpu.VMEM(key_second.shape, bf16),
            pltpu.VMEM(values.shape, bf16),
            pltpu.SMEM(lambdas.T.shape, f32),
            pltpu.VMEM(residual.shape, bf16),
            pltpu.VMEM(norm_gain.shape, bf16),
            pltpu.VMEM((n,) + key_first.shape, bf16),
            pltpu.VMEM((n,) + key_second.shape, bf16),
            pltpu.VMEM((n,) + values.shape, bf16),
            pltpu.VMEM(out_weight.shape, bf16),
            pltpu.VMEM((4, rows, 1), f32),
            pltpu.VMEM((4, rows, 1), f32),
            pltpu.VMEM((4, rows, value_size), f32),
            pltpu.VMEM((n, blk, cols), bf16),
            pltpu.VMEM((n, blk, cols), bf16),
            pltpu.VMEM((n, cols, blk), bf16),
            pltpu.VMEM((4, blk // 2, cols), bf16),
            pltpu.VMEM((4, blk // 2, cols), bf16),
            pltpu.VMEM((4, cols // 2, blk), bf16),
            pltpu.VMEM((3, rows, blk), bf16),
            pltpu.VMEM((3, rows, blk), bf16),
            pltpu.VMEM((2, rows, blk), f32),
            pltpu.VMEM((rows, blk), f32),
            pltpu.VMEM((n, n, rows, blk), bf16),
            pltpu.VMEM((n, 16, blk), bf16),
            pltpu.VMEM((n, rows, cols), bf16),
            pltpu.VMEM((n, 2, rows, blk), bf16),
            pltpu.VMEM((n, 2, rows, blk), bf16),
            pltpu.VMEM((n, 2, rows, blk), f32),
            pltpu.VMEM((n, rows, blk), bf16),
            pltpu.VMEM((n, rows, blk), bf16),
            pltpu.VMEM((n, rows, blk), bf16),
            pltpu.VMEM((n, rows, blk), bf16),
            dma((3,)),
            dma((3, n - 1)),
            dma((2,)),
            dma((3, PARTS * n)),
            dma((2,)),
            dma((3, PARTS * n)),
            dma((2,)),
            dma((3, PARTS * n)),
            dma((4,)),
            dma((8,)),
            dma((1,)),
            dma((n - 1,)),
            dma((1,)),
            dma((2,)),
            dma((2,)),
            dma((n,)),
            dma((1,)),
            dma((n,)),
            dma((1,)),
            dma((2, n)),
            dma((3,)),
            dma((6, n)),
        ],
        compiler_params=pltpu.CompilerParams(
            collective_id=0, has_side_effects=True, vmem_limit_bytes=60 * 1024 * 1024
        ),
    )(
        query_first,
        query_second,
        key_first,
        key_second,
        values,
        lambdas.T,
        residual,
        norm_gain,
        out_weight,
        gate_weight,
        up_weight,
        down_weight,
    )

def solution(mesh):
    return jax.shard_map(
        functools.partial(one_device, dict(mesh.shape)),
        mesh=mesh,
        in_specs=(
            P(("grp", "sp"), "tp"),
            P(("grp", "sp"), "tp"),
            P(("grp", "sp"), "tp"),
            P(("grp", "sp"), "tp"),
            P(("grp", "sp"), None, "tp"),
            P(None, "tp"),
            P(("grp", "sp"), "tp"),
            P("tp"),
            P(None, "tp", None),
            P("sp", "tp"),
            P("sp", "tp"),
            P("tp", "sp"),
        ),
        out_specs=P(("grp", "sp"), "tp"),
        check_vma=False,
    )
```

```python
import functools

import jax
import jax.numpy as jnp
from jax import lax
from jax.experimental import pallas as pl
from jax.experimental.pallas import tpu as pltpu
from jax.sharding import PartitionSpec as P

D = 2048


def per_device(
    query_first,
    key_first,
    query_second,
    key_second,
    values,
    lambdas,
    residual,
    norm_gain,
    out_weight,
    gate_weight,
    up_weight,
    down_weight,
):
    tok_rows = query_first.shape[0]
    heads_here = lambdas.shape[1]
    width_first = query_first.shape[1] // (2 * heads_here)
    width_second = query_second.shape[1] // (2 * heads_here)
    value_size = values.shape[2] // heads_here
    offset = lax.axis_index("sp") * tok_rows
    query_pos = offset + lax.broadcasted_iota(jnp.int32, (tok_rows, 1), 0)
    query_groups = (
        query_first.reshape(tok_rows, heads_here, 2, width_first),
        query_second.reshape(tok_rows, heads_here, 2, width_second),
    )
    key_widths = (width_first, width_second)
    start_state = (
        jnp.full((heads_here, 2, tok_rows, 1), -1e30, jnp.float32),
        jnp.zeros((heads_here, 2, tok_rows, 1), jnp.float32),
        jnp.zeros((heads_here, 2, tok_rows, value_size), jnp.float32),
    )
    states = (start_state, start_state)
    pieces = (
        lax.all_gather(key_first, "sp", axis=0, tiled=True),
        lax.all_gather(key_second, "sp", axis=0, tiled=True),
        lax.all_gather(values, "sp", axis=0, tiled=True),
    )
    piece_rows = pieces[0].shape[0]
    key_pos = lax.broadcasted_iota(jnp.int32, (1, piece_rows), 1)
    allowed = key_pos <= query_pos
    value_rows = pieces[2].reshape(piece_rows, 2, heads_here, value_size)
    results = []
    for group_idx in range(2):
        key_width = key_widths[group_idx]
        key_part = pieces[group_idx].reshape(piece_rows, heads_here, 2, key_width)
        scores = jnp.einsum(
            "qhmd,khmd->hmqk", query_groups[group_idx], key_part, preferred_element_type=jnp.float32
        ) * key_width ** (-0.5)
        scores = jnp.where(allowed, scores, -1e30)
        running, totals, weighted = states[group_idx]
        new_peak = jnp.maximum(running, jnp.max(scores, axis=-1, keepdims=True))
        weights = jnp.where(allowed, jnp.exp(scores - new_peak), 0.0)
        totals = jnp.sum(weights, axis=-1, keepdims=True)
        weighted = jnp.einsum(
            "hmqk,khe->hmqe",
            weights.astype(jnp.bfloat16),
            value_rows[:, group_idx],
            preferred_element_type=jnp.float32,
        )
        results.append((new_peak, totals, weighted))
    states = (results[0], results[1])
    map_out = jnp.stack([states[0][2] / states[0][1], states[1][2] / states[1][1]])
    differ = map_out[:, :, 0] - lambdas[:, :, None, None] * map_out[:, :, 1]
    head_scale = lax.rsqrt(jnp.mean(differ * differ, axis=-1, keepdims=True) + 1e-06)
    attended = (0.8 * differ * head_scale).astype(jnp.bfloat16)
    projection = out_weight.reshape(2, heads_here, value_size, out_weight.shape[2])
    mixed_part = jnp.einsum(
        "ghqe,gher->qr", attended, projection, preferred_element_type=jnp.float32
    )
    mixed = lax.psum_scatter(
        mixed_part.astype(jnp.bfloat16), "tp", scatter_dimension=1, tiled=True
    ).astype(jnp.float32)
    stream = residual.astype(jnp.float32) + mixed
    squares = lax.psum(jnp.sum(stream * stream, axis=1), "tp")
    row_scale = lax.rsqrt(squares[:, None] / D + 1e-06)
    normed = (stream * row_scale * norm_gain.astype(jnp.float32)).astype(jnp.bfloat16)
    full_rows = lax.all_gather(normed, "tp", axis=1, tiled=True)
    pieces = (
        lax.all_gather(gate_weight, "sp", axis=0, tiled=True),
        lax.all_gather(up_weight, "sp", axis=0, tiled=True),
    )
    gate = jnp.dot(full_rows, pieces[0], preferred_element_type=jnp.float32)
    up_part = jnp.dot(full_rows, pieces[1], preferred_element_type=jnp.float32)
    hidden = (jax.nn.silu(gate) * up_part).astype(jnp.bfloat16)
    partial_out = jnp.dot(
        hidden,
        lax.all_gather(down_weight, "sp", axis=1, tiled=True),
        preferred_element_type=jnp.float32,
    )
    ffn = lax.psum_scatter(
        partial_out.astype(jnp.bfloat16), "tp", scatter_dimension=1, tiled=True
    ).astype(jnp.float32)
    return (stream + 0.5 * ffn).astype(jnp.bfloat16)


def flip(index, bits):
    bit = 1
    while bit <= bits:
        if (bits // bit) % 2:
            index = index + bit - 2 * bit * ((index // bit) % 2)
        bit *= 2
    return index


def nt_dot(a, b):
    return lax.dot_general(a, b, (((1,), (1,)), ((), ())), preferred_element_type=jnp.float32)


def dot(a, b):
    return jnp.dot(a, b, preferred_element_type=jnp.float32)


def scoped(name):
    return jax.named_scope(name)


PLAN = (
    {
        (1, 0): ((1, 1, 0), (0, 1, 0)),
        (1, 1): ((0, 1, 0),),
        (2, 0): ((0, 2, 0), (0, 2, 1)),
        (2, 1): ((0, 2, 0), (0, 2, 1), (1, 2, 0)),
        (3, 0): ((0, 3, 1), (0, 3, 0), (0, 3, 2), (1, 3, 0)),
        (3, 1): ((0, 3, 2), (1, 3, 0), (0, 3, 0)),
    },
    {
        (0, 0): ((0, 0, 1),),
        (1, 0): ((0, 1, 2),),
        (1, 1): ((0, 1, 2), (0, 2, 0), (1, 0, 3)),
        (2, 0): ((0, 3, 1), (1, 2, 3), (0, 2, 3)),
    },
    {
        (0, 0): ((0, 0, 2),),
        (1, 0): ((0, 1, 3), (0, 2, 0)),
        (2, 1): ((2, 3), (0, 2, 3)),
        (3, 1): ((0, 3, 1),),
    },
    {
        (0, 1): ((1, 0, 3), (0, 0, 1)),
        (1, 1): ((1, 1, 0),),
        (2, 0): ((0, 3, 0), (2, 1), (0, 1, 3), (2, 3)),
        (2, 1): ((1, 2, 1), (2, 1), (1, 0, 3)),
        (3, 0): ((2, 2), (3, 2)),
    },
    {
        (0, 0): ((0, 0, 3), (2, 2), (5, 0), (1, 0, 3), (4, 1), (1, 0, 2), (2, 3), (2, 1), (1, 0, 1), (4, 2), (4, 3), (3, 2), (5, 2), (5, 1), (5, 3)),
        (0, 1): ((1, 0, 1), (0, 0, 3), (0, 0, 2), (2, 2), (5, 1), (1, 0, 2), (2, 1), (3, 1), (4, 2), (2, 3), (4, 1), (5, 0), (4, 3), (5, 3), (3, 2), (5, 2)),
        (1, 0): ((2, 2), (4, 0), (0, 0, 2), (2, 0), (0, 3, 0), (2, 3), (4, 2), (0, 0, 3), (5, 1), (1, 1, 3), (1, 0, 3), (1, 0, 2), (4, 3), (5, 2), (3, 0), (5, 0), (1, 2, 0)),
        (1, 1): ((4, 0), (0, 1, 3), (2, 0), (3, 0), (4, 2), (0, 0, 3), (2, 2), (0, 3, 0), (0, 0, 2), (4, 3), (1, 0, 2), (1, 2, 0), (1, 1, 3), (5, 2), (1, 1, 2), (2, 3), (1, 3, 0), (3, 2), (5, 3)),
        (2, 0): ((4, 3), (5, 1), (4, 1), (4, 0), (1, 2, 0), (5, 2), (1, 2, 1), (2, 0), (5, 0), (1, 3, 0), (0, 0, 3)),
        (2, 1): ((0, 3, 0), (4, 1), (4, 0), (1, 2, 3), (5, 2), (4, 3), (0, 3, 1), (1, 3, 0), (0, 1, 3), (0, 0, 3), (2, 0), (5, 1), (3, 0), (5, 0)),
        (3, 0): ((4, 1), (1, 3, 1), (5, 3), (2, 1), (4, 0), (2, 0), (5, 2), (1, 3, 2), (4, 2), (5, 0), (5, 1)),
        (3, 1): ((1, 3, 2), (2, 2), (4, 2), (4, 1), (3, 0), (3, 2), (1, 3, 1), (4, 0), (2, 1), (2, 0), (5, 1), (5, 0)),
    },
    {
        (1, 0): ((1, 1, 2),),
        (2, 1): ((1, 3, 1),),
    },
    {
        (1, 0): ((3, 2), (1, 3, 0), (5, 3)),
        (2, 1): ((5, 3), (3, 3), (1, 1, 3)),
    },
    {
        (3, 1): ((5, 2),),
    },
    {
        (1, 1): ((5, 1), (5, 0)),
        (2, 0): ((5, 3), (1, 1, 3)),
    },
    {
        (0, 0): ((3, 3),),
        (2, 0): ((1, 0, 3), (1, 3, 1)),
        (3, 1): ((5, 3),),
    },
    {},
    {
        (0, 1): ((3, 3),),
        (3, 0): ((3, 0), (3, 1)),
    },
    {
        (1, 0): ((3, 3),),
        (2, 1): ((3, 1),),
    },
    {
        (2, 0): ((3, 0), (3, 3)),
        (3, 1): ((3, 1),),
    },
    {},
    {
        (0, 0): ((3, 1),),
        (1, 1): ((3, 3),),
    },
    {},
    {},
    {},
    {},
    {},
    {},
    {},
    {},
    {
        (2, 0): ((3, 1),),
    },
    {},
    {},
    {},
    {},
    {},
    {},
    {},
    {},
    {},
    {},
    {},
    {},
    {},
    {},
    {},
    {},
    {},
    {},
    {},
    {},
    {},
)

TAIL = (
    ("hidden", 3),
    ("await_far", 0),
    ("far", 0, 3),
    ("hidden", 2),
    ("cross", 0, 3),
    ("far", 0, 2),
    ("hidden", 1),
    ("cross", 0, 2),
    ("far", 0, 1),
    ("hidden", 0),
    ("cross", 0, 1),
    ("far", 0, 0),
    ("cross", 0, 0),
    ("await_near", 0),
    ("near", 0, 3),
    ("near", 0, 2),
    ("settle", 0, 3),
    ("near", 0, 1),
    ("near", 0, 0),
    ("await_far", 1),
    ("far", 1, 3),
    ("far", 1, 2),
    ("cross", 1, 3),
    ("settle", 0, 2),
    ("far", 1, 1),
    ("cross", 1, 2),
    ("far", 1, 0),
    ("cross", 1, 1),
    ("cross", 1, 0),
    ("await_near", 1),
    ("near", 1, 3),
    ("near", 1, 2),
    ("settle", 0, 1),
    ("settle", 1, 3),
    ("near", 1, 1),
    ("near", 1, 0),
    ("settle", 0, 0),
    ("settle", 1, 2),
    ("settle", 1, 1),
    ("settle", 1, 0),
)

WEIGHTS_IN, DOWN_IN, HAND_IN, HAND_DOWN, ROW, ACROSS = range(6)


PARTS = 2


def transit_slot(here, source, target):
    outer = 0 if source < here else 2
    if outer:
        return outer + (target if here == 2 else source - 2)
    return outer + (target - 2 if here == 1 else source)


def layer_kernel(
    sp_count,
    widths,
    q1_hbm,
    q2_hbm,
    k1_hbm,
    k2_hbm,
    v_hbm,
    lam_hbm,
    residual_hbm,
    gain_hbm,
    proj_hbm,
    gate_ref,
    up_ref,
    down_ref,
    out_ref,
    q1_ref,
    q2_ref,
    k1_ref,
    k2_ref,
    v_ref,
    lam_ref,
    residual_ref,
    gain_ref,
    k1b,
    k2b,
    vb,
    proj_ref,
    peak,
    total,
    acc,
    wg,
    wu,
    wd,
    tg,
    tu,
    td,
    mp,
    rsb,
    mine_ref,
    stream,
    act,
    gains,
    hid,
    c1,
    c1r,
    po,
    c2,
    c2r,
    c3,
    c3r,
    kv_ss,
    kv_rs,
    w_ss,
    w_rs,
    t_ss,
    t_rs,
    f_ss,
    f_rs,
    own_sem,
    in_sem,
    g_ss,
    g_rs,
    rs_ss,
    rs_rs,
    az_ss,
    az_rs,
    ax_ss,
    ax_rs,
    ac_ss,
    ac_rs,
    c_ss,
    c_rs,
):
    s = lax.axis_index("sp")
    t = lax.axis_index("tp")
    y = lax.axis_index("grp")
    rows, blk = residual_ref.shape
    cols = wg.shape[2]
    hidden_all = gate_ref.shape[1]
    xpeer, cpeer, dpeer = flip(t, 2), flip(t, 1), flip(t, 3)
    others = range(1, sp_count)
    everyone = range(sp_count)
    last = sp_count - 1

    def remote(src, dst, ssem, rsem, **where):
        return pltpu.make_async_remote_copy(
            src_ref=src,
            dst_ref=dst,
            send_sem=ssem,
            recv_sem=rsem,
            device_id=where,
            device_id_type=pl.DeviceIdType.MESH,
        )

    def either(test, action):
        pl.when(test)(lambda: action(True))
        pl.when(jnp.logical_not(test))(lambda: action(False))

    barrier = pltpu.get_barrier_semaphore()
    for k in others:
        pl.semaphore_signal(barrier, inc=1, device_id={"sp": flip(s, k)}, device_id_type=pl.DeviceIdType.MESH)
        pl.semaphore_signal(barrier, inc=1, device_id={"tp": flip(t, k)}, device_id_type=pl.DeviceIdType.MESH)
    pl.semaphore_signal(barrier, inc=1, device_id={"grp": 1 - y}, device_id_type=pl.DeviceIdType.MESH)
    inputs = (
        (k1_hbm, k1_ref),
        (k2_hbm, k2_ref),
        (v_hbm, v_ref),
        (q1_hbm, q1_ref),
        (q2_hbm, q2_ref),
        (gain_hbm, gain_ref),
        (lam_hbm, lam_ref),
        (residual_hbm, residual_ref),
    )
    loads = [pltpu.make_async_copy(far, here, in_sem.at[i]) for i, (far, here) in enumerate(inputs)]
    for load in loads:
        load.start()

    half_d = wg.shape[1] // 2
    extra = sp_count * cols - hidden_all
    d_half = pl.ds(pl.multiple_of(y * half_d, half_d), half_d)

    def kv_copies(back):
        pairs = ((k1_ref, k1b), (k2_ref, k2b), (v_ref, vb))
        right = lax.rem(s + 1, sp_count)
        return [
            remote(dst.at[back] if back else src, dst.at[back + 1], kv_ss.at[i], kv_rs.at[i, back], sp=right)
            for i, (src, dst) in enumerate(pairs)
        ]

    def arrived(back):
        pairs = ((k1_ref, k1b), (k2_ref, k2b), (v_ref, vb))
        left = lax.rem(s + sp_count - 1, sp_count)
        return [
            remote(src, dst.at[back], kv_ss.at[i], kv_rs.at[i, back - 1], sp=left)
            for i, (src, dst) in enumerate(pairs)
        ]

    def piece_bounds(target):
        short = target == last
        begin = hidden_all - cols + extra if short else target * cols
        return (begin, extra, cols - extra) if short else (begin, 0, cols)

    def part_rows(kind, target, part, side):
        _, _, size = piece_bounds(target)
        whole = half_d if kind < 2 else size // 2
        rows_here = whole // PARTS
        return pl.multiple_of(side * whole + part * rows_here, 16), rows_here

    def own_piece(kind, target, part):
        src = (gate_ref, up_ref, down_ref)[kind]
        begin, _, size = piece_bounds(target)
        first, count = part_rows(kind, target, part, y)
        if kind < 2:
            return src.at[pl.ds(first, count), pl.ds(begin, size)]
        return src.at[pl.ds(pl.multiple_of(begin + first, 16), count), :]

    def final_place(kind, source, target, part, side):
        dst = (wg, wu, wd)[kind]
        _, skip, size = piece_bounds(target)
        first, count = part_rows(kind, target, part, side)
        if kind < 2:
            return dst.at[source, pl.ds(first, count), pl.ds(skip, size)]
        return dst.at[source, pl.ds(pl.multiple_of(skip + first, 16), count)]

    def transit_place(kind, here, source, target, part):
        buffer = (tg, tu, td)[kind].at[transit_slot(here, source, target)]
        _, _, size = piece_bounds(target)
        first, count = part_rows(kind, target, part, 0)
        return buffer.at[pl.ds(first, count), pl.ds(0, size)] if kind < 2 else buffer.at[pl.ds(first, count)]

    def weight_hop(kind, here, source, target, part):
        there = here + 1 if target > here else here - 1
        if source == here:
            piece, ssem = own_piece(kind, target, part), w_ss.at[kind // 2]
        else:
            piece = transit_place(kind, here, source, target, part)
            ssem = t_ss.at[kind // 2]
        if there == target:
            place, rsem = final_place(kind, source, target, part, y), w_rs.at[kind, PARTS * source + part]
        else:
            place = transit_place(kind, there, source, target, part)
            rsem = t_rs.at[kind, PARTS * transit_slot(there, source, target) + part]
        return remote(piece, place, ssem, rsem, sp=there)

    def move_weights(kinds, here, source, target):
        for kind in kinds:
            for part in range(PARTS):
                if source != here:
                    before = here - 1 if source < here else here + 1
                    with scoped(f"pass{kind}{part}_{source}{target}"):
                        weight_hop(kind, before, source, target, part).wait_recv()
                weight_hop(kind, here, source, target, part).start()

    def weight_hand(kind, source, target, part):
        place = final_place(kind, source, target, part, y)
        return remote(place, place, f_ss.at[kind // 2], f_rs.at[kind, PARTS * source + part], grp=1 - y)

    def hand_over(kinds, here, source):
        for kind in kinds:
            for part in range(PARTS):
                before = here - 1 if source < here else here + 1
                with scoped(f"hand{kind}{part}_{source}"):
                    weight_hop(kind, before, source, here, part).wait_recv()
                weight_hand(kind, source, here, part).start()

    def own_copy(kind, short):
        src, dst = ((gate_ref, wg), (up_ref, wu), (down_ref, wd))[kind]
        begin = hidden_all - cols + extra if short else pl.multiple_of(s * cols, 128)
        skip, size = (extra, cols - extra) if short else (0, cols)
        if kind < 2:
            return pltpu.make_async_copy(src.at[:, pl.ds(begin, size)], dst.at[s, :, pl.ds(skip, size)], own_sem.at[kind])
        return pltpu.make_async_copy(src.at[pl.ds(begin, size), :], dst.at[s, pl.ds(skip, size)], own_sem.at[kind])

    def act_z(row, begin, target, way):
        piece = act.at[t, row]
        return remote(piece, piece, az_ss.at[way], az_rs.at[row], sp=target)

    def along(here, row, action):
        if row <= here < last:
            action(act_z(row, here, here + 1, 0))
        if row >= here > 0:
            action(act_z(row, here, here - 1, 1))

    def act_x(row):
        piece = act.at[t, row]
        return remote(piece, piece, ax_ss.at[0], ax_rs.at[row], tp=xpeer)

    def act_c(row, second):
        piece = act.at[xpeer if second else t, row]
        return remote(piece, piece, ac_ss.at[0], ac_rs.at[second, row], tp=cpeer)

    def start(copy):
        copy.start()

    def perform(here, event):
        kind, index = event[:2]
        if kind == WEIGHTS_IN:
            move_weights((0, 1), here, index, event[2])
        elif kind == DOWN_IN:
            move_weights((2,), here, index, event[2])
        elif kind == HAND_IN:
            hand_over((0, 1), here, index)
        elif kind == HAND_DOWN:
            hand_over((2,), here, index)
        elif kind == ROW:
            with scoped(f"row{index}"):
                act_z(index, here, here, 0).wait_recv()
            send_row(here, index)
        elif kind == ACROSS:
            with scoped(f"across{index}"):
                act_x(index).wait_recv()
            act_c(index, 1).start()

    def send_row(here, row):
        along(here, row, start)
        act_x(row).start()
        act_c(row, 0).start()

    x = t // 2
    steps = iter(PLAN)

    def next_step():
        plan = next(steps)
        for here in everyone:
            lists = [plan.get((here, side), ()) for side in range(2)]
            tests = [(s == here, lists[0])]
            if lists[0] != lists[1]:
                tests = [(jnp.logical_and(s == here, x == side), lists[side]) for side in range(2)]
            for test, events in tests:
                if events:

                    @pl.when(test)
                    def _(here=here, events=events):
                        for event in events:
                            perform(here, event)

    @pl.when(s == last)
    def _():
        wg[:, :, :extra] = jnp.zeros((sp_count, wg.shape[1], extra), jnp.bfloat16)
        wu[:, :, :extra] = jnp.zeros((sp_count, wg.shape[1], extra), jnp.bfloat16)
        wd[:, :extra, :] = jnp.zeros((sp_count, extra, blk), jnp.bfloat16)

    proj_copy = pltpu.make_async_copy(proj_hbm, proj_ref, own_sem.at[3])
    proj_copy.start()

    def start_own(short):
        for kind in range(3):
            own_copy(kind, short).start()

    either(s == last, start_own)

    for load in loads[:-1]:
        load.wait()
    gains[t] = jnp.broadcast_to(gain_ref[...].reshape(1, blk), gains.shape[1:])
    with scoped("barrier"):
        pl.semaphore_wait(barrier, 2 * (sp_count - 1) + 1)
    next_step()

    @pl.when(s < last)
    def _():
        for copy in kv_copies(0):
            copy.start()

    gain_copies = []
    for k in others:
        copy = remote(gains.at[t], gains.at[t], g_ss.at[0], g_rs.at[k - 1], tp=flip(t, k))
        copy.start()
        gain_copies.append(copy)

    q_refs = (q1_ref, q2_ref)
    lane = lax.broadcasted_iota(jnp.int32, (1, 2 * widths[0]), 1)

    def block(keys, v, diagonal):
        for group in range(2):
            width = widths[group]
            values = v[:, group, :]
            for m in range(2):
                if width % 128:
                    span = slice(0, 2 * width)
                    queries = q_refs[group][:, span]
                    queries = jnp.where(lane // width == m, queries.astype(jnp.float32), 0.0).astype(jnp.bfloat16)
                else:
                    span = slice(m * width, (m + 1) * width)
                    queries = q_refs[group][:, span]
                scores = nt_dot(queries, keys[group][:, span]) * width ** (-0.5)
                state = 2 * group + m
                if diagonal:
                    allowed = lax.broadcasted_iota(jnp.int32, (rows, rows), 1) <= lax.broadcasted_iota(
                        jnp.int32, (rows, rows), 0
                    )
                    scores = jnp.where(allowed, scores, -1e30)
                    top = jnp.max(scores, axis=1, keepdims=True)
                    weights = jnp.exp(scores - top)
                    peak[state] = top
                    total[state] = jnp.sum(weights, axis=1, keepdims=True)
                    acc[state] = dot(weights.astype(jnp.bfloat16), values)
                else:
                    before = peak[state]
                    top = jnp.maximum(before, jnp.max(scores, axis=1, keepdims=True))
                    fade = jnp.exp(before - top)
                    weights = jnp.exp(scores - top)
                    peak[state] = top
                    total[state] = total[state] * fade + jnp.sum(weights, axis=1, keepdims=True)
                    acc[state] = acc[state] * fade + dot(weights.astype(jnp.bfloat16), values)

    with scoped("diag"):
        block((k1_ref, k2_ref), v_ref, True)
    for back in others:

        @pl.when(s >= back)
        def _(back=back):
            with scoped(f"kvwait{back}"):
                for i, copy in enumerate(arrived(back)):
                    copy.wait_recv()
                    if back < last:
                        pl.when(s < last)(kv_copies(back)[i].start)
            with scoped(f"block{back}"):
                block((k1b.at[back], k2b.at[back]), vb.at[back], False)

    next_step()
    proj_copy.wait()
    loads[-1].wait()
    with scoped("finish"):
        attended = []
        for group in range(2):
            first = acc[2 * group] / total[2 * group]
            second = acc[2 * group + 1] / total[2 * group + 1]
            differ = first - lam_ref[0, group] * second
            scale = lax.rsqrt(jnp.mean(differ * differ, axis=1, keepdims=True) + 1e-06)
            attended.append((0.8 * differ * scale).astype(jnp.bfloat16))

    def project(owner):
        columns = pl.ds(pl.multiple_of(owner * blk, blk), blk)
        return dot(attended[0], proj_ref[0, :, columns]) + dot(attended[1], proj_ref[1, :, columns])

    with scoped("project"):
        mp[0] = project(cpeer).astype(jnp.bfloat16)
        mp[1] = project(dpeer).astype(jnp.bfloat16)
        to_core = remote(mp.at[pl.ds(0, 2)], rsb.at[pl.ds(0, 2)], rs_ss.at[0], rs_rs.at[0], tp=cpeer)
        to_core.start()
        to_x = remote(mp.at[2], rsb.at[2], rs_ss.at[0], rs_rs.at[1], tp=xpeer)
        mine_ref[1] = project(xpeer)
        mine_ref[0] = residual_ref[...].astype(jnp.float32) + project(t)
    next_step()
    with scoped("rscore"):
        to_core.wait_recv()
    mp[2] = (mine_ref[1] + rsb[1].astype(jnp.float32)).astype(jnp.bfloat16)
    to_x.start()
    mine_ref[0] = mine_ref[0] + rsb[0].astype(jnp.float32)
    next_step()
    with scoped("rsx"):
        to_x.wait_recv()
    stream[...] = mine_ref[0] + rsb[2].astype(jnp.float32)
    act[t, s] = stream[...].astype(jnp.bfloat16)

    for here in everyone:

        @pl.when(s == here)
        def _(here=here):
            send_row(here, here)

    next_step()

    for copy in gain_copies:
        copy.wait_recv()

    def await_weights(kinds, source):
        def go(short):
            for kind in kinds:

                @pl.when(source != s)
                def _(kind=kind):
                    for part in range(PARTS):
                        place = final_place(kind, source, last if short else 0, part, 1 - y)
                        sem = PARTS * source + part
                        remote(place, place, f_ss.at[kind // 2], f_rs.at[kind, sem], grp=1 - y).wait_recv()

                @pl.when(source == s)
                def _(kind=kind):
                    own_copy(kind, short).wait()

        either(s == last, go)

    with scoped("await_gu"):
        for source in everyone:
            await_weights((0, 1), source)
    column = jnp.minimum(s * cols, hidden_all - cols) + lax.broadcasted_iota(jnp.int32, (1, cols), 1)
    mine = column >= s * cols

    def hidden_of(k):
        row = flip(s, k)
        with scoped(f"acwait{k}"):
            act_c(row, 0).wait_recv()
            act_c(row, 1).wait_recv()
        with scoped(f"hidden{k}"):
            squares = jnp.zeros((rows, 1), jnp.float32)
            for part in range(sp_count):
                piece = act[part, row].astype(jnp.float32)
                squares = squares + jnp.sum(piece * piece, axis=1, keepdims=True)
            scale = lax.rsqrt(squares / (sp_count * blk) + 1e-06)
            gate = jnp.zeros((rows, cols), jnp.float32)
            up = jnp.zeros((rows, cols), jnp.float32)
            for part in range(sp_count):
                gain = gains[part, 0:1, :].astype(jnp.float32)
                normed = (act[part, row].astype(jnp.float32) * scale * gain).astype(jnp.bfloat16)
                gate = gate + dot(normed, wg[part])
                up = up + dot(normed, wu[part])
            hidden = gate / (1.0 + jnp.exp(-gate)) * up
            hid[k] = jnp.where(mine, hidden, 0.0).astype(jnp.bfloat16)

    core = t % 2
    r1, r2, r3 = {}, {}, {}
    for k in everyone:
        for far in range(2):
            r1[k, far] = remote(c1.at[k, far], c1r.at[k, far], c_ss.at[0], c_rs.at[far, k], tp=cpeer)
        r2[k] = remote(c2.at[k], c2r.at[k], c_ss.at[1], c_rs.at[2, k], tp=xpeer)
        if k:
            r3[k] = remote(c3.at[k], c3r.at[k], c_ss.at[2], c_rs.at[3, k], sp=flip(s, 1 if k == 3 else k))

    def block_of(wave, far):
        return 2 * ((1 - x) if far else x) + wave

    def product(wave, k, far):
        with scoped(f"product{wave}{k}{far}"):
            value = dot(hid[k], wd[block_of(wave, far)])

            @pl.when(core == wave)
            def _():
                po[k, far] = value

            @pl.when(core != wave)
            def _():
                c1[k, far] = value.astype(jnp.bfloat16)
                r1[k, far].start()

    def to_other_chip(wave, k):
        @pl.when(core == wave)
        def _():
            with scoped(f"cross{wave}{k}"):
                r1[k, 1].wait_recv()
            c2[k] = (po[k, 1] + c1r[k, 1].astype(jnp.float32)).astype(jnp.bfloat16)
            r2[k].start()

    def settle(wave, k):
        @pl.when(core == wave)
        def _():
            with scoped(f"settle{wave}{k}"):
                r1[k, 0].wait_recv()
                r2[k].wait_recv()
            result = po[k, 0] + c1r[k, 0].astype(jnp.float32) + c2r[k].astype(jnp.float32)
            if k == 2:
                with scoped(f"pair{wave}"):
                    r3[3].wait_recv()
                result = result + c3r[3].astype(jnp.float32)
            if k:
                c3[k] = result.astype(jnp.bfloat16)
                r3[k].start()
            else:
                po[0, 0] = result

    for name, *where in TAIL:
        next_step()
        if name == "hidden":
            hidden_of(where[0])
        elif name in ("far", "near"):
            product(*where, far=int(name == "far"))
        elif name == "cross":
            to_other_chip(*where)
        elif name == "settle":
            settle(*where)
        else:
            with scoped(f"{name}{where[0]}"):
                await_weights((2,), block_of(where[0], name == "await_far"))

    next_step()
    ffn = po[0, 0]
    for k in (1, 2):
        with scoped(f"r3_{k}"):
            r3[k].wait_recv()
        ffn = ffn + c3r[k].astype(jnp.float32)
    out_ref[...] = (stream[...] + 0.5 * ffn).astype(jnp.bfloat16)

    def sent(ref, sem):
        remote(ref, ref, sem, rs_rs.at[0], tp=cpeer).wait_send()

    def weights_sent(sems, width):
        sent(gate_ref.at[:, pl.ds(0, width)], sems.at[0])
        sent(down_ref.at[pl.ds(0, width // 2), :], sems.at[1])

    def width_of(target):
        return piece_bounds(target)[2]

    with scoped("drain"):
        for here in everyone:

            @pl.when(s == here)
            def _(here=here):
                if here < last:
                    for i, buffer in enumerate((k1b, k2b, vb)):
                        sent(buffer.at[pl.ds(0, here + 1)], kv_ss.at[i])
                    sent(act.at[0, pl.ds(0, here + 1)], az_ss.at[0])
                if here:
                    sent(act.at[0, pl.ds(0, sp_count - here)], az_ss.at[1])
                weights_sent(w_ss, sum(width_of(there) for there in everyone if there != here))
                weights_sent(f_ss, (sp_count - 1) * width_of(here))
                through = [
                    width_of(target)
                    for source in everyone
                    for target in everyone
                    if min(source, target) < here < max(source, target)
                ]
                if through:
                    weights_sent(t_ss, sum(through))

        sent(act.at[0], ax_ss.at[0])
        sent(act.at[pl.ds(0, 2)], ac_ss.at[0])
        sent(gains.at[pl.ds(0, sp_count - 1)], g_ss.at[0])
        sent(mp, rs_ss.at[0])
        sent(c1, c_ss.at[0])
        sent(c2, c_ss.at[1])
        sent(c3.at[pl.ds(0, sp_count - 1)], c_ss.at[2])


def fits(axes, query_first, values, lambdas, residual, gate_weight):
    sp, tp = axes["sp"], axes["tp"]
    rows, blk = residual.shape
    depth, hidden_all = gate_weight.shape
    if axes["grp"] != 2 or sp != tp or tp != 4 or lambdas.shape[1] != 1:
        return False
    if depth != blk or blk % 128 or hidden_all % 128 or rows % 16:
        return False
    if (2 * query_first.shape[1]) % 256 or values.shape[2] % 128:
        return False
    cols = -(-hidden_all // (128 * sp)) * 128
    if cols * sp - hidden_all >= cols or cols > hidden_all:
        return False
    if (cols * sp - hidden_all) % 128 or blk % 64 or rows % 32:
        return False
    need = 6 * sp * blk * cols + rows * blk * 2 * 20 * sp
    return need < 40 * 1024 * 1024


def one_device(
    axes,
    query_first,
    key_first,
    query_second,
    key_second,
    values,
    lambdas,
    residual,
    norm_gain,
    out_weight,
    gate_weight,
    up_weight,
    down_weight,
):
    if not fits(axes, query_first, values, lambdas, residual, gate_weight):
        return per_device(
            query_first,
            key_first,
            query_second,
            key_second,
            values,
            lambdas,
            residual,
            norm_gain,
            out_weight,
            gate_weight,
            up_weight,
            down_weight,
        )
    n = axes["sp"]
    rows, blk = residual.shape
    hidden_all = gate_weight.shape[1]
    cols = -(-hidden_all // (128 * n)) * 128
    value_size = values.shape[2]
    widths = (query_first.shape[1] // 2, query_second.shape[1] // 2)
    bf16, f32 = jnp.bfloat16, jnp.float32
    vmem = pl.BlockSpec(memory_space=pltpu.VMEM)
    hbm = pl.BlockSpec(memory_space=pl.ANY)
    dma = pltpu.SemaphoreType.DMA
    return pl.pallas_call(
        functools.partial(layer_kernel, n, widths),
        out_shape=jax.ShapeDtypeStruct((rows, blk), bf16),
        in_specs=[hbm] * 12,
        out_specs=vmem,
        scratch_shapes=[
            pltpu.VMEM(query_first.shape, bf16),
            pltpu.VMEM(query_second.shape, bf16),
            pltpu.VMEM(key_first.shape, bf16),
            pltpu.VMEM(key_second.shape, bf16),
            pltpu.VMEM(values.shape, bf16),
            pltpu.SMEM(lambdas.T.shape, f32),
            pltpu.VMEM(residual.shape, bf16),
            pltpu.VMEM(norm_gain.shape, bf16),
            pltpu.VMEM((n,) + key_first.shape, bf16),
            pltpu.VMEM((n,) + key_second.shape, bf16),
            pltpu.VMEM((n,) + values.shape, bf16),
            pltpu.VMEM(out_weight.shape, bf16),
            pltpu.VMEM((4, rows, 1), f32),
            pltpu.VMEM((4, rows, 1), f32),
            pltpu.VMEM((4, rows, value_size), f32),
            pltpu.VMEM((n, blk, cols), bf16),
            pltpu.VMEM((n, blk, cols), bf16),
            pltpu.VMEM((n, cols, blk), bf16),
            pltpu.VMEM((4, blk // 2, cols), bf16),
            pltpu.VMEM((4, blk // 2, cols), bf16),
            pltpu.VMEM((4, cols // 2, blk), bf16),
            pltpu.VMEM((3, rows, blk), bf16),
            pltpu.VMEM((3, rows, blk), bf16),
            pltpu.VMEM((2, rows, blk), f32),
            pltpu.VMEM((rows, blk), f32),
            pltpu.VMEM((n, n, rows, blk), bf16),
            pltpu.VMEM((n, 16, blk), bf16),
            pltpu.VMEM((n, rows, cols), bf16),
            pltpu.VMEM((n, 2, rows, blk), bf16),
            pltpu.VMEM((n, 2, rows, blk), bf16),
            pltpu.VMEM((n, 2, rows, blk), f32),
            pltpu.VMEM((n, rows, blk), bf16),
            pltpu.VMEM((n, rows, blk), bf16),
            pltpu.VMEM((n, rows, blk), bf16),
            pltpu.VMEM((n, rows, blk), bf16),
            dma((3,)),
            dma((3, n - 1)),
            dma((2,)),
            dma((3, PARTS * n)),
            dma((2,)),
            dma((3, PARTS * n)),
            dma((2,)),
            dma((3, PARTS * n)),
            dma((4,)),
            dma((8,)),
            dma((1,)),
            dma((n - 1,)),
            dma((1,)),
            dma((2,)),
            dma((2,)),
            dma((n,)),
            dma((1,)),
            dma((n,)),
            dma((1,)),
            dma((2, n)),
            dma((3,)),
            dma((4, n)),
        ],
        compiler_params=pltpu.CompilerParams(
            collective_id=0, has_side_effects=True, vmem_limit_bytes=60 * 1024 * 1024
        ),
    )(
        query_first,
        query_second,
        key_first,
        key_second,
        values,
        lambdas.T,
        residual,
        norm_gain,
        out_weight,
        gate_weight,
        up_weight,
        down_weight,
    )

def solution(mesh):
    return jax.shard_map(
        functools.partial(one_device, dict(mesh.shape)),
        mesh=mesh,
        in_specs=(
            P(("grp", "sp"), "tp"),
            P(("grp", "sp"), "tp"),
            P(("grp", "sp"), "tp"),
            P(("grp", "sp"), "tp"),
            P(("grp", "sp"), None, "tp"),
            P(None, "tp"),
            P(("grp", "sp"), "tp"),
            P("tp"),
            P(None, "tp", None),
            P("sp", "tp"),
            P("sp", "tp"),
            P("tp", "sp"),
        ),
        out_specs=P(("grp", "sp"), "tp"),
        check_vma=False,
    )
```

```python
import functools

import jax
import jax.numpy as jnp
from jax import lax
from jax.experimental import pallas as pl
from jax.experimental.pallas import tpu as pltpu
from jax.sharding import PartitionSpec as P

D = 2048


def per_device(
    query_first,
    key_first,
    query_second,
    key_second,
    values,
    lambdas,
    residual,
    norm_gain,
    out_weight,
    gate_weight,
    up_weight,
    down_weight,
):
    tok_rows = query_first.shape[0]
    heads_here = lambdas.shape[1]
    width_first = query_first.shape[1] // (2 * heads_here)
    width_second = query_second.shape[1] // (2 * heads_here)
    value_size = values.shape[2] // heads_here
    offset = lax.axis_index("sp") * tok_rows
    query_pos = offset + lax.broadcasted_iota(jnp.int32, (tok_rows, 1), 0)
    query_groups = (
        query_first.reshape(tok_rows, heads_here, 2, width_first),
        query_second.reshape(tok_rows, heads_here, 2, width_second),
    )
    key_widths = (width_first, width_second)
    start_state = (
        jnp.full((heads_here, 2, tok_rows, 1), -1e30, jnp.float32),
        jnp.zeros((heads_here, 2, tok_rows, 1), jnp.float32),
        jnp.zeros((heads_here, 2, tok_rows, value_size), jnp.float32),
    )
    states = (start_state, start_state)
    pieces = (
        lax.all_gather(key_first, "sp", axis=0, tiled=True),
        lax.all_gather(key_second, "sp", axis=0, tiled=True),
        lax.all_gather(values, "sp", axis=0, tiled=True),
    )
    piece_rows = pieces[0].shape[0]
    key_pos = lax.broadcasted_iota(jnp.int32, (1, piece_rows), 1)
    allowed = key_pos <= query_pos
    value_rows = pieces[2].reshape(piece_rows, 2, heads_here, value_size)
    results = []
    for group_idx in range(2):
        key_width = key_widths[group_idx]
        key_part = pieces[group_idx].reshape(piece_rows, heads_here, 2, key_width)
        scores = jnp.einsum(
            "qhmd,khmd->hmqk", query_groups[group_idx], key_part, preferred_element_type=jnp.float32
        ) * key_width ** (-0.5)
        scores = jnp.where(allowed, scores, -1e30)
        running, totals, weighted = states[group_idx]
        new_peak = jnp.maximum(running, jnp.max(scores, axis=-1, keepdims=True))
        weights = jnp.where(allowed, jnp.exp(scores - new_peak), 0.0)
        totals = jnp.sum(weights, axis=-1, keepdims=True)
        weighted = jnp.einsum(
            "hmqk,khe->hmqe",
            weights.astype(jnp.bfloat16),
            value_rows[:, group_idx],
            preferred_element_type=jnp.float32,
        )
        results.append((new_peak, totals, weighted))
    states = (results[0], results[1])
    map_out = jnp.stack([states[0][2] / states[0][1], states[1][2] / states[1][1]])
    differ = map_out[:, :, 0] - lambdas[:, :, None, None] * map_out[:, :, 1]
    head_scale = lax.rsqrt(jnp.mean(differ * differ, axis=-1, keepdims=True) + 1e-06)
    attended = (0.8 * differ * head_scale).astype(jnp.bfloat16)
    projection = out_weight.reshape(2, heads_here, value_size, out_weight.shape[2])
    mixed_part = jnp.einsum(
        "ghqe,gher->qr", attended, projection, preferred_element_type=jnp.float32
    )
    mixed = lax.psum_scatter(
        mixed_part.astype(jnp.bfloat16), "tp", scatter_dimension=1, tiled=True
    ).astype(jnp.float32)
    stream = residual.astype(jnp.float32) + mixed
    squares = lax.psum(jnp.sum(stream * stream, axis=1), "tp")
    row_scale = lax.rsqrt(squares[:, None] / D + 1e-06)
    normed = (stream * row_scale * norm_gain.astype(jnp.float32)).astype(jnp.bfloat16)
    full_rows = lax.all_gather(normed, "tp", axis=1, tiled=True)
    pieces = (
        lax.all_gather(gate_weight, "sp", axis=0, tiled=True),
        lax.all_gather(up_weight, "sp", axis=0, tiled=True),
    )
    gate = jnp.dot(full_rows, pieces[0], preferred_element_type=jnp.float32)
    up_part = jnp.dot(full_rows, pieces[1], preferred_element_type=jnp.float32)
    hidden = (jax.nn.silu(gate) * up_part).astype(jnp.bfloat16)
    partial_out = jnp.dot(
        hidden,
        lax.all_gather(down_weight, "sp", axis=1, tiled=True),
        preferred_element_type=jnp.float32,
    )
    ffn = lax.psum_scatter(
        partial_out.astype(jnp.bfloat16), "tp", scatter_dimension=1, tiled=True
    ).astype(jnp.float32)
    return (stream + 0.5 * ffn).astype(jnp.bfloat16)


def flip(index, bits):
    bit = 1
    while bit <= bits:
        if (bits // bit) % 2:
            index = index + bit - 2 * bit * ((index // bit) % 2)
        bit *= 2
    return index


def nt_dot(a, b):
    return lax.dot_general(a, b, (((1,), (1,)), ((), ())), preferred_element_type=jnp.float32)


def dot(a, b):
    return jnp.dot(a, b, preferred_element_type=jnp.float32)


def scoped(name):
    return jax.named_scope(name)


PLAN = (
    {
        (1, 0): ((0, 1, 0),),
        (1, 1): ((1, 1, 0), (0, 1, 0)),
        (2, 0): ((0, 2, 1), (1, 2, 0), (0, 2, 0), (1, 2, 1)),
        (2, 1): ((0, 2, 0), (1, 2, 0)),
        (3, 0): ((0, 3, 2), (0, 3, 1), (0, 3, 0)),
        (3, 1): ((0, 3, 2), (0, 3, 1)),
    },
    {
        (0, 1): ((0, 0, 2),),
        (1, 1): ((0, 1, 3),),
        (2, 0): ((2, 3),),
        (2, 1): ((2, 3), (0, 2, 1), (0, 2, 3)),
        (3, 1): ((0, 3, 0),),
    },
    {
        (0, 0): ((1, 0, 1),),
        (1, 0): ((1, 1, 0), (0, 1, 2)),
    },
    {
        (1, 0): ((1, 2, 0), (2, 2)),
        (1, 1): ((0, 1, 2), (0, 2, 0)),
        (2, 0): ((1, 2, 3), (0, 2, 3)),
        (2, 1): ((0, 3, 1),),
    },
    {
        (0, 0): ((0, 0, 1), (2, 1), (3, 1), (5, 0), (0, 0, 2), (0, 0, 3), (1, 0, 3), (5, 1), (2, 2), (4, 2), (1, 0, 2), (2, 3), (4, 1), (4, 3), (3, 2)),
        (0, 1): ((1, 0, 3), (5, 0), (2, 1), (2, 2), (0, 0, 1), (0, 0, 3), (4, 1), (1, 0, 2), (1, 0, 1), (4, 2), (5, 2), (3, 2), (4, 3), (2, 3), (5, 1), (3, 1), (5, 3)),
        (1, 0): ((3, 0), (4, 0), (0, 2, 0), (2, 0), (0, 1, 3), (4, 2), (0, 0, 2), (0, 3, 0), (3, 2), (0, 0, 3), (1, 0, 3), (1, 1, 3), (4, 3), (2, 3), (5, 3), (5, 0), (1, 0, 2), (1, 1, 2), (5, 2), (1, 3, 0)),
        (1, 1): ((4, 0), (2, 2), (0, 0, 2), (2, 3), (1, 0, 3), (1, 2, 0), (2, 0), (4, 2), (0, 0, 3), (4, 3), (5, 1), (1, 0, 2), (5, 2), (1, 1, 3), (0, 3, 0), (3, 0), (5, 0), (5, 3), (1, 3, 0)),
        (2, 0): ((4, 1), (0, 3, 0), (2, 1), (4, 3), (4, 0), (0, 1, 3), (5, 1), (0, 3, 1), (2, 0), (5, 0), (5, 3), (1, 3, 0), (0, 0, 3)),
        (2, 1): ((1, 2, 3), (2, 1), (0, 1, 3), (4, 1), (4, 3), (0, 3, 0), (4, 0), (2, 0), (5, 1), (1, 3, 0), (1, 2, 1), (5, 3), (1, 0, 3), (5, 0), (3, 3), (0, 0, 3), (1, 3, 1), (5, 2), (3, 0)),
        (3, 0): ((2, 2), (3, 2), (1, 3, 0), (5, 3), (1, 3, 2), (4, 1), (4, 0), (1, 3, 1), (2, 1), (4, 2), (5, 2), (2, 0), (5, 1), (5, 0)),
        (3, 1): ((4, 2), (1, 3, 2), (2, 2), (1, 3, 0), (1, 3, 1), (4, 1), (2, 1), (3, 0), (4, 0), (5, 1), (5, 0), (2, 0), (3, 2)),
    },
    {
        (0, 0): ((5, 2), (5, 3)),
        (3, 0): ((3, 0),),
    },
    {
        (2, 1): ((1, 1, 3),),
        (3, 1): ((5, 2),),
    },
    {},
    {
        (1, 1): ((1, 1, 2),),
    },
    {
        (1, 0): ((3, 3), (5, 1)),
        (2, 0): ((1, 3, 1), (3, 3)),
    },
    {
        (0, 1): ((3, 3),),
    },
    {
        (2, 0): ((1, 0, 3),),
        (2, 1): ((3, 1),),
        (3, 0): ((3, 1),),
        (3, 1): ((5, 3), (3, 1)),
    },
    {
        (0, 0): ((3, 3),),
        (2, 0): ((5, 2),),
    },
    {
        (1, 1): ((3, 2), (3, 3)),
        (2, 0): ((1, 1, 3),),
    },
    {},
    {},
    {
        (2, 0): ((3, 0),),
    },
    {},
    {
        (2, 0): ((3, 1),),
    },
    {},
    {},
    {},
    {},
    {},
    {},
    {},
    {},
    {},
    {},
    {},
    {},
    {},
    {},
    {},
    {},
    {},
    {},
    {},
    {},
    {},
    {},
    {},
    {},
    {},
    {},
    {},
)

TAIL = (
    ("hidden", 3),
    ("await_far", 0),
    ("far", 0, 3),
    ("hidden", 2),
    ("cross", 0, 3),
    ("far", 0, 2),
    ("hidden", 1),
    ("cross", 0, 2),
    ("far", 0, 1),
    ("hidden", 0),
    ("cross", 0, 1),
    ("far", 0, 0),
    ("cross", 0, 0),
    ("await_near", 0),
    ("near", 0, 3),
    ("near", 0, 2),
    ("await_far", 1),
    ("far", 1, 3),
    ("far", 1, 2),
    ("cross", 1, 3),
    ("settle", 0, 3),
    ("far", 1, 1),
    ("cross", 1, 2),
    ("far", 1, 0),
    ("cross", 1, 1),
    ("cross", 1, 0),
    ("near", 0, 1),
    ("near", 0, 0),
    ("await_near", 1),
    ("near", 1, 3),
    ("near", 1, 2),
    ("settle", 1, 3),
    ("near", 1, 1),
    ("near", 1, 0),
    ("settle", 0, 2),
    ("settle", 1, 2),
    ("settle", 1, 1),
    ("settle", 1, 0),
    ("settle", 0, 1),
    ("settle", 0, 0),
)

WEIGHTS_IN, DOWN_IN, HAND_IN, HAND_DOWN, ROW, ACROSS = range(6)


PARTS = 2


def transit_slot(here, source, target):
    outer = 0 if source < here else 2
    if outer:
        return outer + (target if here == 2 else source - 2)
    return outer + (target - 2 if here == 1 else source)


def layer_kernel(
    sp_count,
    widths,
    q1_hbm,
    q2_hbm,
    k1_hbm,
    k2_hbm,
    v_hbm,
    lam_hbm,
    residual_hbm,
    gain_hbm,
    proj_hbm,
    gate_ref,
    up_ref,
    down_ref,
    out_ref,
    q1_ref,
    q2_ref,
    k1_ref,
    k2_ref,
    v_ref,
    lam_ref,
    residual_ref,
    gain_ref,
    k1b,
    k2b,
    vb,
    proj_ref,
    peak,
    total,
    acc,
    wg,
    wu,
    wd,
    tg,
    tu,
    td,
    mp,
    rsb,
    mine_ref,
    stream,
    act,
    gains,
    hid,
    c1,
    c1r,
    po,
    c2,
    c2r,
    c3,
    c3r,
    kv_ss,
    kv_rs,
    w_ss,
    w_rs,
    t_ss,
    t_rs,
    f_ss,
    f_rs,
    own_sem,
    in_sem,
    g_ss,
    g_rs,
    rs_ss,
    rs_rs,
    az_ss,
    az_rs,
    ax_ss,
    ax_rs,
    ac_ss,
    ac_rs,
    c_ss,
    c_rs,
):
    s = lax.axis_index("sp")
    t = lax.axis_index("tp")
    y = lax.axis_index("grp")
    rows, blk = residual_ref.shape
    cols = wg.shape[2]
    hidden_all = gate_ref.shape[1]
    xpeer, cpeer, dpeer = flip(t, 2), flip(t, 1), flip(t, 3)
    others = range(1, sp_count)
    everyone = range(sp_count)
    last = sp_count - 1

    def remote(src, dst, ssem, rsem, **where):
        return pltpu.make_async_remote_copy(
            src_ref=src,
            dst_ref=dst,
            send_sem=ssem,
            recv_sem=rsem,
            device_id=where,
            device_id_type=pl.DeviceIdType.MESH,
        )

    def either(test, action):
        pl.when(test)(lambda: action(True))
        pl.when(jnp.logical_not(test))(lambda: action(False))

    barrier = pltpu.get_barrier_semaphore()
    for k in others:
        pl.semaphore_signal(barrier, inc=1, device_id={"sp": flip(s, k)}, device_id_type=pl.DeviceIdType.MESH)
        pl.semaphore_signal(barrier, inc=1, device_id={"tp": flip(t, k)}, device_id_type=pl.DeviceIdType.MESH)
    pl.semaphore_signal(barrier, inc=1, device_id={"grp": 1 - y}, device_id_type=pl.DeviceIdType.MESH)
    inputs = (
        (k1_hbm, k1_ref),
        (k2_hbm, k2_ref),
        (v_hbm, v_ref),
        (q1_hbm, q1_ref),
        (q2_hbm, q2_ref),
        (gain_hbm, gain_ref),
        (lam_hbm, lam_ref),
        (residual_hbm, residual_ref),
    )
    loads = [pltpu.make_async_copy(far, here, in_sem.at[i]) for i, (far, here) in enumerate(inputs)]
    for load in loads:
        load.start()

    half_d = wg.shape[1] // 2
    extra = sp_count * cols - hidden_all
    d_half = pl.ds(pl.multiple_of(y * half_d, half_d), half_d)

    def kv_copies(back):
        pairs = ((k1_ref, k1b), (k2_ref, k2b), (v_ref, vb))
        right = lax.rem(s + 1, sp_count)
        return [
            remote(dst.at[back] if back else src, dst.at[back + 1], kv_ss.at[i], kv_rs.at[i, back], sp=right)
            for i, (src, dst) in enumerate(pairs)
        ]

    def arrived(back):
        pairs = ((k1_ref, k1b), (k2_ref, k2b), (v_ref, vb))
        left = lax.rem(s + sp_count - 1, sp_count)
        return [
            remote(src, dst.at[back], kv_ss.at[i], kv_rs.at[i, back - 1], sp=left)
            for i, (src, dst) in enumerate(pairs)
        ]

    def piece_bounds(target):
        short = target == last
        begin = hidden_all - cols + extra if short else target * cols
        return (begin, extra, cols - extra) if short else (begin, 0, cols)

    def part_rows(kind, target, part, side):
        _, _, size = piece_bounds(target)
        whole = half_d if kind < 2 else size // 2
        rows_here = whole // PARTS
        return pl.multiple_of(side * whole + part * rows_here, 16), rows_here

    def own_piece(kind, target, part):
        src = (gate_ref, up_ref, down_ref)[kind]
        begin, _, size = piece_bounds(target)
        first, count = part_rows(kind, target, part, y)
        if kind < 2:
            return src.at[pl.ds(first, count), pl.ds(begin, size)]
        return src.at[pl.ds(pl.multiple_of(begin + first, 16), count), :]

    def final_place(kind, source, target, part, side):
        dst = (wg, wu, wd)[kind]
        _, skip, size = piece_bounds(target)
        first, count = part_rows(kind, target, part, side)
        if kind < 2:
            return dst.at[source, pl.ds(first, count), pl.ds(skip, size)]
        return dst.at[source, pl.ds(pl.multiple_of(skip + first, 16), count)]

    def transit_place(kind, here, source, target, part):
        buffer = (tg, tu, td)[kind].at[transit_slot(here, source, target)]
        _, _, size = piece_bounds(target)
        first, count = part_rows(kind, target, part, 0)
        return buffer.at[pl.ds(first, count), pl.ds(0, size)] if kind < 2 else buffer.at[pl.ds(first, count)]

    def weight_hop(kind, here, source, target, part):
        there = here + 1 if target > here else here - 1
        if source == here:
            piece, ssem = own_piece(kind, target, part), w_ss.at[kind // 2]
        else:
            piece = transit_place(kind, here, source, target, part)
            ssem = t_ss.at[kind // 2]
        if there == target:
            place, rsem = final_place(kind, source, target, part, y), w_rs.at[kind, PARTS * source + part]
        else:
            place = transit_place(kind, there, source, target, part)
            rsem = t_rs.at[kind, PARTS * transit_slot(there, source, target) + part]
        return remote(piece, place, ssem, rsem, sp=there)

    def move_weights(kinds, here, source, target):
        for kind in kinds:
            for part in range(PARTS):
                if source != here:
                    before = here - 1 if source < here else here + 1
                    with scoped(f"pass{kind}{part}_{source}{target}"):
                        weight_hop(kind, before, source, target, part).wait_recv()
                weight_hop(kind, here, source, target, part).start()

    def weight_hand(kind, source, target, part):
        place = final_place(kind, source, target, part, y)
        return remote(place, place, f_ss.at[kind // 2], f_rs.at[kind, PARTS * source + part], grp=1 - y)

    def hand_over(kinds, here, source):
        for kind in kinds:
            for part in range(PARTS):
                before = here - 1 if source < here else here + 1
                with scoped(f"hand{kind}{part}_{source}"):
                    weight_hop(kind, before, source, here, part).wait_recv()
                weight_hand(kind, source, here, part).start()

    def own_copy(kind, short):
        src, dst = ((gate_ref, wg), (up_ref, wu), (down_ref, wd))[kind]
        begin = hidden_all - cols + extra if short else pl.multiple_of(s * cols, 128)
        skip, size = (extra, cols - extra) if short else (0, cols)
        if kind < 2:
            return pltpu.make_async_copy(src.at[:, pl.ds(begin, size)], dst.at[s, :, pl.ds(skip, size)], own_sem.at[kind])
        return pltpu.make_async_copy(src.at[pl.ds(begin, size), :], dst.at[s, pl.ds(skip, size)], own_sem.at[kind])

    def act_z(row, begin, target, way):
        piece = act.at[t, row]
        return remote(piece, piece, az_ss.at[way], az_rs.at[row], sp=target)

    def along(here, row, action):
        if row <= here < last:
            action(act_z(row, here, here + 1, 0))
        if row >= here > 0:
            action(act_z(row, here, here - 1, 1))

    def act_x(row):
        piece = act.at[t, row]
        return remote(piece, piece, ax_ss.at[0], ax_rs.at[row], tp=xpeer)

    def act_c(row, second):
        piece = act.at[xpeer if second else t, row]
        return remote(piece, piece, ac_ss.at[0], ac_rs.at[second, row], tp=cpeer)

    def start(copy):
        copy.start()

    def perform(here, event):
        kind, index = event[:2]
        if kind == WEIGHTS_IN:
            move_weights((0, 1), here, index, event[2])
        elif kind == DOWN_IN:
            move_weights((2,), here, index, event[2])
        elif kind == HAND_IN:
            hand_over((0, 1), here, index)
        elif kind == HAND_DOWN:
            hand_over((2,), here, index)
        elif kind == ROW:
            with scoped(f"row{index}"):
                act_z(index, here, here, 0).wait_recv()
            send_row(here, index)
        elif kind == ACROSS:
            with scoped(f"across{index}"):
                act_x(index).wait_recv()
            act_c(index, 1).start()

    def send_row(here, row):
        along(here, row, start)
        act_x(row).start()
        act_c(row, 0).start()

    x = t // 2
    steps = iter(PLAN)

    def next_step():
        plan = next(steps)
        for here in everyone:
            lists = [plan.get((here, side), ()) for side in range(2)]
            tests = [(s == here, lists[0])]
            if lists[0] != lists[1]:
                tests = [(jnp.logical_and(s == here, x == side), lists[side]) for side in range(2)]
            for test, events in tests:
                if events:

                    @pl.when(test)
                    def _(here=here, events=events):
                        for event in events:
                            perform(here, event)

    @pl.when(s == last)
    def _():
        wg[:, :, :extra] = jnp.zeros((sp_count, wg.shape[1], extra), jnp.bfloat16)
        wu[:, :, :extra] = jnp.zeros((sp_count, wg.shape[1], extra), jnp.bfloat16)
        wd[:, :extra, :] = jnp.zeros((sp_count, extra, blk), jnp.bfloat16)

    proj_copy = pltpu.make_async_copy(proj_hbm, proj_ref, own_sem.at[3])
    proj_copy.start()

    def start_own(short):
        for kind in range(3):
            own_copy(kind, short).start()

    either(s == last, start_own)

    for load in loads[:-1]:
        load.wait()
    gains[t] = jnp.broadcast_to(gain_ref[...].reshape(1, blk), gains.shape[1:])
    with scoped("barrier"):
        pl.semaphore_wait(barrier, 2 * (sp_count - 1) + 1)
    next_step()

    @pl.when(s < last)
    def _():
        for copy in kv_copies(0):
            copy.start()

    gain_copies = []
    for k in others:
        copy = remote(gains.at[t], gains.at[t], g_ss.at[0], g_rs.at[k - 1], tp=flip(t, k))
        copy.start()
        gain_copies.append(copy)

    q_refs = (q1_ref, q2_ref)
    lane = lax.broadcasted_iota(jnp.int32, (1, 2 * widths[0]), 1)

    def block(keys, v, diagonal):
        for group in range(2):
            width = widths[group]
            values = v[:, group, :]
            for m in range(2):
                if width % 128:
                    span = slice(0, 2 * width)
                    queries = q_refs[group][:, span]
                    queries = jnp.where(lane // width == m, queries.astype(jnp.float32), 0.0).astype(jnp.bfloat16)
                else:
                    span = slice(m * width, (m + 1) * width)
                    queries = q_refs[group][:, span]
                scores = nt_dot(queries, keys[group][:, span]) * width ** (-0.5)
                state = 2 * group + m
                if diagonal:
                    allowed = lax.broadcasted_iota(jnp.int32, (rows, rows), 1) <= lax.broadcasted_iota(
                        jnp.int32, (rows, rows), 0
                    )
                    scores = jnp.where(allowed, scores, -1e30)
                    top = jnp.max(scores, axis=1, keepdims=True)
                    weights = jnp.exp(scores - top)
                    peak[state] = top
                    total[state] = jnp.sum(weights, axis=1, keepdims=True)
                    acc[state] = dot(weights.astype(jnp.bfloat16), values)
                else:
                    before = peak[state]
                    top = jnp.maximum(before, jnp.max(scores, axis=1, keepdims=True))
                    fade = jnp.exp(before - top)
                    weights = jnp.exp(scores - top)
                    peak[state] = top
                    total[state] = total[state] * fade + jnp.sum(weights, axis=1, keepdims=True)
                    acc[state] = acc[state] * fade + dot(weights.astype(jnp.bfloat16), values)

    with scoped("diag"):
        block((k1_ref, k2_ref), v_ref, True)
    for back in others:

        @pl.when(s >= back)
        def _(back=back):
            with scoped(f"kvwait{back}"):
                for i, copy in enumerate(arrived(back)):
                    copy.wait_recv()
                    if back < last:
                        pl.when(s < last)(kv_copies(back)[i].start)
            with scoped(f"block{back}"):
                block((k1b.at[back], k2b.at[back]), vb.at[back], False)

    next_step()
    proj_copy.wait()
    loads[-1].wait()
    with scoped("finish"):
        attended = []
        for group in range(2):
            first = acc[2 * group] / total[2 * group]
            second = acc[2 * group + 1] / total[2 * group + 1]
            differ = first - lam_ref[0, group] * second
            scale = lax.rsqrt(jnp.mean(differ * differ, axis=1, keepdims=True) + 1e-06)
            attended.append((0.8 * differ * scale).astype(jnp.bfloat16))

    def project(owner):
        columns = pl.ds(pl.multiple_of(owner * blk, blk), blk)
        return dot(attended[0], proj_ref[0, :, columns]) + dot(attended[1], proj_ref[1, :, columns])

    with scoped("project"):
        mp[0] = project(cpeer).astype(jnp.bfloat16)
        mp[1] = project(dpeer).astype(jnp.bfloat16)
        to_core = remote(mp.at[pl.ds(0, 2)], rsb.at[pl.ds(0, 2)], rs_ss.at[0], rs_rs.at[0], tp=cpeer)
        to_core.start()
        to_x = remote(mp.at[2], rsb.at[2], rs_ss.at[0], rs_rs.at[1], tp=xpeer)
        mine_ref[1] = project(xpeer)
        mine_ref[0] = residual_ref[...].astype(jnp.float32) + project(t)
    next_step()
    with scoped("rscore"):
        to_core.wait_recv()
    mp[2] = (mine_ref[1] + rsb[1].astype(jnp.float32)).astype(jnp.bfloat16)
    to_x.start()
    mine_ref[0] = mine_ref[0] + rsb[0].astype(jnp.float32)
    next_step()
    with scoped("rsx"):
        to_x.wait_recv()
    stream[...] = mine_ref[0] + rsb[2].astype(jnp.float32)
    act[t, s] = stream[...].astype(jnp.bfloat16)

    for here in everyone:

        @pl.when(s == here)
        def _(here=here):
            send_row(here, here)

    next_step()

    for copy in gain_copies:
        copy.wait_recv()

    def await_weights(kinds, source):
        def go(short):
            for kind in kinds:

                @pl.when(source != s)
                def _(kind=kind):
                    for part in range(PARTS):
                        place = final_place(kind, source, last if short else 0, part, 1 - y)
                        sem = PARTS * source + part
                        remote(place, place, f_ss.at[kind // 2], f_rs.at[kind, sem], grp=1 - y).wait_recv()

                @pl.when(source == s)
                def _(kind=kind):
                    own_copy(kind, short).wait()

        either(s == last, go)

    with scoped("await_gu"):
        for source in everyone:
            await_weights((0, 1), source)
    column = jnp.minimum(s * cols, hidden_all - cols) + lax.broadcasted_iota(jnp.int32, (1, cols), 1)
    mine = column >= s * cols

    def hidden_of(k):
        row = flip(s, k)
        with scoped(f"acwait{k}"):
            act_c(row, 0).wait_recv()
            act_c(row, 1).wait_recv()
        with scoped(f"hidden{k}"):
            squares = jnp.zeros((rows, 1), jnp.float32)
            for part in range(sp_count):
                piece = act[part, row].astype(jnp.float32)
                squares = squares + jnp.sum(piece * piece, axis=1, keepdims=True)
            scale = lax.rsqrt(squares / (sp_count * blk) + 1e-06)
            gate = jnp.zeros((rows, cols), jnp.float32)
            up = jnp.zeros((rows, cols), jnp.float32)
            for part in range(sp_count):
                gain = gains[part, 0:1, :].astype(jnp.float32)
                normed = (act[part, row].astype(jnp.float32) * scale * gain).astype(jnp.bfloat16)
                gate = gate + dot(normed, wg[part])
                up = up + dot(normed, wu[part])
            hidden = gate / (1.0 + jnp.exp(-gate)) * up
            hid[k] = jnp.where(mine, hidden, 0.0).astype(jnp.bfloat16)

    core = t % 2
    half_rows = rows // 2
    r1, r2, r3 = {}, {}, {}
    for k in everyone:
        for far in range(2):
            r1[k, far] = remote(c1.at[k, far], c1r.at[k, far], c_ss.at[0], c_rs.at[far, k], tp=cpeer)
        for h in range(2):
            some = pl.ds(h * half_rows, half_rows)
            r2[k, h] = remote(c2.at[k, some], c2r.at[k, some], c_ss.at[1], c_rs.at[2 + h, k], tp=xpeer)
            if k:
                target = flip(s, 1 if k == 3 else k)
                r3[k, h] = remote(c3.at[k, some], c3r.at[k, some], c_ss.at[2], c_rs.at[4 + h, k], sp=target)

    def block_of(wave, far):
        return 2 * ((1 - x) if far else x) + wave

    def product(wave, k, far):
        with scoped(f"product{wave}{k}{far}"):
            value = dot(hid[k], wd[block_of(wave, far)])

            @pl.when(core == wave)
            def _():
                po[k, far] = value

            @pl.when(core != wave)
            def _():
                c1[k, far] = value.astype(jnp.bfloat16)
                r1[k, far].start()

    def to_other_chip(wave, k):
        @pl.when(core == wave)
        def _():
            with scoped(f"cross{wave}{k}"):
                r1[k, 1].wait_recv()
            for h in range(2):
                some = pl.ds(h * half_rows, half_rows)
                c2[k, some] = (po[k, 1, some] + c1r[k, 1, some].astype(jnp.float32)).astype(jnp.bfloat16)
                r2[k, h].start()

    def settle(wave, k):
        @pl.when(core == wave)
        def _():
            with scoped(f"settle{wave}{k}"):
                r1[k, 0].wait_recv()
            for h in range(2):
                some = pl.ds(h * half_rows, half_rows)
                with scoped(f"settle{wave}{k}{h}"):
                    r2[k, h].wait_recv()
                result = po[k, 0, some] + c1r[k, 0, some].astype(jnp.float32) + c2r[k, some].astype(jnp.float32)
                if k == 2:
                    with scoped(f"pair{wave}{h}"):
                        r3[3, h].wait_recv()
                    result = result + c3r[3, some].astype(jnp.float32)
                if k:
                    c3[k, some] = result.astype(jnp.bfloat16)
                    r3[k, h].start()
                else:
                    po[0, 0, some] = result

    for name, *where in TAIL:
        next_step()
        if name == "hidden":
            hidden_of(where[0])
        elif name in ("far", "near"):
            product(*where, far=int(name == "far"))
        elif name == "cross":
            to_other_chip(*where)
        elif name == "settle":
            settle(*where)
        else:
            with scoped(f"{name}{where[0]}"):
                await_weights((2,), block_of(where[0], name == "await_far"))

    next_step()
    for h in range(2):
        some = pl.ds(h * half_rows, half_rows)
        for k in (1, 2):
            with scoped(f"r3_{k}{h}"):
                r3[k, h].wait_recv()
        ffn = po[0, 0, some] + c3r[1, some].astype(jnp.float32) + c3r[2, some].astype(jnp.float32)
        out_ref[some, :] = (stream[some, :] + 0.5 * ffn).astype(jnp.bfloat16)

    def sent(ref, sem):
        remote(ref, ref, sem, rs_rs.at[0], tp=cpeer).wait_send()

    def weights_sent(sems, width):
        sent(gate_ref.at[:, pl.ds(0, width)], sems.at[0])
        sent(down_ref.at[pl.ds(0, width // 2), :], sems.at[1])

    def width_of(target):
        return piece_bounds(target)[2]

    with scoped("drain"):
        for here in everyone:

            @pl.when(s == here)
            def _(here=here):
                if here < last:
                    for i, buffer in enumerate((k1b, k2b, vb)):
                        sent(buffer.at[pl.ds(0, here + 1)], kv_ss.at[i])
                    sent(act.at[0, pl.ds(0, here + 1)], az_ss.at[0])
                if here:
                    sent(act.at[0, pl.ds(0, sp_count - here)], az_ss.at[1])
                weights_sent(w_ss, sum(width_of(there) for there in everyone if there != here))
                weights_sent(f_ss, (sp_count - 1) * width_of(here))
                through = [
                    width_of(target)
                    for source in everyone
                    for target in everyone
                    if min(source, target) < here < max(source, target)
                ]
                if through:
                    weights_sent(t_ss, sum(through))

        sent(act.at[0], ax_ss.at[0])
        sent(act.at[pl.ds(0, 2)], ac_ss.at[0])
        sent(gains.at[pl.ds(0, sp_count - 1)], g_ss.at[0])
        sent(mp, rs_ss.at[0])
        sent(c1, c_ss.at[0])
        sent(c2, c_ss.at[1])
        sent(c3.at[pl.ds(0, sp_count - 1)], c_ss.at[2])


def fits(axes, query_first, values, lambdas, residual, gate_weight):
    sp, tp = axes["sp"], axes["tp"]
    rows, blk = residual.shape
    depth, hidden_all = gate_weight.shape
    if axes["grp"] != 2 or sp != tp or tp != 4 or lambdas.shape[1] != 1:
        return False
    if depth != blk or blk % 128 or hidden_all % 128 or rows % 16:
        return False
    if (2 * query_first.shape[1]) % 256 or values.shape[2] % 128:
        return False
    cols = -(-hidden_all // (128 * sp)) * 128
    if cols * sp - hidden_all >= cols or cols > hidden_all:
        return False
    if (cols * sp - hidden_all) % 128 or blk % 64 or rows % 32:
        return False
    need = 6 * sp * blk * cols + rows * blk * 2 * 20 * sp
    return need < 40 * 1024 * 1024


def one_device(
    axes,
    query_first,
    key_first,
    query_second,
    key_second,
    values,
    lambdas,
    residual,
    norm_gain,
    out_weight,
    gate_weight,
    up_weight,
    down_weight,
):
    if not fits(axes, query_first, values, lambdas, residual, gate_weight):
        return per_device(
            query_first,
            key_first,
            query_second,
            key_second,
            values,
            lambdas,
            residual,
            norm_gain,
            out_weight,
            gate_weight,
            up_weight,
            down_weight,
        )
    n = axes["sp"]
    rows, blk = residual.shape
    hidden_all = gate_weight.shape[1]
    cols = -(-hidden_all // (128 * n)) * 128
    value_size = values.shape[2]
    widths = (query_first.shape[1] // 2, query_second.shape[1] // 2)
    bf16, f32 = jnp.bfloat16, jnp.float32
    vmem = pl.BlockSpec(memory_space=pltpu.VMEM)
    hbm = pl.BlockSpec(memory_space=pl.ANY)
    dma = pltpu.SemaphoreType.DMA
    return pl.pallas_call(
        functools.partial(layer_kernel, n, widths),
        out_shape=jax.ShapeDtypeStruct((rows, blk), bf16),
        in_specs=[hbm] * 12,
        out_specs=vmem,
        scratch_shapes=[
            pltpu.VMEM(query_first.shape, bf16),
            pltpu.VMEM(query_second.shape, bf16),
            pltpu.VMEM(key_first.shape, bf16),
            pltpu.VMEM(key_second.shape, bf16),
            pltpu.VMEM(values.shape, bf16),
            pltpu.SMEM(lambdas.T.shape, f32),
            pltpu.VMEM(residual.shape, bf16),
            pltpu.VMEM(norm_gain.shape, bf16),
            pltpu.VMEM((n,) + key_first.shape, bf16),
            pltpu.VMEM((n,) + key_second.shape, bf16),
            pltpu.VMEM((n,) + values.shape, bf16),
            pltpu.VMEM(out_weight.shape, bf16),
            pltpu.VMEM((4, rows, 1), f32),
            pltpu.VMEM((4, rows, 1), f32),
            pltpu.VMEM((4, rows, value_size), f32),
            pltpu.VMEM((n, blk, cols), bf16),
            pltpu.VMEM((n, blk, cols), bf16),
            pltpu.VMEM((n, cols, blk), bf16),
            pltpu.VMEM((4, blk // 2, cols), bf16),
            pltpu.VMEM((4, blk // 2, cols), bf16),
            pltpu.VMEM((4, cols // 2, blk), bf16),
            pltpu.VMEM((3, rows, blk), bf16),
            pltpu.VMEM((3, rows, blk), bf16),
            pltpu.VMEM((2, rows, blk), f32),
            pltpu.VMEM((rows, blk), f32),
            pltpu.VMEM((n, n, rows, blk), bf16),
            pltpu.VMEM((n, 16, blk), bf16),
            pltpu.VMEM((n, rows, cols), bf16),
            pltpu.VMEM((n, 2, rows, blk), bf16),
            pltpu.VMEM((n, 2, rows, blk), bf16),
            pltpu.VMEM((n, 2, rows, blk), f32),
            pltpu.VMEM((n, rows, blk), bf16),
            pltpu.VMEM((n, rows, blk), bf16),
            pltpu.VMEM((n, rows, blk), bf16),
            pltpu.VMEM((n, rows, blk), bf16),
            dma((3,)),
            dma((3, n - 1)),
            dma((2,)),
            dma((3, PARTS * n)),
            dma((2,)),
            dma((3, PARTS * n)),
            dma((2,)),
            dma((3, PARTS * n)),
            dma((4,)),
            dma((8,)),
            dma((1,)),
            dma((n - 1,)),
            dma((1,)),
            dma((2,)),
            dma((2,)),
            dma((n,)),
            dma((1,)),
            dma((n,)),
            dma((1,)),
            dma((2, n)),
            dma((3,)),
            dma((6, n)),
        ],
        compiler_params=pltpu.CompilerParams(
            collective_id=0, has_side_effects=True, vmem_limit_bytes=60 * 1024 * 1024
        ),
    )(
        query_first,
        query_second,
        key_first,
        key_second,
        values,
        lambdas.T,
        residual,
        norm_gain,
        out_weight,
        gate_weight,
        up_weight,
        down_weight,
    )

def solution(mesh):
    return jax.shard_map(
        functools.partial(one_device, dict(mesh.shape)),
        mesh=mesh,
        in_specs=(
            P(("grp", "sp"), "tp"),
            P(("grp", "sp"), "tp"),
            P(("grp", "sp"), "tp"),
            P(("grp", "sp"), "tp"),
            P(("grp", "sp"), None, "tp"),
            P(None, "tp"),
            P(("grp", "sp"), "tp"),
            P("tp"),
            P(None, "tp", None),
            P("sp", "tp"),
            P("sp", "tp"),
            P("tp", "sp"),
        ),
        out_specs=P(("grp", "sp"), "tp"),
        check_vma=False,
    )
```

```python
import functools

import jax
import jax.numpy as jnp
from jax import lax
from jax.experimental import pallas as pl
from jax.experimental.pallas import tpu as pltpu
from jax.sharding import PartitionSpec as P

D = 2048


def per_device(
    query_first,
    key_first,
    query_second,
    key_second,
    values,
    lambdas,
    residual,
    norm_gain,
    out_weight,
    gate_weight,
    up_weight,
    down_weight,
):
    tok_rows = query_first.shape[0]
    heads_here = lambdas.shape[1]
    width_first = query_first.shape[1] // (2 * heads_here)
    width_second = query_second.shape[1] // (2 * heads_here)
    value_size = values.shape[2] // heads_here
    offset = lax.axis_index("sp") * tok_rows
    query_pos = offset + lax.broadcasted_iota(jnp.int32, (tok_rows, 1), 0)
    query_groups = (
        query_first.reshape(tok_rows, heads_here, 2, width_first),
        query_second.reshape(tok_rows, heads_here, 2, width_second),
    )
    key_widths = (width_first, width_second)
    start_state = (
        jnp.full((heads_here, 2, tok_rows, 1), -1e30, jnp.float32),
        jnp.zeros((heads_here, 2, tok_rows, 1), jnp.float32),
        jnp.zeros((heads_here, 2, tok_rows, value_size), jnp.float32),
    )
    states = (start_state, start_state)
    pieces = (
        lax.all_gather(key_first, "sp", axis=0, tiled=True),
        lax.all_gather(key_second, "sp", axis=0, tiled=True),
        lax.all_gather(values, "sp", axis=0, tiled=True),
    )
    piece_rows = pieces[0].shape[0]
    key_pos = lax.broadcasted_iota(jnp.int32, (1, piece_rows), 1)
    allowed = key_pos <= query_pos
    value_rows = pieces[2].reshape(piece_rows, 2, heads_here, value_size)
    results = []
    for group_idx in range(2):
        key_width = key_widths[group_idx]
        key_part = pieces[group_idx].reshape(piece_rows, heads_here, 2, key_width)
        scores = jnp.einsum(
            "qhmd,khmd->hmqk", query_groups[group_idx], key_part, preferred_element_type=jnp.float32
        ) * key_width ** (-0.5)
        scores = jnp.where(allowed, scores, -1e30)
        running, totals, weighted = states[group_idx]
        new_peak = jnp.maximum(running, jnp.max(scores, axis=-1, keepdims=True))
        weights = jnp.where(allowed, jnp.exp(scores - new_peak), 0.0)
        totals = jnp.sum(weights, axis=-1, keepdims=True)
        weighted = jnp.einsum(
            "hmqk,khe->hmqe",
            weights.astype(jnp.bfloat16),
            value_rows[:, group_idx],
            preferred_element_type=jnp.float32,
        )
        results.append((new_peak, totals, weighted))
    states = (results[0], results[1])
    map_out = jnp.stack([states[0][2] / states[0][1], states[1][2] / states[1][1]])
    differ = map_out[:, :, 0] - lambdas[:, :, None, None] * map_out[:, :, 1]
    head_scale = lax.rsqrt(jnp.mean(differ * differ, axis=-1, keepdims=True) + 1e-06)
    attended = (0.8 * differ * head_scale).astype(jnp.bfloat16)
    projection = out_weight.reshape(2, heads_here, value_size, out_weight.shape[2])
    mixed_part = jnp.einsum(
        "ghqe,gher->qr", attended, projection, preferred_element_type=jnp.float32
    )
    mixed = lax.psum_scatter(
        mixed_part.astype(jnp.bfloat16), "tp", scatter_dimension=1, tiled=True
    ).astype(jnp.float32)
    stream = residual.astype(jnp.float32) + mixed
    squares = lax.psum(jnp.sum(stream * stream, axis=1), "tp")
    row_scale = lax.rsqrt(squares[:, None] / D + 1e-06)
    normed = (stream * row_scale * norm_gain.astype(jnp.float32)).astype(jnp.bfloat16)
    full_rows = lax.all_gather(normed, "tp", axis=1, tiled=True)
    pieces = (
        lax.all_gather(gate_weight, "sp", axis=0, tiled=True),
        lax.all_gather(up_weight, "sp", axis=0, tiled=True),
    )
    gate = jnp.dot(full_rows, pieces[0], preferred_element_type=jnp.float32)
    up_part = jnp.dot(full_rows, pieces[1], preferred_element_type=jnp.float32)
    hidden = (jax.nn.silu(gate) * up_part).astype(jnp.bfloat16)
    partial_out = jnp.dot(
        hidden,
        lax.all_gather(down_weight, "sp", axis=1, tiled=True),
        preferred_element_type=jnp.float32,
    )
    ffn = lax.psum_scatter(
        partial_out.astype(jnp.bfloat16), "tp", scatter_dimension=1, tiled=True
    ).astype(jnp.float32)
    return (stream + 0.5 * ffn).astype(jnp.bfloat16)


def flip(index, bits):
    bit = 1
    while bit <= bits:
        if (bits // bit) % 2:
            index = index + bit - 2 * bit * ((index // bit) % 2)
        bit *= 2
    return index


def nt_dot(a, b):
    return lax.dot_general(a, b, (((1,), (1,)), ((), ())), preferred_element_type=jnp.float32)


def dot(a, b):
    return jnp.dot(a, b, preferred_element_type=jnp.float32)


def scoped(name):
    return jax.named_scope(name)


PLAN = (
    {
        (1, 0): ((0, 1, 0),),
        (1, 1): ((1, 1, 0), (0, 1, 0)),
        (2, 0): ((0, 2, 1), (1, 2, 0), (0, 2, 0), (1, 2, 1)),
        (2, 1): ((0, 2, 0), (1, 2, 0)),
        (3, 0): ((0, 3, 2), (0, 3, 1), (0, 3, 0)),
        (3, 1): ((0, 3, 2), (0, 3, 1)),
    },
    {
        (0, 1): ((0, 0, 2),),
        (1, 1): ((0, 1, 3),),
        (2, 0): ((2, 3),),
        (2, 1): ((2, 3), (0, 2, 1), (0, 2, 3)),
        (3, 1): ((0, 3, 0),),
    },
    {
        (0, 0): ((1, 0, 1),),
        (1, 0): ((1, 1, 0), (0, 1, 2)),
    },
    {
        (1, 0): ((1, 2, 0), (2, 2)),
        (1, 1): ((0, 1, 2), (0, 2, 0)),
        (2, 0): ((1, 2, 3), (0, 2, 3)),
        (2, 1): ((0, 3, 1),),
    },
    {
        (0, 0): ((0, 0, 1), (2, 1), (3, 1), (5, 0), (0, 0, 2), (0, 0, 3), (1, 0, 3), (5, 1), (2, 2), (4, 2), (1, 0, 2), (2, 3), (4, 1), (4, 3), (3, 2)),
        (0, 1): ((1, 0, 3), (5, 0), (2, 1), (2, 2), (0, 0, 1), (0, 0, 3), (4, 1), (1, 0, 2), (1, 0, 1), (4, 2), (5, 2), (3, 2), (4, 3), (2, 3), (5, 1), (3, 1), (5, 3)),
        (1, 0): ((3, 0), (4, 0), (0, 2, 0), (2, 0), (0, 1, 3), (4, 2), (0, 0, 2), (0, 3, 0), (3, 2), (0, 0, 3), (1, 0, 3), (1, 1, 3), (4, 3), (2, 3), (5, 3), (5, 0), (1, 0, 2), (1, 1, 2), (5, 2), (1, 3, 0)),
        (1, 1): ((4, 0), (2, 2), (0, 0, 2), (2, 3), (1, 0, 3), (1, 2, 0), (2, 0), (4, 2), (0, 0, 3), (4, 3), (5, 1), (1, 0, 2), (5, 2), (1, 1, 3), (0, 3, 0), (3, 0), (5, 0), (5, 3), (1, 3, 0)),
        (2, 0): ((4, 1), (0, 3, 0), (2, 1), (4, 3), (4, 0), (0, 1, 3), (5, 1), (0, 3, 1), (2, 0), (5, 0), (5, 3), (1, 3, 0), (0, 0, 3)),
        (2, 1): ((1, 2, 3), (2, 1), (0, 1, 3), (4, 1), (4, 3), (0, 3, 0), (4, 0), (2, 0), (5, 1), (1, 3, 0), (1, 2, 1), (5, 3), (1, 0, 3), (5, 0), (3, 3), (0, 0, 3), (1, 3, 1), (5, 2), (3, 0)),
        (3, 0): ((2, 2), (3, 2), (1, 3, 0), (5, 3), (1, 3, 2), (4, 1), (4, 0), (1, 3, 1), (2, 1), (4, 2), (5, 2), (2, 0), (5, 1), (5, 0)),
        (3, 1): ((4, 2), (1, 3, 2), (2, 2), (1, 3, 0), (1, 3, 1), (4, 1), (2, 1), (3, 0), (4, 0), (5, 1), (5, 0), (2, 0), (3, 2)),
    },
    {
        (0, 0): ((5, 2), (5, 3)),
        (3, 0): ((3, 0),),
    },
    {
        (2, 1): ((1, 1, 3),),
        (3, 1): ((5, 2),),
    },
    {},
    {
        (1, 1): ((1, 1, 2),),
    },
    {
        (1, 0): ((3, 3), (5, 1)),
        (2, 0): ((1, 3, 1), (3, 3)),
    },
    {
        (0, 1): ((3, 3),),
    },
    {
        (2, 0): ((1, 0, 3),),
        (2, 1): ((3, 1),),
        (3, 0): ((3, 1),),
        (3, 1): ((5, 3), (3, 1)),
    },
    {
        (0, 0): ((3, 3),),
        (2, 0): ((5, 2),),
    },
    {
        (1, 1): ((3, 2), (3, 3)),
        (2, 0): ((1, 1, 3),),
    },
    {},
    {},
    {
        (2, 0): ((3, 0),),
    },
    {},
    {
        (2, 0): ((3, 1),),
    },
    {},
    {},
    {},
    {},
    {},
    {},
    {},
    {},
    {},
    {},
    {},
    {},
    {},
    {},
    {},
    {},
    {},
    {},
    {},
    {},
    {},
    {},
    {},
    {},
    {},
    {},
    {},
)

TAIL = (
    ("hidden", 3),
    ("await_far", 0),
    ("far", 0, 3),
    ("hidden", 2),
    ("cross", 0, 3),
    ("far", 0, 2),
    ("hidden", 1),
    ("cross", 0, 2),
    ("far", 0, 1),
    ("hidden", 0),
    ("cross", 0, 1),
    ("far", 0, 0),
    ("cross", 0, 0),
    ("await_near", 0),
    ("near", 0, 3),
    ("near", 0, 2),
    ("await_far", 1),
    ("far", 1, 3),
    ("far", 1, 2),
    ("cross", 1, 3),
    ("settle", 0, 3),
    ("far", 1, 1),
    ("cross", 1, 2),
    ("far", 1, 0),
    ("cross", 1, 1),
    ("cross", 1, 0),
    ("near", 0, 1),
    ("near", 0, 0),
    ("await_near", 1),
    ("near", 1, 3),
    ("near", 1, 2),
    ("settle", 1, 3),
    ("near", 1, 1),
    ("near", 1, 0),
    ("settle", 0, 2),
    ("settle", 1, 2),
    ("settle", 1, 1),
    ("settle", 1, 0),
    ("settle", 0, 1),
    ("settle", 0, 0),
)

WEIGHTS_IN, DOWN_IN, HAND_IN, HAND_DOWN, ROW, ACROSS = range(6)


PARTS = 2


def transit_slot(here, source, target):
    outer = 0 if source < here else 2
    if outer:
        return outer + (target if here == 2 else source - 2)
    return outer + (target - 2 if here == 1 else source)


def layer_kernel(
    sp_count,
    widths,
    q1_hbm,
    q2_hbm,
    k1_hbm,
    k2_hbm,
    v_hbm,
    lam_hbm,
    residual_hbm,
    gain_hbm,
    proj_hbm,
    gate_ref,
    up_ref,
    down_ref,
    out_ref,
    q1_ref,
    q2_ref,
    k1_ref,
    k2_ref,
    v_ref,
    lam_ref,
    residual_ref,
    gain_ref,
    k1b,
    k2b,
    vb,
    proj_ref,
    peak,
    total,
    acc,
    wg,
    wu,
    wd,
    tg,
    tu,
    td,
    mp,
    rsb,
    mine_ref,
    stream,
    act,
    gains,
    hid,
    c1,
    c1r,
    po,
    c2,
    c2r,
    c3,
    c3r,
    kv_ss,
    kv_rs,
    w_ss,
    w_rs,
    t_ss,
    t_rs,
    f_ss,
    f_rs,
    own_sem,
    in_sem,
    g_ss,
    g_rs,
    rs_ss,
    rs_rs,
    az_ss,
    az_rs,
    ax_ss,
    ax_rs,
    ac_ss,
    ac_rs,
    c_ss,
    c_rs,
):
    s = lax.axis_index("sp")
    t = lax.axis_index("tp")
    y = lax.axis_index("grp")
    rows, blk = residual_ref.shape
    cols = wg.shape[2]
    hidden_all = gate_ref.shape[1]
    xpeer, cpeer, dpeer = flip(t, 2), flip(t, 1), flip(t, 3)
    others = range(1, sp_count)
    everyone = range(sp_count)
    last = sp_count - 1

    def remote(src, dst, ssem, rsem, **where):
        return pltpu.make_async_remote_copy(
            src_ref=src,
            dst_ref=dst,
            send_sem=ssem,
            recv_sem=rsem,
            device_id=where,
            device_id_type=pl.DeviceIdType.MESH,
        )

    def either(test, action):
        pl.when(test)(lambda: action(True))
        pl.when(jnp.logical_not(test))(lambda: action(False))

    barrier = pltpu.get_barrier_semaphore()
    for k in others:
        pl.semaphore_signal(barrier, inc=1, device_id={"tp": flip(t, k)}, device_id_type=pl.DeviceIdType.MESH)
    pl.semaphore_signal(barrier, inc=1, device_id={"grp": 1 - y}, device_id_type=pl.DeviceIdType.MESH)
    for step, inside in ((1, s < last), (-1, s > 0)):

        @pl.when(inside)
        def _(step=step):
            pl.semaphore_signal(barrier, inc=1, device_id={"sp": s + step}, device_id_type=pl.DeviceIdType.MESH)

    inputs = (
        (k1_hbm, k1_ref),
        (k2_hbm, k2_ref),
        (v_hbm, v_ref),
        (q1_hbm, q1_ref),
        (q2_hbm, q2_ref),
        (gain_hbm, gain_ref),
        (lam_hbm, lam_ref),
        (residual_hbm, residual_ref),
    )
    loads = [pltpu.make_async_copy(far, here, in_sem.at[i]) for i, (far, here) in enumerate(inputs)]
    for load in loads:
        load.start()

    half_d = wg.shape[1] // 2
    extra = sp_count * cols - hidden_all
    d_half = pl.ds(pl.multiple_of(y * half_d, half_d), half_d)

    def kv_copies(back):
        pairs = ((k1_ref, k1b), (k2_ref, k2b), (v_ref, vb))
        right = lax.rem(s + 1, sp_count)
        return [
            remote(dst.at[back] if back else src, dst.at[back + 1], kv_ss.at[i], kv_rs.at[i, back], sp=right)
            for i, (src, dst) in enumerate(pairs)
        ]

    def arrived(back):
        pairs = ((k1_ref, k1b), (k2_ref, k2b), (v_ref, vb))
        left = lax.rem(s + sp_count - 1, sp_count)
        return [
            remote(src, dst.at[back], kv_ss.at[i], kv_rs.at[i, back - 1], sp=left)
            for i, (src, dst) in enumerate(pairs)
        ]

    def piece_bounds(target):
        short = target == last
        begin = hidden_all - cols + extra if short else target * cols
        return (begin, extra, cols - extra) if short else (begin, 0, cols)

    def part_rows(kind, target, part, side):
        _, _, size = piece_bounds(target)
        whole = half_d if kind < 2 else size // 2
        rows_here = whole // PARTS
        return pl.multiple_of(side * whole + part * rows_here, 16), rows_here

    def own_piece(kind, target, part):
        src = (gate_ref, up_ref, down_ref)[kind]
        begin, _, size = piece_bounds(target)
        first, count = part_rows(kind, target, part, y)
        if kind < 2:
            return src.at[pl.ds(first, count), pl.ds(begin, size)]
        return src.at[pl.ds(pl.multiple_of(begin + first, 16), count), :]

    def final_place(kind, source, target, part, side):
        dst = (wg, wu, wd)[kind]
        _, skip, size = piece_bounds(target)
        first, count = part_rows(kind, target, part, side)
        if kind < 2:
            return dst.at[source, pl.ds(first, count), pl.ds(skip, size)]
        return dst.at[source, pl.ds(pl.multiple_of(skip + first, 16), count)]

    def transit_place(kind, here, source, target, part):
        buffer = (tg, tu, td)[kind].at[transit_slot(here, source, target)]
        _, _, size = piece_bounds(target)
        first, count = part_rows(kind, target, part, 0)
        return buffer.at[pl.ds(first, count), pl.ds(0, size)] if kind < 2 else buffer.at[pl.ds(first, count)]

    def weight_hop(kind, here, source, target, part):
        there = here + 1 if target > here else here - 1
        if source == here:
            piece, ssem = own_piece(kind, target, part), w_ss.at[kind // 2]
        else:
            piece = transit_place(kind, here, source, target, part)
            ssem = t_ss.at[kind // 2]
        if there == target:
            place, rsem = final_place(kind, source, target, part, y), w_rs.at[kind, PARTS * source + part]
        else:
            place = transit_place(kind, there, source, target, part)
            rsem = t_rs.at[kind, PARTS * transit_slot(there, source, target) + part]
        return remote(piece, place, ssem, rsem, sp=there)

    def move_weights(kinds, here, source, target):
        for kind in kinds:
            for part in range(PARTS):
                if source != here:
                    before = here - 1 if source < here else here + 1
                    with scoped(f"pass{kind}{part}_{source}{target}"):
                        weight_hop(kind, before, source, target, part).wait_recv()
                weight_hop(kind, here, source, target, part).start()

    def weight_hand(kind, source, target, part):
        place = final_place(kind, source, target, part, y)
        return remote(place, place, f_ss.at[kind // 2], f_rs.at[kind, PARTS * source + part], grp=1 - y)

    def hand_over(kinds, here, source):
        for kind in kinds:
            for part in range(PARTS):
                before = here - 1 if source < here else here + 1
                with scoped(f"hand{kind}{part}_{source}"):
                    weight_hop(kind, before, source, here, part).wait_recv()
                weight_hand(kind, source, here, part).start()

    def own_copy(kind, short):
        src, dst = ((gate_ref, wg), (up_ref, wu), (down_ref, wd))[kind]
        begin = hidden_all - cols + extra if short else pl.multiple_of(s * cols, 128)
        skip, size = (extra, cols - extra) if short else (0, cols)
        if kind < 2:
            return pltpu.make_async_copy(src.at[:, pl.ds(begin, size)], dst.at[s, :, pl.ds(skip, size)], own_sem.at[kind])
        return pltpu.make_async_copy(src.at[pl.ds(begin, size), :], dst.at[s, pl.ds(skip, size)], own_sem.at[kind])

    def act_z(row, begin, target, way):
        piece = act.at[t, row]
        return remote(piece, piece, az_ss.at[way], az_rs.at[row], sp=target)

    def along(here, row, action):
        if row <= here < last:
            action(act_z(row, here, here + 1, 0))
        if row >= here > 0:
            action(act_z(row, here, here - 1, 1))

    def act_x(row):
        piece = act.at[t, row]
        return remote(piece, piece, ax_ss.at[0], ax_rs.at[row], tp=xpeer)

    def act_c(row, second):
        piece = act.at[xpeer if second else t, row]
        return remote(piece, piece, ac_ss.at[0], ac_rs.at[second, row], tp=cpeer)

    def start(copy):
        copy.start()

    def perform(here, event):
        kind, index = event[:2]
        if kind == WEIGHTS_IN:
            move_weights((0, 1), here, index, event[2])
        elif kind == DOWN_IN:
            move_weights((2,), here, index, event[2])
        elif kind == HAND_IN:
            hand_over((0, 1), here, index)
        elif kind == HAND_DOWN:
            hand_over((2,), here, index)
        elif kind == ROW:
            with scoped(f"row{index}"):
                act_z(index, here, here, 0).wait_recv()
            send_row(here, index)
        elif kind == ACROSS:
            with scoped(f"across{index}"):
                act_x(index).wait_recv()
            act_c(index, 1).start()

    def send_row(here, row):
        along(here, row, start)
        act_x(row).start()
        act_c(row, 0).start()

    x = t // 2
    steps = iter(PLAN)

    def next_step():
        plan = next(steps)
        for here in everyone:
            lists = [plan.get((here, side), ()) for side in range(2)]
            tests = [(s == here, lists[0])]
            if lists[0] != lists[1]:
                tests = [(jnp.logical_and(s == here, x == side), lists[side]) for side in range(2)]
            for test, events in tests:
                if events:

                    @pl.when(test)
                    def _(here=here, events=events):
                        for event in events:
                            perform(here, event)

    @pl.when(s == last)
    def _():
        wg[:, :, :extra] = jnp.zeros((sp_count, wg.shape[1], extra), jnp.bfloat16)
        wu[:, :, :extra] = jnp.zeros((sp_count, wg.shape[1], extra), jnp.bfloat16)
        wd[:, :extra, :] = jnp.zeros((sp_count, extra, blk), jnp.bfloat16)

    proj_copy = pltpu.make_async_copy(proj_hbm, proj_ref, own_sem.at[3])
    proj_copy.start()

    def start_own(short):
        for kind in range(3):
            own_copy(kind, short).start()

    either(s == last, start_own)

    for load in loads[:-1]:
        load.wait()
    gains[t] = jnp.broadcast_to(gain_ref[...].reshape(1, blk), gains.shape[1:])
    with scoped("barrier"):
        ends = jnp.logical_or(s == 0, s == last)
        pl.semaphore_wait(barrier, jnp.where(ends, sp_count + 1, sp_count + 2))
    next_step()

    @pl.when(s < last)
    def _():
        for copy in kv_copies(0):
            copy.start()

    gain_copies = []
    for k in others:
        copy = remote(gains.at[t], gains.at[t], g_ss.at[0], g_rs.at[k - 1], tp=flip(t, k))
        copy.start()
        gain_copies.append(copy)

    q_refs = (q1_ref, q2_ref)
    lane = lax.broadcasted_iota(jnp.int32, (1, 2 * widths[0]), 1)

    def block(keys, v, diagonal):
        for group in range(2):
            width = widths[group]
            values = v[:, group, :]
            for m in range(2):
                if width % 128:
                    span = slice(0, 2 * width)
                    queries = q_refs[group][:, span]
                    queries = jnp.where(lane // width == m, queries.astype(jnp.float32), 0.0).astype(jnp.bfloat16)
                else:
                    span = slice(m * width, (m + 1) * width)
                    queries = q_refs[group][:, span]
                scores = nt_dot(queries, keys[group][:, span]) * width ** (-0.5)
                state = 2 * group + m
                if diagonal:
                    allowed = lax.broadcasted_iota(jnp.int32, (rows, rows), 1) <= lax.broadcasted_iota(
                        jnp.int32, (rows, rows), 0
                    )
                    scores = jnp.where(allowed, scores, -1e30)
                    top = jnp.max(scores, axis=1, keepdims=True)
                    weights = jnp.exp(scores - top)
                    peak[state] = top
                    total[state] = jnp.sum(weights, axis=1, keepdims=True)
                    acc[state] = dot(weights.astype(jnp.bfloat16), values)
                else:
                    before = peak[state]
                    top = jnp.maximum(before, jnp.max(scores, axis=1, keepdims=True))
                    fade = jnp.exp(before - top)
                    weights = jnp.exp(scores - top)
                    peak[state] = top
                    total[state] = total[state] * fade + jnp.sum(weights, axis=1, keepdims=True)
                    acc[state] = acc[state] * fade + dot(weights.astype(jnp.bfloat16), values)

    with scoped("diag"):
        block((k1_ref, k2_ref), v_ref, True)
    for back in others:

        @pl.when(s >= back)
        def _(back=back):
            with scoped(f"kvwait{back}"):
                for i, copy in enumerate(arrived(back)):
                    copy.wait_recv()
                    if back < last:
                        pl.when(s < last)(kv_copies(back)[i].start)
            with scoped(f"block{back}"):
                block((k1b.at[back], k2b.at[back]), vb.at[back], False)

    next_step()
    proj_copy.wait()
    loads[-1].wait()
    with scoped("finish"):
        attended = []
        for group in range(2):
            first = acc[2 * group] / total[2 * group]
            second = acc[2 * group + 1] / total[2 * group + 1]
            differ = first - lam_ref[0, group] * second
            scale = lax.rsqrt(jnp.mean(differ * differ, axis=1, keepdims=True) + 1e-06)
            attended.append((0.8 * differ * scale).astype(jnp.bfloat16))

    def project(owner):
        columns = pl.ds(pl.multiple_of(owner * blk, blk), blk)
        return dot(attended[0], proj_ref[0, :, columns]) + dot(attended[1], proj_ref[1, :, columns])

    with scoped("project"):
        mp[0] = project(cpeer).astype(jnp.bfloat16)
        mp[1] = project(dpeer).astype(jnp.bfloat16)
        to_core = remote(mp.at[pl.ds(0, 2)], rsb.at[pl.ds(0, 2)], rs_ss.at[0], rs_rs.at[0], tp=cpeer)
        to_core.start()
        to_x = remote(mp.at[2], rsb.at[2], rs_ss.at[0], rs_rs.at[1], tp=xpeer)
        mine_ref[1] = project(xpeer)
        mine_ref[0] = residual_ref[...].astype(jnp.float32) + project(t)
    next_step()
    with scoped("rscore"):
        to_core.wait_recv()
    mp[2] = (mine_ref[1] + rsb[1].astype(jnp.float32)).astype(jnp.bfloat16)
    to_x.start()
    mine_ref[0] = mine_ref[0] + rsb[0].astype(jnp.float32)
    next_step()
    with scoped("rsx"):
        to_x.wait_recv()
    stream[...] = mine_ref[0] + rsb[2].astype(jnp.float32)
    act[t, s] = stream[...].astype(jnp.bfloat16)

    for here in everyone:

        @pl.when(s == here)
        def _(here=here):
            send_row(here, here)

    next_step()

    for copy in gain_copies:
        copy.wait_recv()

    def await_weights(kinds, source):
        def go(short):
            for kind in kinds:

                @pl.when(source != s)
                def _(kind=kind):
                    for part in range(PARTS):
                        place = final_place(kind, source, last if short else 0, part, 1 - y)
                        sem = PARTS * source + part
                        remote(place, place, f_ss.at[kind // 2], f_rs.at[kind, sem], grp=1 - y).wait_recv()

                @pl.when(source == s)
                def _(kind=kind):
                    own_copy(kind, short).wait()

        either(s == last, go)

    with scoped("await_gu"):
        for source in everyone:
            await_weights((0, 1), source)
    column = jnp.minimum(s * cols, hidden_all - cols) + lax.broadcasted_iota(jnp.int32, (1, cols), 1)
    mine = column >= s * cols

    def hidden_of(k):
        row = flip(s, k)
        with scoped(f"acwait{k}"):
            act_c(row, 0).wait_recv()
            act_c(row, 1).wait_recv()
        with scoped(f"hidden{k}"):
            squares = jnp.zeros((rows, 1), jnp.float32)
            for part in range(sp_count):
                piece = act[part, row].astype(jnp.float32)
                squares = squares + jnp.sum(piece * piece, axis=1, keepdims=True)
            scale = lax.rsqrt(squares / (sp_count * blk) + 1e-06)
            gate = jnp.zeros((rows, cols), jnp.float32)
            up = jnp.zeros((rows, cols), jnp.float32)
            for part in range(sp_count):
                gain = gains[part, 0:1, :].astype(jnp.float32)
                normed = (act[part, row].astype(jnp.float32) * scale * gain).astype(jnp.bfloat16)
                gate = gate + dot(normed, wg[part])
                up = up + dot(normed, wu[part])
            hidden = gate / (1.0 + jnp.exp(-gate)) * up
            hid[k] = jnp.where(mine, hidden, 0.0).astype(jnp.bfloat16)

    core = t % 2
    half_rows = rows // 2
    r1, r2, r3 = {}, {}, {}
    for k in everyone:
        for far in range(2):
            r1[k, far] = remote(c1.at[k, far], c1r.at[k, far], c_ss.at[0], c_rs.at[far, k], tp=cpeer)
        for h in range(2):
            some = pl.ds(h * half_rows, half_rows)
            r2[k, h] = remote(c2.at[k, some], c2r.at[k, some], c_ss.at[1], c_rs.at[2 + h, k], tp=xpeer)
            if k:
                target = flip(s, 1 if k == 3 else k)
                r3[k, h] = remote(c3.at[k, some], c3r.at[k, some], c_ss.at[2], c_rs.at[4 + h, k], sp=target)

    def block_of(wave, far):
        return 2 * ((1 - x) if far else x) + wave

    def product(wave, k, far):
        with scoped(f"product{wave}{k}{far}"):
            value = dot(hid[k], wd[block_of(wave, far)])

            @pl.when(core == wave)
            def _():
                po[k, far] = value

            @pl.when(core != wave)
            def _():
                c1[k, far] = value.astype(jnp.bfloat16)
                r1[k, far].start()

    def to_other_chip(wave, k):
        @pl.when(core == wave)
        def _():
            with scoped(f"cross{wave}{k}"):
                r1[k, 1].wait_recv()
            for h in range(2):
                some = pl.ds(h * half_rows, half_rows)
                c2[k, some] = (po[k, 1, some] + c1r[k, 1, some].astype(jnp.float32)).astype(jnp.bfloat16)
                r2[k, h].start()

    def settle(wave, k):
        @pl.when(core == wave)
        def _():
            with scoped(f"settle{wave}{k}"):
                r1[k, 0].wait_recv()
            for h in range(2):
                some = pl.ds(h * half_rows, half_rows)
                with scoped(f"settle{wave}{k}{h}"):
                    r2[k, h].wait_recv()
                result = po[k, 0, some] + c1r[k, 0, some].astype(jnp.float32) + c2r[k, some].astype(jnp.float32)
                if k == 2:
                    with scoped(f"pair{wave}{h}"):
                        r3[3, h].wait_recv()
                    result = result + c3r[3, some].astype(jnp.float32)
                if k:
                    c3[k, some] = result.astype(jnp.bfloat16)
                    r3[k, h].start()
                else:
                    po[0, 0, some] = result

    for name, *where in TAIL:
        next_step()
        if name == "hidden":
            hidden_of(where[0])
        elif name in ("far", "near"):
            product(*where, far=int(name == "far"))
        elif name == "cross":
            to_other_chip(*where)
        elif name == "settle":
            settle(*where)
        else:
            with scoped(f"{name}{where[0]}"):
                await_weights((2,), block_of(where[0], name == "await_far"))

    next_step()
    for h in range(2):
        some = pl.ds(h * half_rows, half_rows)
        for k in (1, 2):
            with scoped(f"r3_{k}{h}"):
                r3[k, h].wait_recv()
        ffn = po[0, 0, some] + c3r[1, some].astype(jnp.float32) + c3r[2, some].astype(jnp.float32)
        out_ref[some, :] = (stream[some, :] + 0.5 * ffn).astype(jnp.bfloat16)

    def sent(ref, sem):
        remote(ref, ref, sem, rs_rs.at[0], tp=cpeer).wait_send()

    def weights_sent(sems, width):
        sent(gate_ref.at[:, pl.ds(0, width)], sems.at[0])
        sent(down_ref.at[pl.ds(0, width // 2), :], sems.at[1])

    def width_of(target):
        return piece_bounds(target)[2]

    with scoped("drain"):
        for here in everyone:

            @pl.when(s == here)
            def _(here=here):
                if here < last:
                    for i, buffer in enumerate((k1b, k2b, vb)):
                        sent(buffer.at[pl.ds(0, here + 1)], kv_ss.at[i])
                    sent(act.at[0, pl.ds(0, here + 1)], az_ss.at[0])
                if here:
                    sent(act.at[0, pl.ds(0, sp_count - here)], az_ss.at[1])
                weights_sent(w_ss, sum(width_of(there) for there in everyone if there != here))
                weights_sent(f_ss, (sp_count - 1) * width_of(here))
                through = [
                    width_of(target)
                    for source in everyone
                    for target in everyone
                    if min(source, target) < here < max(source, target)
                ]
                if through:
                    weights_sent(t_ss, sum(through))

        sent(act.at[0], ax_ss.at[0])
        sent(act.at[pl.ds(0, 2)], ac_ss.at[0])
        sent(gains.at[pl.ds(0, sp_count - 1)], g_ss.at[0])
        sent(mp, rs_ss.at[0])
        sent(c1, c_ss.at[0])
        sent(c2, c_ss.at[1])
        sent(c3.at[pl.ds(0, sp_count - 1)], c_ss.at[2])


def fits(axes, query_first, values, lambdas, residual, gate_weight):
    sp, tp = axes["sp"], axes["tp"]
    rows, blk = residual.shape
    depth, hidden_all = gate_weight.shape
    if axes["grp"] != 2 or sp != tp or tp != 4 or lambdas.shape[1] != 1:
        return False
    if depth != blk or blk % 128 or hidden_all % 128 or rows % 16:
        return False
    if (2 * query_first.shape[1]) % 256 or values.shape[2] % 128:
        return False
    cols = -(-hidden_all // (128 * sp)) * 128
    if cols * sp - hidden_all >= cols or cols > hidden_all:
        return False
    if (cols * sp - hidden_all) % 128 or blk % 64 or rows % 32:
        return False
    need = 6 * sp * blk * cols + rows * blk * 2 * 20 * sp
    return need < 40 * 1024 * 1024


def one_device(
    axes,
    query_first,
    key_first,
    query_second,
    key_second,
    values,
    lambdas,
    residual,
    norm_gain,
    out_weight,
    gate_weight,
    up_weight,
    down_weight,
):
    if not fits(axes, query_first, values, lambdas, residual, gate_weight):
        return per_device(
            query_first,
            key_first,
            query_second,
            key_second,
            values,
            lambdas,
            residual,
            norm_gain,
            out_weight,
            gate_weight,
            up_weight,
            down_weight,
        )
    n = axes["sp"]
    rows, blk = residual.shape
    hidden_all = gate_weight.shape[1]
    cols = -(-hidden_all // (128 * n)) * 128
    value_size = values.shape[2]
    widths = (query_first.shape[1] // 2, query_second.shape[1] // 2)
    bf16, f32 = jnp.bfloat16, jnp.float32
    vmem = pl.BlockSpec(memory_space=pltpu.VMEM)
    hbm = pl.BlockSpec(memory_space=pl.ANY)
    dma = pltpu.SemaphoreType.DMA
    return pl.pallas_call(
        functools.partial(layer_kernel, n, widths),
        out_shape=jax.ShapeDtypeStruct((rows, blk), bf16),
        in_specs=[hbm] * 12,
        out_specs=vmem,
        scratch_shapes=[
            pltpu.VMEM(query_first.shape, bf16),
            pltpu.VMEM(query_second.shape, bf16),
            pltpu.VMEM(key_first.shape, bf16),
            pltpu.VMEM(key_second.shape, bf16),
            pltpu.VMEM(values.shape, bf16),
            pltpu.SMEM(lambdas.T.shape, f32),
            pltpu.VMEM(residual.shape, bf16),
            pltpu.VMEM(norm_gain.shape, bf16),
            pltpu.VMEM((n,) + key_first.shape, bf16),
            pltpu.VMEM((n,) + key_second.shape, bf16),
            pltpu.VMEM((n,) + values.shape, bf16),
            pltpu.VMEM(out_weight.shape, bf16),
            pltpu.VMEM((4, rows, 1), f32),
            pltpu.VMEM((4, rows, 1), f32),
            pltpu.VMEM((4, rows, value_size), f32),
            pltpu.VMEM((n, blk, cols), bf16),
            pltpu.VMEM((n, blk, cols), bf16),
            pltpu.VMEM((n, cols, blk), bf16),
            pltpu.VMEM((4, blk // 2, cols), bf16),
            pltpu.VMEM((4, blk // 2, cols), bf16),
            pltpu.VMEM((4, cols // 2, blk), bf16),
            pltpu.VMEM((3, rows, blk), bf16),
            pltpu.VMEM((3, rows, blk), bf16),
            pltpu.VMEM((2, rows, blk), f32),
            pltpu.VMEM((rows, blk), f32),
            pltpu.VMEM((n, n, rows, blk), bf16),
            pltpu.VMEM((n, 16, blk), bf16),
            pltpu.VMEM((n, rows, cols), bf16),
            pltpu.VMEM((n, 2, rows, blk), bf16),
            pltpu.VMEM((n, 2, rows, blk), bf16),
            pltpu.VMEM((n, 2, rows, blk), f32),
            pltpu.VMEM((n, rows, blk), bf16),
            pltpu.VMEM((n, rows, blk), bf16),
            pltpu.VMEM((n, rows, blk), bf16),
            pltpu.VMEM((n, rows, blk), bf16),
            dma((3,)),
            dma((3, n - 1)),
            dma((2,)),
            dma((3, PARTS * n)),
            dma((2,)),
            dma((3, PARTS * n)),
            dma((2,)),
            dma((3, PARTS * n)),
            dma((4,)),
            dma((8,)),
            dma((1,)),
            dma((n - 1,)),
            dma((1,)),
            dma((2,)),
            dma((2,)),
            dma((n,)),
            dma((1,)),
            dma((n,)),
            dma((1,)),
            dma((2, n)),
            dma((3,)),
            dma((6, n)),
        ],
        compiler_params=pltpu.CompilerParams(
            collective_id=0, has_side_effects=True, vmem_limit_bytes=60 * 1024 * 1024
        ),
    )(
        query_first,
        query_second,
        key_first,
        key_second,
        values,
        lambdas.T,
        residual,
        norm_gain,
        out_weight,
        gate_weight,
        up_weight,
        down_weight,
    )

def solution(mesh):
    return jax.shard_map(
        functools.partial(one_device, dict(mesh.shape)),
        mesh=mesh,
        in_specs=(
            P(("grp", "sp"), "tp"),
            P(("grp", "sp"), "tp"),
            P(("grp", "sp"), "tp"),
            P(("grp", "sp"), "tp"),
            P(("grp", "sp"), None, "tp"),
            P(None, "tp"),
            P(("grp", "sp"), "tp"),
            P("tp"),
            P(None, "tp", None),
            P("sp", "tp"),
            P("sp", "tp"),
            P("tp", "sp"),
        ),
        out_specs=P(("grp", "sp"), "tp"),
        check_vma=False,
    )
```
